32 devices in a mesh: sp: 8 (over z, x), tp: 4 (over y, core).
Axes of the slice: x: 2, y: 2, z: 4, core: 2. Of those that a mesh axis runs over, the one named last changes fastest.
Arguments:
- queries: bfloat16 [1024, 2048], P('sp', 'tp'), may hold values from -15 to 15
- key_rows: bfloat16 [1024, 2048], P('sp', 'tp'), may hold values from -6 to 6
- value_rows: bfloat16 [1024, 2048], P('sp', 'tp'), may hold values from -6 to 6
- break_bias: bfloat16 [1024, 16], P('sp', 'tp'), may hold values from -14 to 1
- stream: bfloat16 [1024, 4096], P('sp', 'tp'), may hold values from -24 to 24
- out_proj: bfloat16 [2048, 4096], P(None, 'tp'), may hold values from -0.5 to 0.5
- norm_gain: float32 [4096], P('tp'), may hold values from 0.1 to 1.9
- expert_ids: int32 [1024, 2], P('sp'), may hold values from 0 to 15, all different within a row; in each aligned block of 128 rows (0 to 127, 128 to 255, ...) at most 32 rows name the same one
- route_weights: float32 [1024, 2], P('sp'), may hold values from 0.1 to 2.5
- gate_proj: bfloat16 [16, 4096, 384], P('sp', 'tp'), may hold values from -0.09375 to 0.09375
- up_proj: bfloat16 [16, 4096, 384], P('sp', 'tp'), may hold values from -0.09375 to 0.09375
- down_proj: bfloat16 [16, 384, 4096], P('sp', None, 'tp'), may hold values from -0.3125 to 0.3125
- shared_gate: bfloat16 [4096, 384], P('tp'), may hold values from -0.09375 to 0.09375
- shared_up: bfloat16 [4096, 384], P('tp'), may hold values from -0.09375 to 0.09375
- shared_down: bfloat16 [384, 4096], P(None, 'tp'), may hold values from -0.3125 to 0.3125
Outputs:
- result: bfloat16 [1024, 4096], P('sp', 'tp')
The draws below stay inside these ranges and needn't reach their ends.
Inputs may be any that keep to these rules, and one draw needn't show every extreme that they name: `expert_ids`: each row names 2 different experts; within the rows of one index of sp no expert is named by more than 32 rows, a bound that some block reaches of them.
All inputs are finite; a program needn't handle non-finite values.
Results may differ from the reference program's by a relative error of at most 0.022.
Values may be sent and summed in bfloat16 or wider, within the bound.
A program may use at most 64 MiB of HBM per device.

```python
import math
import jax
import jax.numpy as jnp
import numpy as np
from jax import lax

D = 4096
ATTENTION_HEADS = 16
HD = 128
FFE = 384
FFS = 384
TOPK = 2
TOK_DEV = 128
SEQUENCE_TOKENS = 1024
EXPERTS = 16
CAP = 32
N_SP = 8
N_TP = 4


score_shift = 3.125


def draw_break_bias(key, part):
    every_key_rows = jax.random.split(jax.random.fold_in(key, 11), 5)
    fast_share = 0.5
    head_draw = jax.random.uniform(every_key_rows[0], (ATTENTION_HEADS,))
    fast_heads = head_draw < fast_share
    head_level = jnp.where(fast_heads, jnp.log(1.0 / 40.0), jnp.log(1.0 / SEQUENCE_TOKENS)) - score_shift
    block_shift = jax.random.uniform(every_key_rows[1], (SEQUENCE_TOKENS // TOK_DEV, ATTENTION_HEADS), minval=-0.7, maxval=0.7)
    jitter = 0.5 * jax.random.normal(every_key_rows[2], (SEQUENCE_TOKENS, ATTENTION_HEADS))
    logarithm_break_ratio = head_level[None, :] + jnp.repeat(block_shift, TOK_DEV, axis=0) + jitter
    stick_break_mask = jax.random.uniform(every_key_rows[3], (SEQUENCE_TOKENS, ATTENTION_HEADS)) < 4.0 / SEQUENCE_TOKENS
    break_probability = jax.random.uniform(every_key_rows[4], (SEQUENCE_TOKENS, ATTENTION_HEADS), minval=0.2, maxval=0.5)
    stick_break_level = jnp.log(break_probability / (1.0 - break_probability))
    return jnp.clip(jnp.where(stick_break_mask, stick_break_level, logarithm_break_ratio), -14.0, 1.0).astype(jnp.bfloat16)


def draw_stream(key, part):
    every_key_rows = jax.random.split(jax.random.fold_in(key, 23), 3)
    column_level = jnp.linspace(jnp.log(0.3), jnp.log(3.0), D) + 0.4 * jax.random.normal(every_key_rows[0], (D,))
    row_level = jax.random.uniform(every_key_rows[1], (SEQUENCE_TOKENS, 1), minval=jnp.log(0.15), maxval=jnp.log(1.5))
    base_values = jax.random.normal(every_key_rows[2], (SEQUENCE_TOKENS, D))
    scaled = base_values * jnp.exp(column_level)[None, :] * jnp.exp(row_level)
    return jnp.clip(scaled, -24.0, 24.0).astype(jnp.bfloat16)


def levels(rng, dims, shards, low, high):
    loudness, own = 1.0, jax.random.fold_in(rng, 6)
    for axis_at, blocks in shards:
        steps = jnp.exp(jax.random.uniform(jax.random.fold_in(own, axis_at), (blocks,), jnp.float32, low / len(shards), high / len(shards)))
        loudness = loudness * jnp.repeat(steps, dims[axis_at] // blocks).reshape([-1 if axis == axis_at else 1 for axis in range(len(dims))])
    return loudness


def deal_out(key, own, number, rows, amount, top, reach, lean):
    order = jax.random.permutation(key, amount)
    heavy_load, usual = shares(amount, rows * top, reach, lean, True), shares(amount, rows * top, reach, lean, False)
    places = jnp.arange(amount)

    def named(tallies, turn):
        used = int((tallies > 0).sum())
        fixed = max(1, used // 4)
        shifted = fixed + (places - fixed + turn * (used - fixed)) % max(1, amount - fixed)
        return jnp.zeros((amount,), jnp.int32).at[order[jnp.where(places < fixed, places, shifted)]].set(jnp.asarray(tallies, jnp.int32))

    tallies = jnp.where(number % 4 == 0, named(heavy_load, number // 4), named(usual, number - number // 4 - 1))
    mixed = jax.random.permutation(jax.random.fold_in(own, 3), amount)
    donor, receiver = mixed[0:amount // 2 * 2:2], mixed[1:amount // 2 * 2:2]
    room = jnp.minimum(tallies[donor] - 1, reach - tallies[receiver]) // 2
    room = jnp.where((donor == order[0]) | (receiver == order[0]) | (tallies[receiver] == 0), 0, jnp.maximum(room, 0))
    shifted = jax.random.randint(jax.random.fold_in(own, 4), (amount // 2,), 0, 1 << 20) % (room + 1)
    tallies = tallies.at[donor].add(-shifted).at[receiver].add(shifted)
    members = jnp.searchsorted(jnp.cumsum(tallies), jnp.arange(rows * top), side="right").astype(jnp.int32)
    table = members.reshape(top, rows).T
    table = table[jax.random.permutation(jax.random.fold_in(own, 1), rows)]
    turn = jax.random.randint(jax.random.fold_in(own, 2), (rows, 1), 0, top)
    return jnp.take_along_axis(table, (jnp.arange(top)[None, :] + turn) % top, axis=1)


def shares(number_of, total, bound, slope, full):
    portions = [(1 << 20) // math.isqrt(grade ** slope) + 1 for grade in range(1, number_of + 1)]
    largest = bound if full else min(bound, max(-(-total // number_of), total * portions[0] // sum(portions)))
    least = 1 if total - largest >= number_of - 1 else 0
    given, spare = [largest] + [least] * (number_of - 1), total - largest - least * (number_of - 1)
    while spare > 0:
        candidates = [i for i in range(1, number_of) if given[i] < largest] or [i for i in range(1, number_of) if given[i] < bound]
        pool, remaining = sum([portions[i] for i in candidates]), spare
        for i in candidates:
            more = min(bound - given[i], max(1, remaining * portions[i] // pool), spare)
            given[i] = given[i] + more
            spare = spare - more
    return np.array(given)


def normal_values(key, extent, deviation, bound, shards=(), held_as=jnp.bfloat16):
    loudness = levels(key, extent, shards, -0.22, 0.18) if shards else 1.0
    drawn = jax.random.normal(key, extent, jnp.float32) * deviation * loudness
    return jnp.minimum(jnp.maximum(drawn, -bound), bound).astype(held_as)


def setup_inputs(seed: int = 0) -> dict:
    streams_of = jax.random.split(jax.random.key(seed), 16)
    queries = normal_values(streams_of[0], (SEQUENCE_TOKENS, ATTENTION_HEADS * HD), 2.5, 15.0, ((0, 8), (1, 4)))
    key_rows = normal_values(streams_of[1], (SEQUENCE_TOKENS, ATTENTION_HEADS * HD), 1.0, 6.0, ((0, 8), (1, 4)))
    value_rows = normal_values(streams_of[2], (SEQUENCE_TOKENS, ATTENTION_HEADS * HD), 1.0, 6.0, ((0, 8), (1, 4)))
    break_bias = draw_break_bias(jax.random.fold_in(streams_of[15], 71), 0)
    stream = draw_stream(jax.random.fold_in(streams_of[15], 71), 0)
    out_proj = normal_values(streams_of[5], (ATTENTION_HEADS * HD, D), (ATTENTION_HEADS * HD // 16) ** -0.5, 0.5, ((1, 4),))
    norm_gain = jnp.clip(1.0 + 0.18 * jax.random.normal(streams_of[6], (D,), jnp.float32), 0.1, 1.9)
    expert_ids_keys = jax.random.split(jax.random.fold_in(streams_of[7], 1), SEQUENCE_TOKENS // TOK_DEV)
    expert_ids_turns = jax.random.permutation(jax.random.fold_in(streams_of[7], 3), SEQUENCE_TOKENS // TOK_DEV)
    expert_ids = jax.vmap(lambda own, number: deal_out(jax.random.fold_in(streams_of[7], 2), own, number, TOK_DEV, EXPERTS, TOPK, CAP, 2))(expert_ids_keys, expert_ids_turns).reshape((SEQUENCE_TOKENS, TOPK))
    route_weights = jnp.clip(jnp.exp(math.log(2.5) - 3.218876 * jax.random.uniform(streams_of[8], (SEQUENCE_TOKENS, TOPK), jnp.float32) ** levels(streams_of[8], (SEQUENCE_TOKENS, TOPK), ((0, 8),), -0.2, 0.2)), 0.1, 2.5)
    gate_proj = normal_values(streams_of[9], (EXPERTS, D, FFE), D ** -0.5, 0.09375, ((0, 8), (1, 4)))
    up_proj = normal_values(streams_of[10], (EXPERTS, D, FFE), D ** -0.5, 0.09375, ((0, 8), (1, 4)))
    down_proj = normal_values(streams_of[11], (EXPERTS, FFE, D), FFE ** -0.5, 0.3125, ((0, 8), (2, 4)))
    shared_gate = normal_values(streams_of[12], (D, FFS), D ** -0.5, 0.09375, ((0, 4),))
    shared_up = normal_values(streams_of[13], (D, FFS), D ** -0.5, 0.09375, ((0, 4),))
    shared_down = normal_values(streams_of[14], (FFS, D), FFS ** -0.5, 0.3125, ((1, 4),))
    return {"queries": queries, "key_rows": key_rows, "value_rows": value_rows, "break_bias": break_bias, "stream": stream, "out_proj": out_proj, "norm_gain": norm_gain, "expert_ids": expert_ids, "route_weights": route_weights, "gate_proj": gate_proj, "up_proj": up_proj, "down_proj": down_proj, "shared_gate": shared_gate, "shared_up": shared_up, "shared_down": shared_down}


EPS = 1e-06
query_block = 128

def stick_attention(queries, key_rows, value_rows, break_bias):
    head_q = queries.astype(jnp.float32).reshape(SEQUENCE_TOKENS, ATTENTION_HEADS, HD)
    head_k = key_rows.astype(jnp.float32).reshape(SEQUENCE_TOKENS, ATTENTION_HEADS, HD)
    head_v = value_rows.astype(jnp.float32).reshape(SEQUENCE_TOKENS, ATTENTION_HEADS, HD)
    bias_heads = break_bias.astype(jnp.float32).T
    key_pos = jnp.arange(SEQUENCE_TOKENS, dtype=jnp.int32)

    def one_block(block_index):
        offset = block_index * query_block
        query_part = lax.dynamic_slice_in_dim(head_q, offset, query_block, 0)
        positions = offset + jnp.arange(query_block, dtype=jnp.int32)
        logits = jnp.einsum('thd,shd->hts', query_part, head_k) * HD ** (-0.5) + bias_heads[:, None, :]
        before = (key_pos[None, :] < positions[:, None])[None]
        log_fail = jnp.where(before, jax.nn.log_sigmoid(-logits), 0.0)
        tail_sum = lax.cumsum(log_fail, axis=2, reverse=True) - log_fail
        weights = jnp.where(before, jnp.exp(jax.nn.log_sigmoid(logits) + tail_sum), 0.0)
        return jnp.einsum('hts,shd->thd', weights, head_v)
    outputs = lax.map(one_block, jnp.arange(SEQUENCE_TOKENS // query_block, dtype=jnp.int32))
    return outputs.reshape(SEQUENCE_TOKENS, ATTENTION_HEADS * HD).astype(jnp.bfloat16)

def block_sum(row_block, weight):
    feature_cut = row_block.shape[1] // N_TP

    def add_block(running, block_index):
        part_rows = lax.dynamic_slice_in_dim(row_block, block_index * feature_cut, feature_cut, 1)
        part_weight = lax.dynamic_slice_in_dim(weight, block_index * feature_cut, feature_cut, 0)
        partial_value = jnp.dot(part_rows, part_weight, preferred_element_type=jnp.float32).astype(jnp.bfloat16)
        partial_value = lax.optimization_barrier(partial_value)
        return (running + partial_value.astype(jnp.float32), None)
    start_sum = jnp.zeros((row_block.shape[0], weight.shape[1]), jnp.float32)
    running, _ = lax.scan(add_block, start_sum, jnp.arange(N_TP, dtype=jnp.int32))
    return running

def reference(queries, key_rows, value_rows, break_bias, stream, out_proj, norm_gain, expert_ids, route_weights, gate_proj, up_proj, down_proj, shared_gate, shared_up, shared_down):
    attended = stick_attention(queries, key_rows, value_rows, break_bias)
    mixed = (stream.astype(jnp.float32) + jnp.dot(attended, out_proj, preferred_element_type=jnp.float32)).astype(jnp.bfloat16)
    mixed = lax.optimization_barrier(mixed)
    mixed_f = mixed.astype(jnp.float32)
    inv_rms = lax.rsqrt(lax.optimization_barrier(jnp.mean(mixed_f * mixed_f, axis=1, keepdims=True)) + EPS)
    normed = (mixed_f * inv_rms * norm_gain[None, :]).astype(jnp.bfloat16)
    shared_hidden = (jax.nn.silu(block_sum(normed, shared_gate)) * block_sum(normed, shared_up)).astype(jnp.bfloat16)
    shared_out = jnp.dot(shared_hidden, shared_down, preferred_element_type=jnp.float32)
    rows_max = N_SP * CAP
    padded = jnp.concatenate([normed, jnp.zeros((1, D), jnp.bfloat16)], 0)

    def one_expert(running, expert):
        matches = expert_ids == expert
        chosen = jnp.any(matches, axis=1)
        weight_row = lax.optimization_barrier(jnp.sum(jnp.where(matches, route_weights, 0.0), axis=1))
        weight_pad = jnp.concatenate([weight_row, jnp.zeros((1,), jnp.float32)], 0)
        picked = jnp.nonzero(chosen, size=rows_max, fill_value=SEQUENCE_TOKENS)[0].astype(jnp.int32)
        row_block = padded[picked]
        gate_pre = block_sum(row_block, gate_proj[expert])
        up_pre = block_sum(row_block, up_proj[expert])
        hidden = (jax.nn.silu(gate_pre) * up_pre).astype(jnp.bfloat16)
        expert_out = jnp.dot(hidden, down_proj[expert], preferred_element_type=jnp.float32).astype(jnp.bfloat16)
        scaled = weight_pad[picked][:, None] * expert_out.astype(jnp.float32)
        return (running.at[picked].add(scaled), None)
    routed, _ = lax.scan(one_expert, jnp.zeros((SEQUENCE_TOKENS + 1, D), jnp.float32), jnp.arange(EXPERTS, dtype=jnp.int32))
    return (mixed_f + shared_out + routed[:SEQUENCE_TOKENS]).astype(jnp.bfloat16)
```

```python
import functools

import jax
import jax.numpy as jnp
from jax import lax
from jax.experimental import pallas as pl
from jax.experimental.pallas import tpu as pltpu
from jax.sharding import PartitionSpec as P

EPS = 1e-06
F32 = jnp.float32
BF16 = jnp.bfloat16


def attention_kernel(
    heads, hd, n_sp, inner, q_ref, k_ref, v_ref, b_ref, o_ref, kbuf, vbuf, bbuf, acc, carry, send_sem, recv_sem
):
    tok = q_ref.shape[0]
    own = lax.axis_index("sp")
    outer = n_sp // inner
    z_own = own // inner
    x_own = own % inner
    above = z_own < outer - 1
    below = z_own > 0

    barrier = pltpu.get_barrier_semaphore()

    def greet(target):
        pl.semaphore_signal(
            barrier, inc=1, device_id={"sp": target}, device_id_type=pl.DeviceIdType.MESH
        )

    @pl.when(above)
    def _():
        greet(own + inner)

    @pl.when(below)
    def _():
        greet(own - inner)

    for d in range(1, inner):
        greet(z_own * inner + (x_own + d) % inner)
    pl.semaphore_wait(barrier, inner - 1 + above.astype(jnp.int32) + below.astype(jnp.int32))

    def copies(sources, block, z_block, lane, target):
        return [
            pltpu.make_async_remote_copy(
                src_ref=src,
                dst_ref=dst.at[block],
                send_sem=send_sem.at[kind, z_block, lane],
                recv_sem=recv_sem.at[kind, block],
                device_id={"sp": target},
                device_id_type=pl.DeviceIdType.MESH,
            )
            for kind, (src, dst) in enumerate(zip(sources, (kbuf, vbuf, bbuf)))
        ]

    def held(block):
        return (kbuf.at[block], vbuf.at[block], bbuf.at[block])

    def start_all(group):
        for c in group:
            c.start()

    def wait_sent(group):
        for c in group:
            c.wait_send()

    def wait_arrived(block):
        for c in copies(held(block), block, 0, 0, (own + 1) % n_sp):
            c.wait_recv()

    def own_sends(act):
        mine = (k_ref, v_ref, b_ref)

        @pl.when(above)
        def _():
            act(copies(mine, own, z_own, 0, own + inner))

        for d in range(1, inner):
            x_to = (x_own + d) % inner

            @pl.when(x_to > x_own)
            def _():
                act(copies(mine, own, z_own, d, z_own * inner + x_to))

    def relays(z_block, act):
        block = z_block * inner + x_own

        @pl.when(above)
        def _():
            act(copies(held(block), block, z_block, 0, own + inner))

        for d in range(1, inner):
            act(copies(held(block), block, z_block, d, z_own * inner + (x_own + d) % inner))

    own_sends(start_all)

    scale = hd ** (-0.5)
    row = lax.broadcasted_iota(jnp.int32, (tok, tok), 0)
    col = lax.broadcasted_iota(jnp.int32, (tok, tok), 1)
    later = (row > col).astype(F32)
    sums = jnp.concatenate([later, jnp.ones((tok, tok), F32)], axis=1).astype(BF16)
    sums = jnp.concatenate([sums, sums], axis=0)
    pick_rows = max(16, heads)
    pick = (
        lax.broadcasted_iota(jnp.int32, (pick_rows, hd), 0)
        == lax.broadcasted_iota(jnp.int32, (pick_rows, hd), 1)
    ).astype(F32).astype(BF16)
    acc[...] = jnp.zeros_like(acc)
    carry[...] = jnp.zeros_like(carry)

    def compute(keys, values, offsets, diagonal):
        bias = lax.dot_general(
            pick, offsets[...], (((1,), (1,)), ((), ())), preferred_element_type=F32
        )
        for h in range(heads):
            cols = slice(h * hd, (h + 1) * hd)
            z = lax.dot_general(
                q_ref[:, cols], keys[:, cols], (((1,), (1,)), ((), ())), preferred_element_type=F32
            )
            z = z * scale + bias[h : h + 1, :]
            low = jnp.log1p(jnp.exp(-jnp.abs(z)))
            fail = -(jnp.maximum(z, 0.0) + low)
            hit = jnp.minimum(z, 0.0) - low
            if diagonal:
                before = col < row
                fail = jnp.where(before, fail, 0.0)
            high = fail.astype(BF16)
            rest = (fail - high.astype(F32)).astype(BF16)
            both = jnp.dot(
                jnp.concatenate([high, rest], axis=1), sums, preferred_element_type=F32
            )
            before_sum = carry[h]
            w = jnp.exp(hit + both[:, :tok] + before_sum)
            if diagonal:
                w = jnp.where(before, w, 0.0)
            carry[h] = before_sum + both[:, tok:]
            acc[:, cols] += jnp.dot(w.astype(BF16), values[:, cols], preferred_element_type=F32)

    compute(k_ref, v_ref, b_ref, True)

    def group(i, _):
        z_block = z_own - i

        @pl.when(z_block > 0)
        def _():
            wait_arrived((z_block - 1) * inner + x_own)
            relays(z_block - 1, start_all)

        def member(m, _):
            x_block = inner - 1 - m
            block = z_block * inner + x_block

            @pl.when(block < own)
            def _():
                @pl.when(x_block != x_own)
                def _():
                    wait_arrived(block)

                compute(*held(block), False)

            return 0

        lax.fori_loop(0, inner, member, 0)
        return 0

    lax.fori_loop(0, z_own + 1, group, 0)
    o_ref[...] = acc[...].astype(BF16)

    own_sends(wait_sent)

    def drain(z_block, _):
        relays(z_block, wait_sent)
        return 0

    lax.fori_loop(0, z_own, drain, 0)


def attention(queries, keys, values, bias, heads, hd, n_sp):
    tok = queries.shape[0]
    inner = max(d for d in range(1, n_sp + 1) if n_sp % d == 0 and d * d <= n_sp)
    vmem = pl.BlockSpec(memory_space=pltpu.VMEM)
    return pl.pallas_call(
        functools.partial(attention_kernel, heads, hd, n_sp, inner),
        out_shape=jax.ShapeDtypeStruct((tok, heads * hd), BF16),
        in_specs=[vmem] * 4,
        out_specs=vmem,
        scratch_shapes=[
            pltpu.VMEM((n_sp, tok, heads * hd), BF16),
            pltpu.VMEM((n_sp, tok, heads * hd), BF16),
            pltpu.VMEM((n_sp, tok, hd), BF16),
            pltpu.VMEM((tok, heads * hd), F32),
            pltpu.VMEM((heads, tok, tok), F32),
            pltpu.SemaphoreType.DMA((3, n_sp // inner, inner)),
            pltpu.SemaphoreType.DMA((3, n_sp)),
        ],
        compiler_params=pltpu.CompilerParams(
            vmem_limit_bytes=40 * 2**20, collective_id=0, has_side_effects=True
        ),
        cost_estimate=pl.CostEstimate(flops=2 * 10**9, bytes_accessed=2**22, transcendentals=10**6),
    )(queries, keys, values, bias)


def exchange_kernel(n_tp, gu_ref, o_ref, parts, mine, spread, send_parts, recv_parts, send_rows, recv_rows):
    width = gu_ref.shape[2] // 2
    me = lax.axis_index("tp")
    barrier = pltpu.get_barrier_semaphore()
    others = [(me + d) % n_tp for d in range(1, n_tp)]
    for to in others:
        pl.semaphore_signal(
            barrier, inc=1, device_id={"tp": to}, device_id_type=pl.DeviceIdType.MESH
        )
    pl.semaphore_wait(barrier, n_tp - 1)
    first, second = [], []
    for d, to in enumerate(others):
        copy = pltpu.make_async_remote_copy(
            src_ref=gu_ref.at[to],
            dst_ref=parts.at[d],
            send_sem=send_parts.at[d],
            recv_sem=recv_parts.at[d],
            device_id={"tp": to},
            device_id_type=pl.DeviceIdType.MESH,
        )
        copy.start()
        first.append(copy)
    total = gu_ref[me].astype(F32)
    for d, copy in enumerate(first):
        copy.wait_recv()
        total = total + parts[d].astype(F32)
    gate = total[:, :width]
    mine[...] = (jax.nn.silu(gate) * total[:, width:]).astype(BF16)
    for d, to in enumerate(others):
        copy = pltpu.make_async_remote_copy(
            src_ref=mine,
            dst_ref=spread.at[d],
            send_sem=send_rows.at[d],
            recv_sem=recv_rows.at[d],
            device_id={"tp": to},
            device_id_type=pl.DeviceIdType.MESH,
        )
        copy.start()
        second.append(copy)
    o_ref[me] = mine[...]
    for d, copy in enumerate(second):
        copy.wait_recv()
        o_ref[(me + n_tp - 1 - d) % n_tp] = spread[d]
    for copy in first + second:
        copy.wait_send()


def exchange(gate_up, n_tp):
    rows, width = gate_up.shape[0] // n_tp, gate_up.shape[1] // 2
    vmem = pl.BlockSpec(memory_space=pltpu.VMEM)
    dma = pltpu.SemaphoreType.DMA((n_tp - 1,))
    hidden = pl.pallas_call(
        functools.partial(exchange_kernel, n_tp),
        out_shape=jax.ShapeDtypeStruct((n_tp, rows, width), BF16),
        in_specs=[vmem],
        out_specs=vmem,
        scratch_shapes=[
            pltpu.VMEM((n_tp - 1, rows, 2 * width), BF16),
            pltpu.VMEM((rows, width), BF16),
            pltpu.VMEM((n_tp - 1, rows, width), BF16),
            dma,
            dma,
            dma,
            dma,
        ],
        compiler_params=pltpu.CompilerParams(
            vmem_limit_bytes=24 * 2**20, collective_id=1, has_side_effects=True
        ),
        cost_estimate=pl.CostEstimate(flops=10**8, bytes_accessed=2**21, transcendentals=10**5),
    )(gate_up.reshape(n_tp, rows, 2 * width))
    return hidden.reshape(n_tp * rows, width)


MESH = pl.DeviceIdType.MESH


def rows_contract(lhs, rhs):
    return lax.dot_general(lhs, rhs, (((1,), (1,)), ((), ())), preferred_element_type=F32)


def rcopy(src, dst, send_sem, recv_sem, where):
    return pltpu.make_async_remote_copy(
        src_ref=src,
        dst_ref=dst,
        send_sem=send_sem,
        recv_sem=recv_sem,
        device_id=where,
        device_id_type=MESH,
    )


def plane_order(z, outer):
    if outer != 4:
        return [(z + i) % outer for i in range(outer)]
    middle = ((z + 1) // 2) % 2
    near = z + 1 - 2 * (z % 2)
    across = 3 - z
    two = (z + 2) % 4
    return [
        z,
        near,
        middle * across + (1 - middle) * two,
        middle * two + (1 - middle) * across,
    ]


def greet_all(n_sp, n_tp, own, me):
    barrier = pltpu.get_barrier_semaphore()
    for d in range(1, n_sp):
        pl.semaphore_signal(
            barrier, inc=1, device_id={"sp": (own + d) % n_sp}, device_id_type=MESH
        )
    for d in range(1, n_tp):
        pl.semaphore_signal(
            barrier, inc=1, device_id={"tp": (me + d) % n_tp}, device_id_type=MESH
        )
    pl.semaphore_wait(barrier, n_sp + n_tp - 2)


class Experts:
    def __init__(self, n_sp, n_tp, inner, experts_local, cap, refs):
        self.n_sp, self.n_tp, self.inner = n_sp, n_tp, inner
        self.outer = n_sp // inner
        self.el, self.cap = experts_local, cap
        self.rw = experts_local * cap
        self.__dict__.update(refs)
        self.own = lax.axis_index("sp")
        self.me = lax.axis_index("tp")
        self.z = self.own // inner
        self.x = self.own % inner
        self.order = plane_order(self.z, self.outer)
        self.tok, self.width = self.mixed.shape
        self.ff = self.down.shape[1]
        self.total_width = self.width * n_tp

    def load_weights(self):
        ff = self.ff
        self.loads = [
            pltpu.make_async_copy(src, dst, self.w_sem.at[i])
            for i, (src, dst) in enumerate(
                (
                    (self.s_gate, self.wsgu.at[:, pl.ds(0, ff)]),
                    (self.s_up, self.wsgu.at[:, pl.ds(ff, ff)]),
                    (self.gate, self.wgu.at[:, :, pl.ds(0, ff)]),
                    (self.up, self.wgu.at[:, :, pl.ds(ff, ff)]),
                    (self.down, self.wd),
                    (self.s_down, self.wsd),
                )
            )
        ]
        for load in self.loads:
            load.start()

    def meta_copies(self, ref, send, recv):
        return [
            rcopy(
                ref.at[self.own],
                ref.at[self.own],
                send.at[d],
                recv.at[self.own],
                {"sp": (self.own + d) % self.n_sp},
            )
            for d in range(1, self.n_sp)
        ]

    def wait_table(self, ref, send, recv, block):
        rcopy(
            ref.at[block], ref.at[block], send.at[0], recv.at[block], {"sp": (self.own + 1) % self.n_sp}
        ).wait_recv()

    def route(self):
        ids = self.ids[...]
        experts = self.el * self.n_sp
        top_k, tok = ids.shape
        expert_of = lax.broadcasted_iota(jnp.int32, (experts, tok), 0)
        named = [ids[k : k + 1, :] == expert_of for k in range(top_k)]
        named_any = functools.reduce(jnp.logical_or, named).astype(F32).astype(BF16)
        before = (
            lax.broadcasted_iota(jnp.int32, (tok, tok), 0)
            < lax.broadcasted_iota(jnp.int32, (tok, tok), 1)
        ).astype(F32).astype(BF16)
        rank = jnp.dot(named_any, before, preferred_element_type=F32)
        self.meta[self.own] = jnp.zeros((8, tok), F32)
        for k in range(top_k):
            mine = jnp.sum(jnp.where(named[k], rank, 0.0), axis=0, keepdims=True)
            slot = ids[k : k + 1, :].astype(F32) * self.cap + mine
            self.meta[self.own, k : k + 1, :] = slot
        self.top_k = top_k
        self.meta_group = self.meta_copies(self.meta, self.meta_s, self.meta_r)
        for c in self.meta_group:
            c.start()

    def slot_hits(self, block, first, count):
        spot = (
            lax.broadcasted_iota(jnp.int32, (count, self.tok), 0) + first
        ).astype(F32)
        return [self.meta[block, k : k + 1, :] == spot for k in range(self.top_k)]

    def build_back(self):
        rows = self.inner * self.rw
        for plane in range(self.outer):
            hits = self.slot_hits(self.own, plane * rows, rows)
            weight = sum(
                jnp.where(hits[k], self.wts[k : k + 1, :], 0.0) for k in range(self.top_k)
            )
            self.back[plane] = jnp.transpose(weight).astype(BF16)

    def dense_copy(self, src, plane, step):
        return rcopy(
            src,
            self.dense.at[plane],
            self.dense_s.at[plane, (step + 1) // 2],
            self.dense_r.at[plane],
            {"sp": (self.z + step) * self.inner + self.x},
        )

    def spread_own(self, act):
        for step in (1, -1):

            @pl.when(self.z < self.outer - 1 if step == 1 else self.z > 0)
            def _():
                act(self.dense_copy(self.mixed, self.z, step))

    def hand_on(self, plane, act):
        @pl.when((plane < self.z) & (self.z < self.outer - 1))
        def _():
            act(self.dense_copy(self.dense.at[plane], plane, 1))

        @pl.when((plane > self.z) & (self.z > 0))
        def _():
            act(self.dense_copy(self.dense.at[plane], plane, -1))

    def take_dense(self, i):
        plane = self.order[i]
        rcopy(
            self.dense.at[plane],
            self.dense.at[plane],
            self.dense_s.at[plane, 0],
            self.dense_r.at[plane],
            {"sp": (self.own + 1) % self.n_sp},
        ).wait_recv()
        self.hand_on(plane, lambda c: c.start())

    def cross_copies(self, i):
        return [
            rcopy(
                self.picked.at[i, (self.x + d) % self.inner],
                self.rows.at[i, self.x],
                self.x_s.at[i, d],
                self.x_r.at[i, self.x],
                {"sp": self.z * self.inner + (self.x + d) % self.inner},
            )
            for d in range(1, self.inner)
        ]

    def select(self, i):
        block = self.order[i] * self.inner + self.x
        if i:
            self.wait_table(self.meta, self.meta_s, self.meta_r, block)
        rows = self.inner * self.rw
        hits = self.slot_hits(block, self.z * rows, rows)
        pick = functools.reduce(jnp.logical_or, hits).astype(F32).astype(BF16)
        source = self.dense[self.order[i]] if i else self.mixed[...]
        got = jnp.dot(pick, source, preferred_element_type=F32).astype(BF16)
        for p in range(self.inner):
            self.picked[i, p] = got[p * self.rw : (p + 1) * self.rw]
        for c in self.cross_copies(i):
            c.start()
        self.rows[i, self.x] = self.picked[i, self.x]

    def tp_copies(self, src, dst, send, recv):
        return [
            rcopy(src(to), dst, send.at[d], recv.at[self.me], {"tp": to})
            for d, to in ((d, (self.me + d) % self.n_tp) for d in range(1, self.n_tp))
        ]

    def tp_wait(self, dst, send, recv):
        for d in range(1, self.n_tp):
            other = (self.me + d) % self.n_tp
            rcopy(
                dst(other), dst(other), send.at[0], recv.at[other], {"tp": (self.me + 1) % self.n_tp}
            ).wait_recv()

    def send_squares(self):
        wide = self.mixed[...].astype(F32)
        column = jnp.sum(wide * wide, axis=1, keepdims=True)
        row = jnp.transpose(jnp.broadcast_to(column, (self.tok, self.tok)))
        self.ssq[self.me] = row[:8]
        self.ssq_group = self.tp_copies(
            lambda to: self.ssq.at[self.me], self.ssq.at[self.me], self.ssq_s, self.ssq_r
        )
        for c in self.ssq_group:
            c.start()

    def send_scales(self):
        self.tp_wait(lambda other: self.ssq.at[other], self.ssq_s, self.ssq_r)
        total = self.ssq[0]
        for p in range(1, self.n_tp):
            total = total + self.ssq[p]
        self.inv[self.own] = lax.rsqrt(total / self.total_width + EPS)
        self.inv_group = self.meta_copies(self.inv, self.inv_s, self.inv_r)
        for c in self.inv_group:
            c.start()

    def send_parts(self, s, value):
        chunk = value.shape[0] // self.n_tp
        for p in range(self.n_tp):
            self.gu[s, p] = value[p * chunk : (p + 1) * chunk]
        group = self.tp_copies(
            lambda to: self.gu.at[s, to], self.parts.at[s, self.me], self.part_s.at[s], self.part_r.at[s]
        )
        for c in group:
            c.start()
        self.part_groups[s] = group

    def gate_up(self, i):
        if i == 0:
            self.loads[2].wait()
            self.loads[3].wait()
        for d in range(1, self.inner):
            x_from = (self.x + d) % self.inner
            rcopy(
                self.rows.at[i, x_from],
                self.rows.at[i, x_from],
                self.x_s.at[i, d],
                self.x_r.at[i, x_from],
                {"sp": (self.own + 1) % self.n_sp},
            ).wait_recv()
        normed = []
        for d in range(self.inner):
            block = self.order[i] * self.inner + (self.x + d) % self.inner
            if d:
                self.wait_table(self.meta, self.meta_s, self.meta_r, block)
            if i or d:
                self.wait_table(self.inv, self.inv_s, self.inv_r, block)
        for p in range(self.inner):
            block = self.order[i] * self.inner + p
            hits = self.slot_hits(block, self.own * self.rw, self.rw)
            pick = functools.reduce(jnp.logical_or, hits)
            scale = jnp.sum(
                jnp.where(pick, self.inv[block, 0:1, :], 0.0), axis=1, keepdims=True
            )
            wide = self.rows[i, p].astype(F32)
            normed.append((wide * scale * self.gain[...]).astype(BF16))
        out = []
        for e in range(self.el):
            rows = jnp.concatenate(
                [n[e * self.cap : (e + 1) * self.cap] for n in normed], axis=0
            )
            out.append(jnp.dot(rows, self.wgu[e], preferred_element_type=F32).astype(BF16))
        self.send_parts(i, jnp.concatenate(out, axis=0))

    def shared_gate_up(self):
        self.loads[0].wait()
        self.loads[1].wait()
        scale = jnp.transpose(jnp.broadcast_to(self.inv[self.own, 0:1, :], (self.tok, self.tok)))
        normed = (
            self.mixed[...].astype(F32) * scale[:, 0:1] * self.gain[...]
        ).astype(BF16)
        value = jnp.dot(normed, self.wsgu[...], preferred_element_type=F32).astype(BF16)
        self.send_parts(self.outer, value)

    def hidden(self, s):
        self.tp_wait(lambda other: self.parts.at[s, other], self.part_s.at[s], self.part_r.at[s])
        total = self.gu[s, self.me].astype(F32)
        for d in range(1, self.n_tp):
            total = total + self.parts[s, (self.me + d) % self.n_tp].astype(F32)
        act = jax.nn.silu(total[:, : self.ff]) * total[:, self.ff :]
        self.hid[s, self.me] = act.astype(BF16)
        group = self.tp_copies(
            lambda to: self.hid.at[s, self.me], self.hid.at[s, self.me], self.hid_s.at[s], self.hid_r.at[s]
        )
        for c in group:
            c.start()
        self.hid_groups[s] = group

    def all_hidden(self, s):
        self.tp_wait(lambda other: self.hid.at[s, other], self.hid_s.at[s], self.hid_r.at[s])
        return jnp.concatenate([self.hid[s, p] for p in range(self.n_tp)], axis=0)

    def return_copies(self, i):
        return [
            rcopy(
                self.outs.at[i, (self.x + d) % self.inner],
                self.ret.at[self.own],
                self.ret_s.at[i, d],
                self.ret_r.at[self.own],
                {"sp": self.order[i] * self.inner + (self.x + d) % self.inner},
            )
            for d in range(0 if i else 1, self.inner)
        ]

    def down_rows(self, i):
        if i == 0:
            self.loads[4].wait()
        hidden = self.all_hidden(i)
        span = self.inner * self.cap
        for e in range(self.el):
            out = jnp.dot(
                hidden[e * span : (e + 1) * span], self.wd[e], preferred_element_type=F32
            ).astype(BF16)
            for p in range(self.inner):
                self.outs[i, p, e * self.cap : (e + 1) * self.cap, :] = out[
                    p * self.cap : (p + 1) * self.cap
                ]
        for c in self.return_copies(i):
            c.start()
        if i == 0:
            self.ret[self.own] = self.outs[0, self.x]

    def shared_down(self):
        self.loads[5].wait()
        shared = jnp.dot(
            self.all_hidden(self.outer), self.wsd[...], preferred_element_type=F32
        )
        self.acc[...] = self.mixed[...].astype(F32) + shared

    def collect(self, i, last=False):
        plane = self.order[i]
        for d in range(0 if i else 1, self.inner):
            block = plane * self.inner + (self.x + d) % self.inner
            rcopy(
                self.ret.at[block],
                self.ret.at[block],
                self.ret_s.at[i, d],
                self.ret_r.at[block],
                {"sp": (self.own + 1) % self.n_sp},
            ).wait_recv()
        rows = jnp.concatenate(
            [self.ret[plane * self.inner + p] for p in range(self.inner)], axis=0
        )
        got = jnp.dot(self.back[plane], rows, preferred_element_type=F32)
        if last:
            self.out[...] = (self.acc[...] + got).astype(BF16)
        else:
            self.acc[...] += got

    def finish(self):
        def sent(c):
            c.wait_send()

        self.spread_own(sent)
        for i in range(1, self.outer):
            self.hand_on(self.order[i], sent)
        groups = [self.meta_group, self.inv_group, self.ssq_group]
        groups += list(self.part_groups.values()) + list(self.hid_groups.values())
        groups += [self.cross_copies(i) for i in range(self.outer)]
        groups += [self.return_copies(i) for i in range(self.outer)]
        for group in groups:
            for c in group:
                c.wait_send()

    def run(self):
        outer = self.outer
        self.part_groups, self.hid_groups = {}, {}
        self.spread_own(lambda c: c.start())
        self.send_squares()
        self.select(0)
        self.build_back()
        self.send_scales()
        self.shared_gate_up()
        self.gate_up(0)
        for i in range(1, outer + 1):
            if i < outer:
                self.take_dense(i)
                self.select(i)
            if i == 1:
                self.hidden(outer)
            self.hidden(i - 1)
            if i == 1:
                self.shared_down()
            if i < outer:
                self.gate_up(i)
            self.down_rows(i - 1)
        for i in range(outer):
            self.collect(i, i == outer - 1)
        self.finish()


MOE_INPUTS = (
    "mixed", "ids", "wts", "gain", "gate", "up", "down", "s_gate", "s_up", "s_down",
)


def moe_scratch(n_sp, n_tp, inner, el, cap, tok, width, ff):
    outer, rw = n_sp // inner, el * cap
    chunk = inner * rw // n_tp
    chunk_s = tok // n_tp
    assert chunk == chunk_s
    vmem, dma = pltpu.VMEM, pltpu.SemaphoreType.DMA
    return {
        "wgu": vmem((el, width, 2 * ff), BF16),
        "wd": vmem((el, ff, width), BF16),
        "wsgu": vmem((width, 2 * ff), BF16),
        "wsd": vmem((ff, width), BF16),
        "dense": vmem((outer, tok, width), BF16),
        "picked": vmem((outer, inner, rw, width), BF16),
        "rows": vmem((outer, inner, rw, width), BF16),
        "meta": vmem((n_sp, 8, tok), F32),
        "inv": vmem((n_sp, 8, tok), F32),
        "ssq": vmem((n_tp, 8, tok), F32),
        "gu": vmem((outer + 1, n_tp, chunk, 2 * ff), BF16),
        "parts": vmem((outer + 1, n_tp, chunk, 2 * ff), BF16),
        "hid": vmem((outer + 1, n_tp, chunk, ff), BF16),
        "outs": vmem((outer, inner, rw, width), BF16),
        "ret": vmem((n_sp, rw, width), BF16),
        "back": vmem((outer, tok, inner * rw), BF16),
        "acc": vmem((tok, width), F32),
        "w_sem": dma((6,)),
        "meta_s": dma((n_sp,)),
        "meta_r": dma((n_sp,)),
        "inv_s": dma((n_sp,)),
        "inv_r": dma((n_sp,)),
        "ssq_s": dma((n_tp,)),
        "ssq_r": dma((n_tp,)),
        "dense_s": dma((outer, 2)),
        "dense_r": dma((outer,)),
        "x_s": dma((outer, inner)),
        "x_r": dma((outer, inner)),
        "part_s": dma((outer + 1, n_tp)),
        "part_r": dma((outer + 1, n_tp)),
        "hid_s": dma((outer + 1, n_tp)),
        "hid_r": dma((outer + 1, n_tp)),
        "ret_s": dma((outer, inner)),
        "ret_r": dma((n_sp,)),
    }


def moe_kernel(n_sp, n_tp, inner, el, cap, names, *refs):
    work = Experts(n_sp, n_tp, inner, el, cap, dict(zip(names, refs)))
    work.load_weights()
    work.route_ready = None
    greet_all(n_sp, n_tp, work.own, work.me)
    work.route()
    work.run()


def moe(mixed, ids, wts, gain, gate, up, down, s_gate, s_up, s_down, n_sp, n_tp, inner, cap):
    tok, width = mixed.shape
    el, ff = down.shape[:2]
    scratch = moe_scratch(n_sp, n_tp, inner, el, cap, tok, width, ff)
    vmem = pl.BlockSpec(memory_space=pltpu.VMEM)
    hbm = pl.BlockSpec(memory_space=pltpu.MemorySpace.HBM)
    names = MOE_INPUTS + ("out",) + tuple(scratch)
    return pl.pallas_call(
        functools.partial(moe_kernel, n_sp, n_tp, inner, el, cap, names),
        out_shape=jax.ShapeDtypeStruct((tok, width), BF16),
        in_specs=[vmem] * 4 + [hbm] * 6,
        out_specs=vmem,
        scratch_shapes=list(scratch.values()),
        compiler_params=pltpu.CompilerParams(
            vmem_limit_bytes=40 * 2**20, collective_id=2, has_side_effects=True
        ),
        cost_estimate=pl.CostEstimate(flops=10**10, bytes_accessed=2**23, transcendentals=10**6),
    )(mixed, ids, wts, gain, gate, up, down, s_gate, s_up, s_down)


def body(
    queries,
    key_rows,
    value_rows,
    break_bias,
    stream,
    out_proj,
    norm_gain,
    expert_ids,
    route_weights,
    gate_proj,
    up_proj,
    down_proj,
    shared_gate,
    shared_up,
    shared_down,
):
    tok = queries.shape[0]
    heads = break_bias.shape[1]
    hd = queries.shape[1] // heads
    n_sp = lax.axis_size("sp")
    n_tp = lax.axis_size("tp")
    width = stream.shape[1] * n_tp

    bias_wide = jnp.pad(break_bias, ((0, 0), (0, hd - heads)))

    experts_local = gate_proj.shape[0]
    experts = experts_local * n_sp
    top_k = expert_ids.shape[1]
    cap = 2 * top_k * tok // experts
    n_inner = max(d for d in range(1, n_sp + 1) if n_sp % d == 0 and d * d <= n_sp)
    plane_rows = n_inner * experts_local * cap
    if cap % 16 == 0 and plane_rows == tok and tok % (16 * n_tp) == 0:
        attended = attention(queries, key_rows, value_rows, bias_wide, heads, hd, n_sp)
        projected = jnp.dot(
            lax.all_gather(attended, "tp", axis=1, tiled=True), out_proj, preferred_element_type=F32
        )
        mixed = (stream.astype(F32) + projected).astype(BF16)
        return moe(
            mixed, expert_ids.T, route_weights.T, norm_gain[None, :], gate_proj, up_proj, down_proj,
            shared_gate, shared_up, shared_down, n_sp, n_tp, n_inner, cap,
        )
    expert_of = jnp.arange(experts, dtype=jnp.int32)
    named = expert_ids[:, :, None] == expert_of[None, None, :]
    named_any = jnp.any(named, axis=1).astype(BF16)
    token = jnp.arange(tok, dtype=jnp.int32)
    earlier = (token[None, :] < token[:, None]).astype(BF16)
    rank_all = jnp.dot(earlier, named_any, preferred_element_type=F32)
    rank = jnp.sum(jnp.where(named, rank_all[:, None, :], 0.0), axis=2).astype(jnp.int32)
    slot = expert_ids * cap + rank
    slots = experts * cap
    place = jnp.arange(slots, dtype=jnp.int32)
    spot = slot[:, :, None] == place[None, None, :]
    send_pick = jnp.any(spot, axis=1).astype(BF16)
    back_pick = jnp.sum(jnp.where(spot, route_weights[:, :, None], 0.0), axis=1).astype(BF16)

    attended = attention(queries, key_rows, value_rows, bias_wide, heads, hd, n_sp)
    projected = jnp.dot(
        lax.all_gather(attended, "tp", axis=1, tiled=True), out_proj, preferred_element_type=F32
    )
    mixed = (stream.astype(F32) + projected).astype(BF16)
    mixed = lax.optimization_barrier(mixed)
    mixed_f = mixed.astype(F32)
    square_sum = lax.psum(jnp.sum(mixed_f * mixed_f, axis=1), "tp")
    inv_rms = lax.rsqrt(square_sum / width + EPS)
    normed = (mixed_f * inv_rms[:, None] * norm_gain[None, :]).astype(BF16)

    send = lax.dot_general(
        send_pick, normed, (((0,), (0,)), ((), ())), preferred_element_type=F32
    ).astype(BF16)
    send = send.reshape(n_sp, experts_local * cap, normed.shape[1])
    arrived = lax.all_to_all(send, "sp", split_axis=0, concat_axis=0, tiled=True)
    arrived = arrived.reshape(n_sp, experts_local, cap, -1)
    gates, ups = [], []
    for e in range(experts_local):
        rows = arrived[:, e].reshape(n_sp * cap, -1)
        gates.append(jnp.dot(rows, gate_proj[e], preferred_element_type=F32).astype(BF16))
        ups.append(jnp.dot(rows, up_proj[e], preferred_element_type=F32).astype(BF16))
    gates.append(jnp.dot(normed, shared_gate, preferred_element_type=F32).astype(BF16))
    ups.append(jnp.dot(normed, shared_up, preferred_element_type=F32).astype(BF16))
    gate_all = jnp.concatenate(gates, axis=0)
    up_all = jnp.concatenate(ups, axis=0)
    gate_up = jnp.concatenate([gate_all, up_all], axis=1)
    hidden = exchange(gate_up, n_tp)
    outs = []
    for e in range(experts_local):
        rows = hidden[e * n_sp * cap : (e + 1) * n_sp * cap]
        out = jnp.dot(rows, down_proj[e], preferred_element_type=F32).astype(BF16)
        outs.append(out.reshape(n_sp, 1, cap, -1))
    expert_out = jnp.concatenate(outs, axis=1).reshape(n_sp, experts_local * cap, -1)
    returned = lax.all_to_all(expert_out, "sp", split_axis=0, concat_axis=0, tiled=True)
    returned = returned.reshape(slots, -1)
    shared_out = jnp.dot(
        hidden[experts_local * n_sp * cap :], shared_down, preferred_element_type=F32
    )
    routed = jnp.dot(back_pick, returned, preferred_element_type=F32)
    return (mixed_f + shared_out + routed).astype(BF16)


def solution(mesh):
    in_specs = (
        P("sp", "tp"),
        P("sp", "tp"),
        P("sp", "tp"),
        P("sp", "tp"),
        P("sp", "tp"),
        P(None, "tp"),
        P("tp"),
        P("sp", None),
        P("sp", None),
        P("sp", "tp", None),
        P("sp", "tp", None),
        P("sp", None, "tp"),
        P("tp", None),
        P("tp", None),
        P(None, "tp"),
    )
    return jax.shard_map(body, mesh=mesh, in_specs=in_specs, out_specs=P("sp", "tp"), check_vma=False)
```

```python
import functools

import jax
import jax.numpy as jnp
from jax import lax
from jax.experimental import pallas as pl
from jax.experimental.pallas import tpu as pltpu
from jax.sharding import PartitionSpec as P

EPS = 1e-06
F32 = jnp.float32
BF16 = jnp.bfloat16


def attention_kernel(
    heads, hd, n_sp, inner, q_ref, k_ref, v_ref, b_ref, o_ref, kbuf, vbuf, bbuf, acc, carry, send_sem, recv_sem
):
    tok = q_ref.shape[0]
    own = lax.axis_index("sp")
    outer = n_sp // inner
    z_own = own // inner
    x_own = own % inner
    above = z_own < outer - 1
    below = z_own > 0

    barrier = pltpu.get_barrier_semaphore()

    def greet(target):
        pl.semaphore_signal(
            barrier, inc=1, device_id={"sp": target}, device_id_type=pl.DeviceIdType.MESH
        )

    @pl.when(above)
    def _():
        greet(own + inner)

    @pl.when(below)
    def _():
        greet(own - inner)

    for d in range(1, inner):
        greet(z_own * inner + (x_own + d) % inner)
    pl.semaphore_wait(barrier, inner - 1 + above.astype(jnp.int32) + below.astype(jnp.int32))

    def copies(sources, block, z_block, lane, target):
        return [
            pltpu.make_async_remote_copy(
                src_ref=src,
                dst_ref=dst.at[block],
                send_sem=send_sem.at[kind, z_block, lane],
                recv_sem=recv_sem.at[kind, block],
                device_id={"sp": target},
                device_id_type=pl.DeviceIdType.MESH,
            )
            for kind, (src, dst) in enumerate(zip(sources, (kbuf, vbuf, bbuf)))
        ]

    def held(block):
        return (kbuf.at[block], vbuf.at[block], bbuf.at[block])

    def start_all(group):
        for c in group:
            c.start()

    def wait_sent(group):
        for c in group:
            c.wait_send()

    def wait_arrived(block):
        for c in copies(held(block), block, 0, 0, (own + 1) % n_sp):
            c.wait_recv()

    def own_sends(act):
        mine = (k_ref, v_ref, b_ref)

        @pl.when(above)
        def _():
            act(copies(mine, own, z_own, 0, own + inner))

        for d in range(1, inner):
            x_to = (x_own + d) % inner

            @pl.when(x_to > x_own)
            def _():
                act(copies(mine, own, z_own, d, z_own * inner + x_to))

    def relays(z_block, act):
        block = z_block * inner + x_own

        @pl.when(above)
        def _():
            act(copies(held(block), block, z_block, 0, own + inner))

        for d in range(1, inner):
            act(copies(held(block), block, z_block, d, z_own * inner + (x_own + d) % inner))

    own_sends(start_all)

    scale = hd ** (-0.5)
    row = lax.broadcasted_iota(jnp.int32, (tok, tok), 0)
    col = lax.broadcasted_iota(jnp.int32, (tok, tok), 1)
    later = (row > col).astype(F32)
    sums = jnp.concatenate([later, jnp.ones((tok, tok), F32)], axis=1).astype(BF16)
    sums = jnp.concatenate([sums, sums], axis=0)
    pick_rows = max(16, heads)
    pick = (
        lax.broadcasted_iota(jnp.int32, (pick_rows, hd), 0)
        == lax.broadcasted_iota(jnp.int32, (pick_rows, hd), 1)
    ).astype(F32).astype(BF16)
    acc[...] = jnp.zeros_like(acc)
    carry[...] = jnp.zeros_like(carry)

    def compute(keys, values, offsets, diagonal):
        bias = lax.dot_general(
            pick, offsets[...], (((1,), (1,)), ((), ())), preferred_element_type=F32
        )
        for h in range(heads):
            cols = slice(h * hd, (h + 1) * hd)
            z = lax.dot_general(
                q_ref[:, cols], keys[:, cols], (((1,), (1,)), ((), ())), preferred_element_type=F32
            )
            z = z * scale + bias[h : h + 1, :]
            low = jnp.log1p(jnp.exp(-jnp.abs(z)))
            fail = -(jnp.maximum(z, 0.0) + low)
            hit = jnp.minimum(z, 0.0) - low
            if diagonal:
                before = col < row
                fail = jnp.where(before, fail, 0.0)
            high = fail.astype(BF16)
            rest = (fail - high.astype(F32)).astype(BF16)
            both = jnp.dot(
                jnp.concatenate([high, rest], axis=1), sums, preferred_element_type=F32
            )
            before_sum = carry[h]
            w = jnp.exp(hit + both[:, :tok] + before_sum)
            if diagonal:
                w = jnp.where(before, w, 0.0)
            carry[h] = before_sum + both[:, tok:]
            acc[:, cols] += jnp.dot(w.astype(BF16), values[:, cols], preferred_element_type=F32)

    compute(k_ref, v_ref, b_ref, True)

    def group(i, _):
        z_block = z_own - i

        @pl.when(z_block > 0)
        def _():
            wait_arrived((z_block - 1) * inner + x_own)
            relays(z_block - 1, start_all)

        def member(m, _):
            x_block = inner - 1 - m
            block = z_block * inner + x_block

            @pl.when(block < own)
            def _():
                @pl.when(x_block != x_own)
                def _():
                    wait_arrived(block)

                compute(*held(block), False)

            return 0

        lax.fori_loop(0, inner, member, 0)
        return 0

    lax.fori_loop(0, z_own + 1, group, 0)
    o_ref[...] = acc[...].astype(BF16)

    own_sends(wait_sent)

    def drain(z_block, _):
        relays(z_block, wait_sent)
        return 0

    lax.fori_loop(0, z_own, drain, 0)


def attention(queries, keys, values, bias, heads, hd, n_sp):
    tok = queries.shape[0]
    inner = max(d for d in range(1, n_sp + 1) if n_sp % d == 0 and d * d <= n_sp)
    vmem = pl.BlockSpec(memory_space=pltpu.VMEM)
    return pl.pallas_call(
        functools.partial(attention_kernel, heads, hd, n_sp, inner),
        out_shape=jax.ShapeDtypeStruct((tok, heads * hd), BF16),
        in_specs=[vmem] * 4,
        out_specs=vmem,
        scratch_shapes=[
            pltpu.VMEM((n_sp, tok, heads * hd), BF16),
            pltpu.VMEM((n_sp, tok, heads * hd), BF16),
            pltpu.VMEM((n_sp, tok, hd), BF16),
            pltpu.VMEM((tok, heads * hd), F32),
            pltpu.VMEM((heads, tok, tok), F32),
            pltpu.SemaphoreType.DMA((3, n_sp // inner, inner)),
            pltpu.SemaphoreType.DMA((3, n_sp)),
        ],
        compiler_params=pltpu.CompilerParams(
            vmem_limit_bytes=40 * 2**20, collective_id=0, has_side_effects=True
        ),
        cost_estimate=pl.CostEstimate(flops=2 * 10**9, bytes_accessed=2**22, transcendentals=10**6),
    )(queries, keys, values, bias)


def exchange_kernel(n_tp, gu_ref, o_ref, parts, mine, spread, send_parts, recv_parts, send_rows, recv_rows):
    width = gu_ref.shape[2] // 2
    me = lax.axis_index("tp")
    barrier = pltpu.get_barrier_semaphore()
    others = [(me + d) % n_tp for d in range(1, n_tp)]
    for to in others:
        pl.semaphore_signal(
            barrier, inc=1, device_id={"tp": to}, device_id_type=pl.DeviceIdType.MESH
        )
    pl.semaphore_wait(barrier, n_tp - 1)
    first, second = [], []
    for d, to in enumerate(others):
        copy = pltpu.make_async_remote_copy(
            src_ref=gu_ref.at[to],
            dst_ref=parts.at[d],
            send_sem=send_parts.at[d],
            recv_sem=recv_parts.at[d],
            device_id={"tp": to},
            device_id_type=pl.DeviceIdType.MESH,
        )
        copy.start()
        first.append(copy)
    total = gu_ref[me].astype(F32)
    for d, copy in enumerate(first):
        copy.wait_recv()
        total = total + parts[d].astype(F32)
    gate = total[:, :width]
    mine[...] = (jax.nn.silu(gate) * total[:, width:]).astype(BF16)
    for d, to in enumerate(others):
        copy = pltpu.make_async_remote_copy(
            src_ref=mine,
            dst_ref=spread.at[d],
            send_sem=send_rows.at[d],
            recv_sem=recv_rows.at[d],
            device_id={"tp": to},
            device_id_type=pl.DeviceIdType.MESH,
        )
        copy.start()
        second.append(copy)
    o_ref[me] = mine[...]
    for d, copy in enumerate(second):
        copy.wait_recv()
        o_ref[(me + n_tp - 1 - d) % n_tp] = spread[d]
    for copy in first + second:
        copy.wait_send()


def exchange(gate_up, n_tp):
    rows, width = gate_up.shape[0] // n_tp, gate_up.shape[1] // 2
    vmem = pl.BlockSpec(memory_space=pltpu.VMEM)
    dma = pltpu.SemaphoreType.DMA((n_tp - 1,))
    hidden = pl.pallas_call(
        functools.partial(exchange_kernel, n_tp),
        out_shape=jax.ShapeDtypeStruct((n_tp, rows, width), BF16),
        in_specs=[vmem],
        out_specs=vmem,
        scratch_shapes=[
            pltpu.VMEM((n_tp - 1, rows, 2 * width), BF16),
            pltpu.VMEM((rows, width), BF16),
            pltpu.VMEM((n_tp - 1, rows, width), BF16),
            dma,
            dma,
            dma,
            dma,
        ],
        compiler_params=pltpu.CompilerParams(
            vmem_limit_bytes=24 * 2**20, collective_id=1, has_side_effects=True
        ),
        cost_estimate=pl.CostEstimate(flops=10**8, bytes_accessed=2**21, transcendentals=10**5),
    )(gate_up.reshape(n_tp, rows, 2 * width))
    return hidden.reshape(n_tp * rows, width)


MESH = pl.DeviceIdType.MESH


def rows_contract(lhs, rhs):
    return lax.dot_general(lhs, rhs, (((1,), (1,)), ((), ())), preferred_element_type=F32)


def rcopy(src, dst, send_sem, recv_sem, where):
    return pltpu.make_async_remote_copy(
        src_ref=src,
        dst_ref=dst,
        send_sem=send_sem,
        recv_sem=recv_sem,
        device_id=where,
        device_id_type=MESH,
    )


def plane_order(z, outer):
    if outer != 4:
        return [(z + i) % outer for i in range(outer)]
    middle = ((z + 1) // 2) % 2
    near = z + 1 - 2 * (z % 2)
    across = 3 - z
    two = (z + 2) % 4
    return [
        z,
        near,
        middle * across + (1 - middle) * two,
        middle * two + (1 - middle) * across,
    ]


def greet_all(n_sp, n_tp, own, me):
    barrier = pltpu.get_barrier_semaphore()
    for d in range(1, n_sp):
        pl.semaphore_signal(
            barrier, inc=1, device_id={"sp": (own + d) % n_sp}, device_id_type=MESH
        )
    for d in range(1, n_tp):
        pl.semaphore_signal(
            barrier, inc=1, device_id={"tp": (me + d) % n_tp}, device_id_type=MESH
        )
    pl.semaphore_wait(barrier, n_sp + n_tp - 2)


class Experts:
    def __init__(self, n_sp, n_tp, inner, experts_local, cap, refs):
        self.n_sp, self.n_tp, self.inner = n_sp, n_tp, inner
        self.outer = n_sp // inner
        self.el, self.cap = experts_local, cap
        self.rw = experts_local * cap
        self.__dict__.update(refs)
        self.own = lax.axis_index("sp")
        self.me = lax.axis_index("tp")
        self.z = self.own // inner
        self.x = self.own % inner
        self.order = plane_order(self.z, self.outer)
        self.tok, self.width = self.mixed.shape
        self.ff = self.down.shape[1]
        self.total_width = self.width * n_tp

    def load_weights(self):
        ff = self.ff
        self.loads = [
            pltpu.make_async_copy(src, dst, self.w_sem.at[i])
            for i, (src, dst) in enumerate(
                (
                    (self.s_gate, self.wsgu.at[:, pl.ds(0, ff)]),
                    (self.s_up, self.wsgu.at[:, pl.ds(ff, ff)]),
                    (self.gate, self.wgu.at[:, :, pl.ds(0, ff)]),
                    (self.up, self.wgu.at[:, :, pl.ds(ff, ff)]),
                    (self.down, self.wd),
                    (self.s_down, self.wsd),
                )
            )
        ]
        for load in self.loads:
            load.start()

    def meta_copies(self, ref, send, recv):
        return [
            rcopy(
                ref.at[self.own],
                ref.at[self.own],
                send.at[d],
                recv.at[self.own],
                {"sp": (self.own + d) % self.n_sp},
            )
            for d in range(1, self.n_sp)
        ]

    def wait_table(self, ref, send, recv, block):
        rcopy(
            ref.at[block], ref.at[block], send.at[0], recv.at[block], {"sp": (self.own + 1) % self.n_sp}
        ).wait_recv()

    def route(self):
        ids = self.ids[...]
        experts = self.el * self.n_sp
        top_k, tok = ids.shape
        expert_of = lax.broadcasted_iota(jnp.int32, (experts, tok), 0)
        named = [ids[k : k + 1, :] == expert_of for k in range(top_k)]
        named_any = functools.reduce(jnp.logical_or, named).astype(F32).astype(BF16)
        before = (
            lax.broadcasted_iota(jnp.int32, (tok, tok), 0)
            < lax.broadcasted_iota(jnp.int32, (tok, tok), 1)
        ).astype(F32).astype(BF16)
        rank = jnp.dot(named_any, before, preferred_element_type=F32)
        self.meta[self.own] = jnp.zeros((8, tok), F32)
        for k in range(top_k):
            mine = jnp.sum(jnp.where(named[k], rank, 0.0), axis=0, keepdims=True)
            slot = ids[k : k + 1, :].astype(F32) * self.cap + mine
            self.meta[self.own, k : k + 1, :] = slot
        self.top_k = top_k
        self.meta_group = self.meta_copies(self.meta, self.meta_s, self.meta_r)
        for c in self.meta_group:
            c.start()

    def slot_hits(self, block, first, count):
        spot = (
            lax.broadcasted_iota(jnp.int32, (count, self.tok), 0) + first
        ).astype(F32)
        return [self.meta[block, k : k + 1, :] == spot for k in range(self.top_k)]

    def build_back(self):
        rows = self.inner * self.rw
        for plane in range(self.outer):
            hits = self.slot_hits(self.own, plane * rows, rows)
            weight = sum(
                jnp.where(hits[k], self.wts[k : k + 1, :], 0.0) for k in range(self.top_k)
            )
            self.back[plane] = jnp.transpose(weight).astype(BF16)

    def dense_copy(self, src, plane, step):
        return rcopy(
            src,
            self.dense.at[plane],
            self.dense_s.at[plane, (step + 1) // 2],
            self.dense_r.at[plane],
            {"sp": (self.z + step) * self.inner + self.x},
        )

    def spread_own(self, act):
        for step in (1, -1):

            @pl.when(self.z < self.outer - 1 if step == 1 else self.z > 0)
            def _():
                act(self.dense_copy(self.mixed, self.z, step))

    def hand_on(self, plane, act):
        @pl.when((plane < self.z) & (self.z < self.outer - 1))
        def _():
            act(self.dense_copy(self.dense.at[plane], plane, 1))

        @pl.when((plane > self.z) & (self.z > 0))
        def _():
            act(self.dense_copy(self.dense.at[plane], plane, -1))

    def take_dense(self, i):
        plane = self.order[i]
        rcopy(
            self.dense.at[plane],
            self.dense.at[plane],
            self.dense_s.at[plane, 0],
            self.dense_r.at[plane],
            {"sp": (self.own + 1) % self.n_sp},
        ).wait_recv()
        self.hand_on(plane, lambda c: c.start())

    def cross_copies(self, i):
        return [
            rcopy(
                self.picked.at[i, (self.x + d) % self.inner],
                self.rows.at[i, self.x],
                self.x_s.at[i, d],
                self.x_r.at[i, self.x],
                {"sp": self.z * self.inner + (self.x + d) % self.inner},
            )
            for d in range(1, self.inner)
        ]

    def select(self, i):
        block = self.order[i] * self.inner + self.x
        if i:
            self.wait_table(self.meta, self.meta_s, self.meta_r, block)
        rows = self.inner * self.rw
        hits = self.slot_hits(block, self.z * rows, rows)
        pick = functools.reduce(jnp.logical_or, hits).astype(F32).astype(BF16)
        source = self.dense[self.order[i]] if i else self.mixed[...]
        got = jnp.dot(pick, source, preferred_element_type=F32).astype(BF16)
        for p in range(self.inner):
            self.picked[i, p] = got[p * self.rw : (p + 1) * self.rw]
        for c in self.cross_copies(i):
            c.start()
        self.rows[i, self.x] = self.picked[i, self.x]

    def tp_copies(self, src, dst, send, recv):
        return [
            rcopy(src(to), dst, send.at[d], recv.at[self.me], {"tp": to})
            for d, to in ((d, (self.me + d) % self.n_tp) for d in range(1, self.n_tp))
        ]

    def tp_wait(self, dst, send, recv):
        for d in range(1, self.n_tp):
            other = (self.me + d) % self.n_tp
            rcopy(
                dst(other), dst(other), send.at[0], recv.at[other], {"tp": (self.me + 1) % self.n_tp}
            ).wait_recv()

    def send_squares(self):
        wide = self.mixed[...].astype(F32)
        column = jnp.sum(wide * wide, axis=1, keepdims=True)
        row = jnp.transpose(jnp.broadcast_to(column, (self.tok, self.tok)))
        self.ssq[self.me] = row[:8]
        self.ssq_group = self.tp_copies(
            lambda to: self.ssq.at[self.me], self.ssq.at[self.me], self.ssq_s, self.ssq_r
        )
        for c in self.ssq_group:
            c.start()

    def send_scales(self):
        self.tp_wait(lambda other: self.ssq.at[other], self.ssq_s, self.ssq_r)
        total = self.ssq[0]
        for p in range(1, self.n_tp):
            total = total + self.ssq[p]
        self.inv[self.own] = lax.rsqrt(total / self.total_width + EPS)
        self.inv_group = self.meta_copies(self.inv, self.inv_s, self.inv_r)
        for c in self.inv_group:
            c.start()

    def send_parts(self, s, value):
        chunk = value.shape[0] // self.n_tp
        for p in range(self.n_tp):
            self.gu[s, p] = value[p * chunk : (p + 1) * chunk]
        group = self.tp_copies(
            lambda to: self.gu.at[s, to], self.parts.at[s, self.me], self.part_s.at[s], self.part_r.at[s]
        )
        for c in group:
            c.start()
        self.part_groups[s] = group

    def gate_up(self, i):
        if i == 0:
            self.loads[2].wait()
            self.loads[3].wait()
        for d in range(1, self.inner):
            x_from = (self.x + d) % self.inner
            rcopy(
                self.rows.at[i, x_from],
                self.rows.at[i, x_from],
                self.x_s.at[i, d],
                self.x_r.at[i, x_from],
                {"sp": (self.own + 1) % self.n_sp},
            ).wait_recv()
        normed = []
        for d in range(self.inner):
            block = self.order[i] * self.inner + (self.x + d) % self.inner
            if d:
                self.wait_table(self.meta, self.meta_s, self.meta_r, block)
            if i or d:
                self.wait_table(self.inv, self.inv_s, self.inv_r, block)
        for p in range(self.inner):
            block = self.order[i] * self.inner + p
            hits = self.slot_hits(block, self.own * self.rw, self.rw)
            pick = functools.reduce(jnp.logical_or, hits)
            scale = jnp.sum(
                jnp.where(pick, self.inv[block, 0:1, :], 0.0), axis=1, keepdims=True
            )
            wide = self.rows[i, p].astype(F32)
            normed.append((wide * scale * self.gain[...]).astype(BF16))
        out = []
        for e in range(self.el):
            rows = jnp.concatenate(
                [n[e * self.cap : (e + 1) * self.cap] for n in normed], axis=0
            )
            out.append(jnp.dot(rows, self.wgu[e], preferred_element_type=F32).astype(BF16))
        self.send_parts(i, jnp.concatenate(out, axis=0))

    def shared_gate_up(self):
        self.loads[0].wait()
        self.loads[1].wait()
        scale = jnp.transpose(jnp.broadcast_to(self.inv[self.own, 0:1, :], (self.tok, self.tok)))
        normed = (
            self.mixed[...].astype(F32) * scale[:, 0:1] * self.gain[...]
        ).astype(BF16)
        value = jnp.dot(normed, self.wsgu[...], preferred_element_type=F32).astype(BF16)
        self.send_parts(self.outer, value)

    def hidden(self, s):
        self.tp_wait(lambda other: self.parts.at[s, other], self.part_s.at[s], self.part_r.at[s])
        total = self.gu[s, self.me].astype(F32)
        for d in range(1, self.n_tp):
            total = total + self.parts[s, (self.me + d) % self.n_tp].astype(F32)
        act = jax.nn.silu(total[:, : self.ff]) * total[:, self.ff :]
        self.hid[s, self.me] = act.astype(BF16)
        group = self.tp_copies(
            lambda to: self.hid.at[s, self.me], self.hid.at[s, self.me], self.hid_s.at[s], self.hid_r.at[s]
        )
        for c in group:
            c.start()
        self.hid_groups[s] = group

    def all_hidden(self, s):
        self.tp_wait(lambda other: self.hid.at[s, other], self.hid_s.at[s], self.hid_r.at[s])
        return jnp.concatenate([self.hid[s, p] for p in range(self.n_tp)], axis=0)

    def return_copies(self, i):
        return [
            rcopy(
                self.outs.at[i, (self.x + d) % self.inner],
                self.ret.at[self.own],
                self.ret_s.at[i, d],
                self.ret_r.at[self.own],
                {"sp": self.order[i] * self.inner + (self.x + d) % self.inner},
            )
            for d in range(0 if i else 1, self.inner)
        ]

    def down_rows(self, i):
        if i == 0:
            self.loads[4].wait()
        hidden = self.all_hidden(i)
        span = self.inner * self.cap
        for e in range(self.el):
            out = jnp.dot(
                hidden[e * span : (e + 1) * span], self.wd[e], preferred_element_type=F32
            ).astype(BF16)
            for p in range(self.inner):
                self.outs[i, p, e * self.cap : (e + 1) * self.cap, :] = out[
                    p * self.cap : (p + 1) * self.cap
                ]
        for c in self.return_copies(i):
            c.start()
        if i == 0:
            self.ret[self.own] = self.outs[0, self.x]

    def shared_down(self):
        self.loads[5].wait()
        shared = jnp.dot(
            self.all_hidden(self.outer), self.wsd[...], preferred_element_type=F32
        )
        self.acc[...] = self.mixed[...].astype(F32) + shared

    def collect(self, i, last=False):
        plane = self.order[i]
        for d in range(0 if i else 1, self.inner):
            block = plane * self.inner + (self.x + d) % self.inner
            rcopy(
                self.ret.at[block],
                self.ret.at[block],
                self.ret_s.at[i, d],
                self.ret_r.at[block],
                {"sp": (self.own + 1) % self.n_sp},
            ).wait_recv()
        rows = jnp.concatenate(
            [self.ret[plane * self.inner + p] for p in range(self.inner)], axis=0
        )
        got = jnp.dot(self.back[plane], rows, preferred_element_type=F32)
        if last:
            self.out[...] = (self.acc[...] + got).astype(BF16)
        else:
            self.acc[...] += got

    def finish(self):
        def sent(c):
            c.wait_send()

        self.spread_own(sent)
        for i in range(1, self.outer):
            self.hand_on(self.order[i], sent)
        groups = [self.meta_group, self.inv_group, self.ssq_group]
        groups += list(self.part_groups.values()) + list(self.hid_groups.values())
        groups += [self.cross_copies(i) for i in range(self.outer)]
        groups += [self.return_copies(i) for i in range(self.outer)]
        for group in groups:
            for c in group:
                c.wait_send()

    def run(self):
        outer = self.outer
        self.part_groups, self.hid_groups = {}, {}
        self.spread_own(lambda c: c.start())
        self.send_squares()
        self.select(0)
        self.send_scales()
        self.shared_gate_up()
        self.gate_up(0)
        for i in range(1, outer + 1):
            if i < outer:
                self.take_dense(i)
                self.select(i)
            if i == 1:
                self.hidden(outer)
            self.hidden(i - 1)
            if i == 1:
                self.shared_down()
            if i < outer:
                self.gate_up(i)
            self.down_rows(i - 1)
        for i in range(outer):
            self.collect(i, i == outer - 1)
        self.finish()


def moe_scratch(n_sp, n_tp, inner, el, cap, tok, width, ff):
    outer, rw = n_sp // inner, el * cap
    chunk = inner * rw // n_tp
    chunk_s = tok // n_tp
    assert chunk == chunk_s
    vmem, dma = pltpu.VMEM, pltpu.SemaphoreType.DMA
    return {
        "wgu": vmem((el, width, 2 * ff), BF16),
        "wd": vmem((el, ff, width), BF16),
        "wsgu": vmem((width, 2 * ff), BF16),
        "wsd": vmem((ff, width), BF16),
        "dense": vmem((outer, tok, width), BF16),
        "picked": vmem((outer, inner, rw, width), BF16),
        "rows": vmem((outer, inner, rw, width), BF16),
        "meta": vmem((n_sp, 8, tok), F32),
        "inv": vmem((n_sp, 8, tok), F32),
        "ssq": vmem((n_tp, 8, tok), F32),
        "gu": vmem((outer + 1, n_tp, chunk, 2 * ff), BF16),
        "parts": vmem((outer + 1, n_tp, chunk, 2 * ff), BF16),
        "hid": vmem((outer + 1, n_tp, chunk, ff), BF16),
        "outs": vmem((outer, inner, rw, width), BF16),
        "ret": vmem((n_sp, rw, width), BF16),
        "back": vmem((outer, tok, inner * rw), BF16),
        "acc": vmem((tok, width), F32),
        "w_sem": dma((6,)),
        "meta_s": dma((n_sp,)),
        "meta_r": dma((n_sp,)),
        "inv_s": dma((n_sp,)),
        "inv_r": dma((n_sp,)),
        "ssq_s": dma((n_tp,)),
        "ssq_r": dma((n_tp,)),
        "dense_s": dma((outer, 2)),
        "dense_r": dma((outer,)),
        "x_s": dma((outer, inner)),
        "x_r": dma((outer, inner)),
        "part_s": dma((outer + 1, n_tp)),
        "part_r": dma((outer + 1, n_tp)),
        "hid_s": dma((outer + 1, n_tp)),
        "hid_r": dma((outer + 1, n_tp)),
        "ret_s": dma((outer, inner)),
        "ret_r": dma((n_sp,)),
    }


class Attend:
    def __init__(self, n_sp, n_tp, inner, refs):
        self.n_sp, self.n_tp, self.inner = n_sp, n_tp, inner
        self.outer = n_sp // inner
        self.__dict__.update(refs)
        self.own = lax.axis_index("sp")
        self.me = lax.axis_index("tp")
        self.z = self.own // inner
        self.x = self.own % inner
        self.order = plane_order(self.z, self.outer)
        self.heads, self.tok = self.bias.shape
        self.hd = self.queries.shape[1] // self.heads
        self.partner = self.me + 1 - 2 * (self.me % 2)
        self.peers = [(self.me + 2 * d) % n_tp for d in range(1, n_tp // 2)]

    def load(self):
        pairs = (
            (self.keys, self.kv),
            (self.values, self.vv),
            (self.queries, self.qv),
            (self.bias, self.bv),
        )
        self.loads = [
            pltpu.make_async_copy(src, dst, self.a_sem.at[i]) for i, (src, dst) in enumerate(pairs)
        ]
        for c in self.loads:
            c.start()

    def load_late(self):
        pairs = ((self.stream, self.sv), (self.out_proj, self.wo))
        self.late = [
            pltpu.make_async_copy(src, dst, self.a_sem.at[4 + i])
            for i, (src, dst) in enumerate(pairs)
        ]
        for c in self.late:
            c.start()

    def head_of(self, ref, head):
        return ref.at[:, pl.ds(pl.multiple_of(head * self.hd, self.hd), self.hd)]

    def exchange_copies(self, kind, i):
        src, dst = ((self.kv, self.kb), (self.vv, self.vb), (self.qv, self.qb))[kind]
        plane = self.order[i]
        target = dst.at[self.z, self.x] if kind < 2 else dst.at[self.z]
        return [
            rcopy(
                self.head_of(src, plane),
                target,
                self.e_s.at[kind, i],
                self.q_r.at[self.z] if kind == 2 else self.kv_r.at[kind, self.z, self.x],
                {"sp": plane * self.inner + self.x},
            )
        ]

    def side_copies(self, kind, i):
        dst = (self.kb, self.vb)[kind]
        plane = self.order[i]
        src = dst.at[plane, self.x] if i else self.head_of((self.kv, self.vv)[kind], self.z)
        return [
            rcopy(
                src,
                dst.at[plane, self.x],
                self.side_s.at[kind, i, d],
                self.kv_r.at[kind, plane, self.x],
                {"sp": self.z * self.inner + (self.x + d) % self.inner},
            )
            for d in range(1, self.inner)
        ]

    def wait_kv(self, kind, plane, x):
        dst = (self.kb, self.vb)[kind].at[plane, x]
        rcopy(
            dst, dst, self.e_s.at[kind, 0], self.kv_r.at[kind, plane, x], {"sp": (self.own + 1) % self.n_sp}
        ).wait_recv()

    def bias_copies(self):
        return [
            rcopy(
                self.bi.at[self.own],
                self.bi.at[self.own],
                self.bi_s.at[d],
                self.bi_r.at[self.own],
                {"sp": (self.own + d) % self.n_sp},
            )
            for d in range(1, self.n_sp)
        ]

    def exchange(self):
        for kind in range(3):
            self.loads[kind].wait()
            for i in range(self.outer - 1, 0, -1):
                for c in self.exchange_copies(kind, i):
                    c.start()
            if kind < 2:
                for c in self.side_copies(kind, 0):
                    c.start()
        self.loads[3].wait()
        self.bi[self.own, : self.heads, :] = self.bv[...].astype(F32)
        for c in self.bias_copies():
            c.start()
        self.kb[self.z, self.x] = self.head_of(self.kv, self.z)[...]
        self.vb[self.z, self.x] = self.head_of(self.vv, self.z)[...]
        self.qb[self.z] = self.head_of(self.qv, self.z)[...]

    def hand_over(self):
        for i in range(1, self.outer):
            for kind in range(2):
                self.wait_kv(kind, self.order[i], self.x)
                for c in self.side_copies(kind, i):
                    c.start()
        for d in range(1, self.n_sp):
            block = (self.own + d) % self.n_sp
            rcopy(
                self.bi.at[block],
                self.bi.at[block],
                self.bi_s.at[d],
                self.bi_r.at[block],
                {"sp": (self.own + 1) % self.n_sp},
            ).wait_recv()

    def compute(self):
        tok, hd = self.tok, self.hd
        scale = hd ** (-0.5)
        row = lax.broadcasted_iota(jnp.int32, (tok, tok), 0)
        col = lax.broadcasted_iota(jnp.int32, (tok, tok), 1)
        later = (row > col).astype(F32)
        sums = jnp.concatenate([later, jnp.ones((tok, tok), F32)], axis=1).astype(BF16)
        sums = jnp.concatenate([sums, sums], axis=0)
        for j in range(self.outer):
            for d in range(1, self.inner):
                for kind in range(2):
                    self.wait_kv(kind, j, (self.x + d) % self.inner)

            @pl.when(self.z != j)
            def _():
                rcopy(
                    self.qb.at[j], self.qb.at[j], self.e_s.at[2, 0], self.q_r.at[j], {"sp": (self.own + 1) % self.n_sp}
                ).wait_recv()

            q = self.qb[j]
            acc = jnp.zeros((tok, hd), F32)
            carry = jnp.zeros((tok, tok), F32)
            for k in range(j, -1, -1):
                for p in range(self.inner - 1, -1, -1):
                    bias = self.bi[k * self.inner + p, pl.ds(self.z, 1), :]
                    logit = rows_contract(q, self.kb[k, p]) * scale + bias
                    low = jnp.log(1.0 + jnp.exp(-jnp.abs(logit)))
                    fail = -(jnp.maximum(logit, 0.0) + low)
                    hit = jnp.minimum(logit, 0.0) - low
                    if k == j:
                        before = col < row + (self.x - p) * tok
                        fail = jnp.where(before, fail, 0.0)
                    high = fail.astype(BF16)
                    rest = (fail - high.astype(F32)).astype(BF16)
                    both = jnp.dot(
                        jnp.concatenate([high, rest], axis=1), sums, preferred_element_type=F32
                    )
                    w = jnp.exp(hit + both[:, :tok] + carry)
                    if k == j:
                        w = jnp.where(before, w, 0.0)
                    carry = carry + both[:, tok:]
                    acc = acc + jnp.dot(
                        w.astype(BF16), self.vb[k, p], preferred_element_type=F32
                    )
            self.ob[j] = acc.astype(BF16)

            @pl.when(self.z != j)
            def _():
                self.out_copy(j).start()

            @pl.when(self.z == j)
            def _():
                self.att[self.me, self.z] = self.ob[j]

    def out_copy(self, j):
        return rcopy(
            self.ob.at[j],
            self.att.at[self.me, self.z],
            self.o_s.at[j],
            self.att_r.at[self.me, self.z],
            {"sp": j * self.inner + self.x},
        )

    def wait_att(self, source, head):
        piece = self.att.at[source, head]
        rcopy(
            piece, piece, self.o_s.at[0], self.att_r.at[source, head], {"tp": (self.me + 1) % self.n_tp}
        ).wait_recv()

    def piece_copies(self, source, head, slot, targets):
        piece = self.att.at[source, head]
        return [
            rcopy(piece, piece, self.g_s.at[slot + n, head], self.att_r.at[source, head], {"tp": to})
            for n, to in enumerate(targets)
        ]

    def gather(self):
        wide = self.heads * self.hd

        def part(source):
            rows = jnp.concatenate([self.att[source, h] for h in range(self.outer)], axis=1)
            first = pl.multiple_of(source * wide, wide)
            return jnp.dot(rows, self.wo[pl.ds(first, wide), :], preferred_element_type=F32)

        slots = 1 + len(self.peers)
        for i in range(self.outer):
            head = self.order[i]
            if i:
                self.wait_att(self.me, head)
            for c in self.piece_copies(self.me, head, 0, self.peers + [self.partner]):
                c.start()
        for c in self.late:
            c.wait()
        self.acc[...] = self.sv[...].astype(F32) + part(self.me)
        for n, peer in enumerate(self.peers):
            for i in range(self.outer):
                self.wait_att(peer, self.order[i])
                for c in self.piece_copies(peer, self.order[i], slots + n, [self.partner]):
                    c.start()
        for i in range(self.outer):
            self.wait_att(self.partner, self.order[i])
        self.acc[...] += part(self.partner)
        for peer in self.peers:
            self.acc[...] += part(peer)
        others = [(self.partner + 2 * d) % self.n_tp for d in range(1, self.n_tp // 2)]
        for other in others:
            for i in range(self.outer):
                self.wait_att(other, self.order[i])
        total = self.acc[...]
        for other in others:
            total = total + part(other)
        self.mixed[...] = total.astype(BF16)

    def finish(self):
        groups = [self.bias_copies()]
        for i in range(1, self.outer):
            groups += [self.exchange_copies(kind, i) for kind in range(3)]
        for i in range(self.outer):
            groups += [self.side_copies(kind, i) for kind in range(2)]
            groups.append(
                self.piece_copies(self.me, self.order[i], 0, self.peers + [self.partner])
            )
            for n, peer in enumerate(self.peers):
                groups.append(
                    self.piece_copies(
                        peer, self.order[i], 1 + len(self.peers) + n, [self.partner]
                    )
                )
        for group in groups:
            for c in group:
                c.wait_send()
        for j in range(self.outer):

            @pl.when(self.z != j)
            def _():
                self.out_copy(j).wait_send()


LAYER_INPUTS = (
    "queries", "keys", "values", "bias", "stream", "out_proj", "gain_in", "ids_in", "wts_in",
    "gate", "up", "down", "s_gate", "s_up", "s_down",
)


def attend_scratch(n_sp, n_tp, inner, heads, hd, tok, width, top_k):
    outer = n_sp // inner
    vmem, dma = pltpu.VMEM, pltpu.SemaphoreType.DMA
    wide = heads * hd
    return {
        "qv": vmem((tok, wide), BF16),
        "kv": vmem((tok, wide), BF16),
        "vv": vmem((tok, wide), BF16),
        "bv": vmem((heads, tok), BF16),
        "sv": vmem((tok, width), BF16),
        "wo": vmem((n_tp * wide, width), BF16),
        "qb": vmem((outer, tok, hd), BF16),
        "kb": vmem((outer, inner, tok, hd), BF16),
        "vb": vmem((outer, inner, tok, hd), BF16),
        "bi": vmem((n_sp, 8, tok), F32),
        "ob": vmem((outer, tok, hd), BF16),
        "att": vmem((n_tp, outer, tok, hd), BF16),
        "mixed": vmem((tok, width), BF16),
        "gain": vmem((1, width), F32),
        "ids": vmem((top_k, tok), jnp.int32),
        "wts": vmem((top_k, tok), F32),
        "a_sem": dma((6,)),
        "s_sem": dma((3,)),
        "e_s": dma((3, outer)),
        "q_r": dma((outer,)),
        "kv_r": dma((2, outer, inner)),
        "side_s": dma((2, outer, inner)),
        "bi_s": dma((n_sp,)),
        "bi_r": dma((n_sp,)),
        "o_s": dma((outer,)),
        "att_r": dma((n_tp, outer)),
        "g_s": dma((n_tp, outer)),
    }


def layer_kernel(n_sp, n_tp, inner, el, cap, names, *refs):
    named = dict(zip(names, refs))
    first = Attend(n_sp, n_tp, inner, named)
    second = Experts(n_sp, n_tp, inner, el, cap, named)
    first.load()
    small = [
        pltpu.make_async_copy(named[name + "_in"], named[name], named["s_sem"].at[i])
        for i, name in enumerate(("ids", "wts", "gain"))
    ]
    for c in small:
        c.start()
    greet_all(n_sp, n_tp, first.own, first.me)
    first.exchange()
    first.load_late()
    second.load_weights()
    for c in small:
        c.wait()
    second.route()
    second.build_back()
    first.hand_over()
    first.compute()
    first.gather()
    second.run()
    first.finish()


def layer(operands, n_sp, n_tp, inner, cap, heads, hd):
    tok, width = operands[4].shape
    el, ff = operands[11].shape[:2]
    top_k = operands[7].shape[0]
    scratch = attend_scratch(n_sp, n_tp, inner, heads, hd, tok, width, top_k)
    scratch |= moe_scratch(n_sp, n_tp, inner, el, cap, tok, width, ff)
    hbm = pl.BlockSpec(memory_space=pltpu.MemorySpace.HBM)
    names = LAYER_INPUTS + ("out",) + tuple(scratch)
    return pl.pallas_call(
        functools.partial(layer_kernel, n_sp, n_tp, inner, el, cap, names),
        out_shape=jax.ShapeDtypeStruct((tok, width), BF16),
        in_specs=[hbm] * len(operands),
        out_specs=pl.BlockSpec(memory_space=pltpu.VMEM),
        scratch_shapes=list(scratch.values()),
        compiler_params=pltpu.CompilerParams(
            vmem_limit_bytes=56 * 2**20, collective_id=0, has_side_effects=True
        ),
        cost_estimate=pl.CostEstimate(flops=10**10, bytes_accessed=2**24, transcendentals=10**6),
    )(*operands)


def body(
    queries,
    key_rows,
    value_rows,
    break_bias,
    stream,
    out_proj,
    norm_gain,
    expert_ids,
    route_weights,
    gate_proj,
    up_proj,
    down_proj,
    shared_gate,
    shared_up,
    shared_down,
):
    tok = queries.shape[0]
    heads = break_bias.shape[1]
    hd = queries.shape[1] // heads
    n_sp = lax.axis_size("sp")
    n_tp = lax.axis_size("tp")
    width = stream.shape[1] * n_tp

    bias_wide = jnp.pad(break_bias, ((0, 0), (0, hd - heads)))

    experts_local = gate_proj.shape[0]
    experts = experts_local * n_sp
    top_k = expert_ids.shape[1]
    cap = 2 * top_k * tok // experts
    n_inner = max(d for d in range(1, n_sp + 1) if n_sp % d == 0 and d * d <= n_sp)
    plane_rows = n_inner * experts_local * cap
    if heads * n_inner == n_sp and plane_rows == tok and cap % 16 == 0 and tok % (16 * n_tp) == 0:
        operands = (
            queries, key_rows, value_rows, break_bias.T, stream, out_proj, norm_gain[None, :],
            expert_ids.T, route_weights.T, gate_proj, up_proj, down_proj,
            shared_gate, shared_up, shared_down,
        )
        return layer(operands, n_sp, n_tp, n_inner, cap, heads, hd)
    expert_of = jnp.arange(experts, dtype=jnp.int32)
    named = expert_ids[:, :, None] == expert_of[None, None, :]
    named_any = jnp.any(named, axis=1).astype(BF16)
    token = jnp.arange(tok, dtype=jnp.int32)
    earlier = (token[None, :] < token[:, None]).astype(BF16)
    rank_all = jnp.dot(earlier, named_any, preferred_element_type=F32)
    rank = jnp.sum(jnp.where(named, rank_all[:, None, :], 0.0), axis=2).astype(jnp.int32)
    slot = expert_ids * cap + rank
    slots = experts * cap
    place = jnp.arange(slots, dtype=jnp.int32)
    spot = slot[:, :, None] == place[None, None, :]
    send_pick = jnp.any(spot, axis=1).astype(BF16)
    back_pick = jnp.sum(jnp.where(spot, route_weights[:, :, None], 0.0), axis=1).astype(BF16)

    attended = attention(queries, key_rows, value_rows, bias_wide, heads, hd, n_sp)
    projected = jnp.dot(
        lax.all_gather(attended, "tp", axis=1, tiled=True), out_proj, preferred_element_type=F32
    )
    mixed = (stream.astype(F32) + projected).astype(BF16)
    mixed = lax.optimization_barrier(mixed)
    mixed_f = mixed.astype(F32)
    square_sum = lax.psum(jnp.sum(mixed_f * mixed_f, axis=1), "tp")
    inv_rms = lax.rsqrt(square_sum / width + EPS)
    normed = (mixed_f * inv_rms[:, None] * norm_gain[None, :]).astype(BF16)

    send = lax.dot_general(
        send_pick, normed, (((0,), (0,)), ((), ())), preferred_element_type=F32
    ).astype(BF16)
    send = send.reshape(n_sp, experts_local * cap, normed.shape[1])
    arrived = lax.all_to_all(send, "sp", split_axis=0, concat_axis=0, tiled=True)
    arrived = arrived.reshape(n_sp, experts_local, cap, -1)
    gates, ups = [], []
    for e in range(experts_local):
        rows = arrived[:, e].reshape(n_sp * cap, -1)
        gates.append(jnp.dot(rows, gate_proj[e], preferred_element_type=F32).astype(BF16))
        ups.append(jnp.dot(rows, up_proj[e], preferred_element_type=F32).astype(BF16))
    gates.append(jnp.dot(normed, shared_gate, preferred_element_type=F32).astype(BF16))
    ups.append(jnp.dot(normed, shared_up, preferred_element_type=F32).astype(BF16))
    gate_all = jnp.concatenate(gates, axis=0)
    up_all = jnp.concatenate(ups, axis=0)
    gate_up = jnp.concatenate([gate_all, up_all], axis=1)
    hidden = exchange(gate_up, n_tp)
    outs = []
    for e in range(experts_local):
        rows = hidden[e * n_sp * cap : (e + 1) * n_sp * cap]
        out = jnp.dot(rows, down_proj[e], preferred_element_type=F32).astype(BF16)
        outs.append(out.reshape(n_sp, 1, cap, -1))
    expert_out = jnp.concatenate(outs, axis=1).reshape(n_sp, experts_local * cap, -1)
    returned = lax.all_to_all(expert_out, "sp", split_axis=0, concat_axis=0, tiled=True)
    returned = returned.reshape(slots, -1)
    shared_out = jnp.dot(
        hidden[experts_local * n_sp * cap :], shared_down, preferred_element_type=F32
    )
    routed = jnp.dot(back_pick, returned, preferred_element_type=F32)
    return (mixed_f + shared_out + routed).astype(BF16)


def solution(mesh):
    in_specs = (
        P("sp", "tp"),
        P("sp", "tp"),
        P("sp", "tp"),
        P("sp", "tp"),
        P("sp", "tp"),
        P(None, "tp"),
        P("tp"),
        P("sp", None),
        P("sp", None),
        P("sp", "tp", None),
        P("sp", "tp", None),
        P("sp", None, "tp"),
        P("tp", None),
        P("tp", None),
        P(None, "tp"),
    )
    return jax.shard_map(body, mesh=mesh, in_specs=in_specs, out_specs=P("sp", "tp"), check_vma=False)
```

```python
import functools

import jax
import jax.numpy as jnp
from jax import lax
from jax.experimental import pallas as pl
from jax.experimental.pallas import tpu as pltpu
from jax.sharding import PartitionSpec as P

EPS = 1e-06
F32 = jnp.float32
BF16 = jnp.bfloat16


def attention_kernel(
    heads, hd, n_sp, inner, q_ref, k_ref, v_ref, b_ref, o_ref, kbuf, vbuf, bbuf, acc, carry, send_sem, recv_sem
):
    tok = q_ref.shape[0]
    own = lax.axis_index("sp")
    outer = n_sp // inner
    z_own = own // inner
    x_own = own % inner
    above = z_own < outer - 1
    below = z_own > 0

    barrier = pltpu.get_barrier_semaphore()

    def greet(target):
        pl.semaphore_signal(
            barrier, inc=1, device_id={"sp": target}, device_id_type=pl.DeviceIdType.MESH
        )

    @pl.when(above)
    def _():
        greet(own + inner)

    @pl.when(below)
    def _():
        greet(own - inner)

    for d in range(1, inner):
        greet(z_own * inner + (x_own + d) % inner)
    pl.semaphore_wait(barrier, inner - 1 + above.astype(jnp.int32) + below.astype(jnp.int32))

    def copies(sources, block, z_block, lane, target):
        return [
            pltpu.make_async_remote_copy(
                src_ref=src,
                dst_ref=dst.at[block],
                send_sem=send_sem.at[kind, z_block, lane],
                recv_sem=recv_sem.at[kind, block],
                device_id={"sp": target},
                device_id_type=pl.DeviceIdType.MESH,
            )
            for kind, (src, dst) in enumerate(zip(sources, (kbuf, vbuf, bbuf)))
        ]

    def held(block):
        return (kbuf.at[block], vbuf.at[block], bbuf.at[block])

    def start_all(group):
        for c in group:
            c.start()

    def wait_sent(group):
        for c in group:
            c.wait_send()

    def wait_arrived(block):
        for c in copies(held(block), block, 0, 0, (own + 1) % n_sp):
            c.wait_recv()

    def own_sends(act):
        mine = (k_ref, v_ref, b_ref)

        @pl.when(above)
        def _():
            act(copies(mine, own, z_own, 0, own + inner))

        for d in range(1, inner):
            x_to = (x_own + d) % inner

            @pl.when(x_to > x_own)
            def _():
                act(copies(mine, own, z_own, d, z_own * inner + x_to))

    def relays(z_block, act):
        block = z_block * inner + x_own

        @pl.when(above)
        def _():
            act(copies(held(block), block, z_block, 0, own + inner))

        for d in range(1, inner):
            act(copies(held(block), block, z_block, d, z_own * inner + (x_own + d) % inner))

    own_sends(start_all)

    scale = hd ** (-0.5)
    row = lax.broadcasted_iota(jnp.int32, (tok, tok), 0)
    col = lax.broadcasted_iota(jnp.int32, (tok, tok), 1)
    later = (row > col).astype(F32)
    sums = jnp.concatenate([later, jnp.ones((tok, tok), F32)], axis=1).astype(BF16)
    sums = jnp.concatenate([sums, sums], axis=0)
    pick_rows = max(16, heads)
    pick = (
        lax.broadcasted_iota(jnp.int32, (pick_rows, hd), 0)
        == lax.broadcasted_iota(jnp.int32, (pick_rows, hd), 1)
    ).astype(F32).astype(BF16)
    acc[...] = jnp.zeros_like(acc)
    carry[...] = jnp.zeros_like(carry)

    def compute(keys, values, offsets, diagonal):
        bias = lax.dot_general(
            pick, offsets[...], (((1,), (1,)), ((), ())), preferred_element_type=F32
        )
        for h in range(heads):
            cols = slice(h * hd, (h + 1) * hd)
            z = lax.dot_general(
                q_ref[:, cols], keys[:, cols], (((1,), (1,)), ((), ())), preferred_element_type=F32
            )
            z = z * scale + bias[h : h + 1, :]
            low = jnp.log1p(jnp.exp(-jnp.abs(z)))
            fail = -(jnp.maximum(z, 0.0) + low)
            hit = jnp.minimum(z, 0.0) - low
            if diagonal:
                before = col < row
                fail = jnp.where(before, fail, 0.0)
            high = fail.astype(BF16)
            rest = (fail - high.astype(F32)).astype(BF16)
            both = jnp.dot(
                jnp.concatenate([high, rest], axis=1), sums, preferred_element_type=F32
            )
            before_sum = carry[h]
            w = jnp.exp(hit + both[:, :tok] + before_sum)
            if diagonal:
                w = jnp.where(before, w, 0.0)
            carry[h] = before_sum + both[:, tok:]
            acc[:, cols] += jnp.dot(w.astype(BF16), values[:, cols], preferred_element_type=F32)

    compute(k_ref, v_ref, b_ref, True)

    def group(i, _):
        z_block = z_own - i

        @pl.when(z_block > 0)
        def _():
            wait_arrived((z_block - 1) * inner + x_own)
            relays(z_block - 1, start_all)

        def member(m, _):
            x_block = inner - 1 - m
            block = z_block * inner + x_block

            @pl.when(block < own)
            def _():
                @pl.when(x_block != x_own)
                def _():
                    wait_arrived(block)

                compute(*held(block), False)

            return 0

        lax.fori_loop(0, inner, member, 0)
        return 0

    lax.fori_loop(0, z_own + 1, group, 0)
    o_ref[...] = acc[...].astype(BF16)

    own_sends(wait_sent)

    def drain(z_block, _):
        relays(z_block, wait_sent)
        return 0

    lax.fori_loop(0, z_own, drain, 0)


def attention(queries, keys, values, bias, heads, hd, n_sp):
    tok = queries.shape[0]
    inner = max(d for d in range(1, n_sp + 1) if n_sp % d == 0 and d * d <= n_sp)
    vmem = pl.BlockSpec(memory_space=pltpu.VMEM)
    return pl.pallas_call(
        functools.partial(attention_kernel, heads, hd, n_sp, inner),
        out_shape=jax.ShapeDtypeStruct((tok, heads * hd), BF16),
        in_specs=[vmem] * 4,
        out_specs=vmem,
        scratch_shapes=[
            pltpu.VMEM((n_sp, tok, heads * hd), BF16),
            pltpu.VMEM((n_sp, tok, heads * hd), BF16),
            pltpu.VMEM((n_sp, tok, hd), BF16),
            pltpu.VMEM((tok, heads * hd), F32),
            pltpu.VMEM((heads, tok, tok), F32),
            pltpu.SemaphoreType.DMA((3, n_sp // inner, inner)),
            pltpu.SemaphoreType.DMA((3, n_sp)),
        ],
        compiler_params=pltpu.CompilerParams(
            vmem_limit_bytes=40 * 2**20, collective_id=0, has_side_effects=True
        ),
        cost_estimate=pl.CostEstimate(flops=2 * 10**9, bytes_accessed=2**22, transcendentals=10**6),
    )(queries, keys, values, bias)


def exchange_kernel(n_tp, gu_ref, o_ref, parts, mine, spread, send_parts, recv_parts, send_rows, recv_rows):
    width = gu_ref.shape[2] // 2
    me = lax.axis_index("tp")
    barrier = pltpu.get_barrier_semaphore()
    others = [(me + d) % n_tp for d in range(1, n_tp)]
    for to in others:
        pl.semaphore_signal(
            barrier, inc=1, device_id={"tp": to}, device_id_type=pl.DeviceIdType.MESH
        )
    pl.semaphore_wait(barrier, n_tp - 1)
    first, second = [], []
    for d, to in enumerate(others):
        copy = pltpu.make_async_remote_copy(
            src_ref=gu_ref.at[to],
            dst_ref=parts.at[d],
            send_sem=send_parts.at[d],
            recv_sem=recv_parts.at[d],
            device_id={"tp": to},
            device_id_type=pl.DeviceIdType.MESH,
        )
        copy.start()
        first.append(copy)
    total = gu_ref[me].astype(F32)
    for d, copy in enumerate(first):
        copy.wait_recv()
        total = total + parts[d].astype(F32)
    gate = total[:, :width]
    mine[...] = (jax.nn.silu(gate) * total[:, width:]).astype(BF16)
    for d, to in enumerate(others):
        copy = pltpu.make_async_remote_copy(
            src_ref=mine,
            dst_ref=spread.at[d],
            send_sem=send_rows.at[d],
            recv_sem=recv_rows.at[d],
            device_id={"tp": to},
            device_id_type=pl.DeviceIdType.MESH,
        )
        copy.start()
        second.append(copy)
    o_ref[me] = mine[...]
    for d, copy in enumerate(second):
        copy.wait_recv()
        o_ref[(me + n_tp - 1 - d) % n_tp] = spread[d]
    for copy in first + second:
        copy.wait_send()


def exchange(gate_up, n_tp):
    rows, width = gate_up.shape[0] // n_tp, gate_up.shape[1] // 2
    vmem = pl.BlockSpec(memory_space=pltpu.VMEM)
    dma = pltpu.SemaphoreType.DMA((n_tp - 1,))
    hidden = pl.pallas_call(
        functools.partial(exchange_kernel, n_tp),
        out_shape=jax.ShapeDtypeStruct((n_tp, rows, width), BF16),
        in_specs=[vmem],
        out_specs=vmem,
        scratch_shapes=[
            pltpu.VMEM((n_tp - 1, rows, 2 * width), BF16),
            pltpu.VMEM((rows, width), BF16),
            pltpu.VMEM((n_tp - 1, rows, width), BF16),
            dma,
            dma,
            dma,
            dma,
        ],
        compiler_params=pltpu.CompilerParams(
            vmem_limit_bytes=24 * 2**20, collective_id=1, has_side_effects=True
        ),
        cost_estimate=pl.CostEstimate(flops=10**8, bytes_accessed=2**21, transcendentals=10**5),
    )(gate_up.reshape(n_tp, rows, 2 * width))
    return hidden.reshape(n_tp * rows, width)


MESH = pl.DeviceIdType.MESH


def rows_contract(lhs, rhs):
    return lax.dot_general(lhs, rhs, (((1,), (1,)), ((), ())), preferred_element_type=F32)


def rcopy(src, dst, send_sem, recv_sem, where):
    return pltpu.make_async_remote_copy(
        src_ref=src,
        dst_ref=dst,
        send_sem=send_sem,
        recv_sem=recv_sem,
        device_id=where,
        device_id_type=MESH,
    )


def plane_order(z, outer):
    step = 1 - 2 * ((2 * z) // outer)
    return [(z + step * i + outer) % outer for i in range(outer)]


def greet_all(n_sp, n_tp, own, me):
    barrier = pltpu.get_barrier_semaphore()
    for d in range(1, n_sp):
        pl.semaphore_signal(
            barrier, inc=1, device_id={"sp": (own + d) % n_sp}, device_id_type=MESH
        )
    for d in range(1, n_tp):
        pl.semaphore_signal(
            barrier, inc=1, device_id={"tp": (me + d) % n_tp}, device_id_type=MESH
        )


def await_all(n_sp, n_tp):
    pl.semaphore_wait(pltpu.get_barrier_semaphore(), n_sp + n_tp - 2)


class Experts:
    def __init__(self, n_sp, n_tp, inner, experts_local, cap, refs):
        self.n_sp, self.n_tp, self.inner = n_sp, n_tp, inner
        self.outer = n_sp // inner
        self.el, self.cap = experts_local, cap
        self.rw = experts_local * cap
        self.__dict__.update(refs)
        self.own = lax.axis_index("sp")
        self.me = lax.axis_index("tp")
        self.z = self.own // inner
        self.x = self.own % inner
        self.order = plane_order(self.z, self.outer)
        self.side = self.z // 2
        self.within = self.z % 2
        self.mate = self.z + 1 - 2 * self.within
        self.middle = 1 + self.side
        self.between = (self.z > 0) & (self.z < self.outer - 1)
        self.at_end = jnp.logical_not(self.between)
        self.tok, self.width = self.mixed.shape
        self.ff = self.down.shape[1]
        self.total_width = self.width * n_tp

    def load_weights(self):
        ff = self.ff
        self.loads = [
            pltpu.make_async_copy(src, dst, self.w_sem.at[i])
            for i, (src, dst) in enumerate(
                (
                    (self.s_gate, self.wsgu.at[:, pl.ds(0, ff)]),
                    (self.s_up, self.wsgu.at[:, pl.ds(ff, ff)]),
                    (self.gate, self.wgu.at[:, :, pl.ds(0, ff)]),
                    (self.up, self.wgu.at[:, :, pl.ds(ff, ff)]),
                    (self.down, self.wd),
                    (self.s_down, self.wsd),
                )
            )
        ]
        for load in self.loads:
            load.start()

    def meta_copies(self, ref, send, recv):
        return [
            rcopy(
                ref.at[self.own],
                ref.at[self.own],
                send.at[d],
                recv.at[self.own],
                {"sp": (self.own + d) % self.n_sp},
            )
            for d in range(1, self.n_sp)
        ]

    def wait_table(self, ref, send, recv, block):
        rcopy(
            ref.at[block], ref.at[block], send.at[0], recv.at[block], {"sp": (self.own + 1) % self.n_sp}
        ).wait_recv()

    def route(self):
        ids = self.ids[...]
        experts = self.el * self.n_sp
        top_k, tok = ids.shape
        expert_of = lax.broadcasted_iota(jnp.int32, (experts, tok), 0)
        named = [ids[k : k + 1, :] == expert_of for k in range(top_k)]
        named_any = functools.reduce(jnp.logical_or, named).astype(F32).astype(BF16)
        before = (
            lax.broadcasted_iota(jnp.int32, (tok, tok), 0)
            < lax.broadcasted_iota(jnp.int32, (tok, tok), 1)
        ).astype(F32).astype(BF16)
        rank = jnp.dot(named_any, before, preferred_element_type=F32)
        self.meta[self.own] = jnp.zeros((8, tok), F32)
        for k in range(top_k):
            mine = jnp.sum(jnp.where(named[k], rank, 0.0), axis=0, keepdims=True)
            slot = ids[k : k + 1, :].astype(F32) * self.cap + mine
            self.meta[self.own, k : k + 1, :] = slot
            self.meta[self.own, top_k + k : top_k + k + 1, :] = self.wts[k : k + 1, :]
        self.top_k = top_k

    def send_route(self):
        self.meta_group = self.meta_copies(self.meta, self.meta_s, self.meta_r)
        for c in self.meta_group:
            c.start()

    def slot_hits(self, block, first, count):
        spot = (
            lax.broadcasted_iota(jnp.int32, (count, self.tok), 0) + first
        ).astype(F32)
        return [self.meta[block, k : k + 1, :] == spot for k in range(self.top_k)]

    def back_of(self, block, plane):
        rows = self.inner * self.rw
        hits = self.slot_hits(block, plane * rows, rows)
        weight = sum(
            jnp.where(
                hits[k], self.meta[block, self.top_k + k : self.top_k + k + 1, :], 0.0
            )
            for k in range(self.top_k)
        )
        return jnp.transpose(weight).astype(BF16)

    def build_back(self):
        self.back[0] = self.back_of(self.own, self.z)
        self.back[1] = self.back_of(self.own, self.mate)

    def dense_copy(self, src, plane, step):
        return rcopy(
            src,
            self.dense.at[plane],
            self.dense_s.at[plane, (step + 1) // 2],
            self.dense_r.at[plane],
            {"sp": (self.z + step) * self.inner + self.x},
        )

    def spread_own(self, act):
        for step in (1, -1):

            @pl.when(self.z < self.outer - 1 if step == 1 else self.z > 0)
            def _():
                act(self.dense_copy(self.mixed, self.z, step))

    def hand_on(self, plane, act):
        @pl.when((plane < self.z) & (self.z < self.outer - 1))
        def _():
            act(self.dense_copy(self.dense.at[plane], plane, 1))

        @pl.when((plane > self.z) & (self.z > 0))
        def _():
            act(self.dense_copy(self.dense.at[plane], plane, -1))

    def receive(self, plane):
        rcopy(
            self.dense.at[plane],
            self.dense.at[plane],
            self.dense_s.at[plane, 0],
            self.dense_r.at[plane],
            {"sp": (self.own + 1) % self.n_sp},
        ).wait_recv()
        self.hand_on(plane, lambda c: c.start())

    def take_dense(self, i):
        last = self.outer - 1
        if i == last:

            @pl.when(self.at_end)
            def _():
                self.receive(self.order[i])

            return
        self.receive(self.order[i])
        if i == 1:

            @pl.when(self.between)
            def _():
                self.receive(self.order[last])

    def cross_copies(self, i):
        return [
            rcopy(
                self.picked.at[i, (self.x + d) % self.inner],
                self.rows.at[i, self.x],
                self.x_s.at[i, d],
                self.x_r.at[i, self.x],
                {"sp": self.z * self.inner + (self.x + d) % self.inner},
            )
            for d in range(1, self.inner)
        ]

    def select(self, i):
        block = self.order[i] * self.inner + self.x
        if i:
            self.wait_table(self.meta, self.meta_s, self.meta_r, block)
        rows = self.inner * self.rw
        hits = self.slot_hits(block, self.z * rows, rows)
        pick = functools.reduce(jnp.logical_or, hits).astype(F32).astype(BF16)
        source = self.dense[self.order[i]] if i else self.mixed[...]
        got = jnp.dot(pick, source, preferred_element_type=F32).astype(BF16)
        for p in range(self.inner):
            self.picked[i, p] = got[p * self.rw : (p + 1) * self.rw]
        for c in self.cross_copies(i):
            c.start()
        self.rows[i, self.x] = self.picked[i, self.x]

    def tp_copies(self, src, dst, send, recv):
        return [
            rcopy(src(to), dst, send.at[d], recv.at[self.me], {"tp": to})
            for d, to in ((d, (self.me + d) % self.n_tp) for d in range(1, self.n_tp))
        ]

    def tp_wait(self, dst, send, recv):
        for d in range(1, self.n_tp):
            other = (self.me + d) % self.n_tp
            rcopy(
                dst(other), dst(other), send.at[0], recv.at[other], {"tp": (self.me + 1) % self.n_tp}
            ).wait_recv()

    def send_squares(self):
        wide = self.mixed[...].astype(F32)
        column = jnp.sum(wide * wide, axis=1, keepdims=True)
        row = jnp.transpose(jnp.broadcast_to(column, (self.tok, self.tok)))
        self.ssq[self.me] = row[:8]
        self.ssq_group = self.tp_copies(
            lambda to: self.ssq.at[self.me], self.ssq.at[self.me], self.ssq_s, self.ssq_r
        )
        for c in self.ssq_group:
            c.start()

    def send_scales(self):
        self.tp_wait(lambda other: self.ssq.at[other], self.ssq_s, self.ssq_r)
        total = self.ssq[0]
        for p in range(1, self.n_tp):
            total = total + self.ssq[p]
        self.inv[self.own] = lax.rsqrt(total / self.total_width + EPS)
        self.inv_group = self.meta_copies(self.inv, self.inv_s, self.inv_r)
        for c in self.inv_group:
            c.start()

    def send_parts(self, s, value):
        chunk = value.shape[0] // self.n_tp
        for p in range(self.n_tp):
            self.gu[s, p] = value[p * chunk : (p + 1) * chunk]
        group = self.tp_copies(
            lambda to: self.gu.at[s, to], self.parts.at[s, self.me], self.part_s.at[s], self.part_r.at[s]
        )
        for c in group:
            c.start()
        self.part_groups[s] = group

    def gate_up(self, i):
        if i == 0:
            self.loads[2].wait()
            self.loads[3].wait()
        for d in range(1, self.inner):
            x_from = (self.x + d) % self.inner
            rcopy(
                self.rows.at[i, x_from],
                self.rows.at[i, x_from],
                self.x_s.at[i, d],
                self.x_r.at[i, x_from],
                {"sp": (self.own + 1) % self.n_sp},
            ).wait_recv()
        normed = []
        for d in range(self.inner):
            block = self.order[i] * self.inner + (self.x + d) % self.inner
            if d:
                self.wait_table(self.meta, self.meta_s, self.meta_r, block)
            if i or d:
                self.wait_table(self.inv, self.inv_s, self.inv_r, block)
        for p in range(self.inner):
            block = self.order[i] * self.inner + p
            hits = self.slot_hits(block, self.own * self.rw, self.rw)
            pick = functools.reduce(jnp.logical_or, hits)
            scale = jnp.sum(
                jnp.where(pick, self.inv[block, 0:1, :], 0.0), axis=1, keepdims=True
            )
            wide = self.rows[i, p].astype(F32)
            normed.append((wide * scale * self.gain[...]).astype(BF16))
        out = []
        for e in range(self.el):
            rows = jnp.concatenate(
                [n[e * self.cap : (e + 1) * self.cap] for n in normed], axis=0
            )
            out.append(jnp.dot(rows, self.wgu[e], preferred_element_type=F32).astype(BF16))
        self.send_parts(i, jnp.concatenate(out, axis=0))

    def shared_gate_up(self):
        self.loads[0].wait()
        self.loads[1].wait()
        scale = jnp.transpose(jnp.broadcast_to(self.inv[self.own, 0:1, :], (self.tok, self.tok)))
        normed = (
            self.mixed[...].astype(F32) * scale[:, 0:1] * self.gain[...]
        ).astype(BF16)
        value = jnp.dot(normed, self.wsgu[...], preferred_element_type=F32).astype(BF16)
        self.send_parts(self.outer, value)

    def hidden(self, s):
        self.tp_wait(lambda other: self.parts.at[s, other], self.part_s.at[s], self.part_r.at[s])
        total = self.gu[s, self.me].astype(F32)
        for d in range(1, self.n_tp):
            total = total + self.parts[s, (self.me + d) % self.n_tp].astype(F32)
        act = jax.nn.silu(total[:, : self.ff]) * total[:, self.ff :]
        self.hid[s, self.me] = act.astype(BF16)
        group = self.tp_copies(
            lambda to: self.hid.at[s, self.me], self.hid.at[s, self.me], self.hid_s.at[s], self.hid_r.at[s]
        )
        for c in group:
            c.start()
        self.hid_groups[s] = group

    def all_hidden(self, s):
        self.tp_wait(lambda other: self.hid.at[s, other], self.hid_s.at[s], self.hid_r.at[s])
        return jnp.concatenate([self.hid[s, p] for p in range(self.n_tp)], axis=0)

    def return_copies(self, i):
        return [
            rcopy(
                self.outs.at[i, (self.x + d) % self.inner],
                self.ret.at[self.own],
                self.ret_s.at[i, d],
                self.ret_r.at[self.own],
                {"sp": self.order[i] * self.inner + (self.x + d) % self.inner},
            )
            for d in range(0 if i else 1, self.inner)
        ]

    def halves(self):
        half = self.width // 2
        return [pl.ds(h * half, half) for h in range(2)]

    def over_copies(self, i, c, first):
        return [
            rcopy(
                self.outs.at[i, (self.x + d) % self.inner, :, cols],
                self.over.at[c, self.within, self.x, :, cols],
                self.over_s.at[i, d, h],
                self.over_r.at[c, self.within, self.x, h],
                {"sp": self.middle * self.inner + (self.x + d) % self.inner},
            )
            for h, cols in enumerate(self.halves())
            for d in range(first, self.inner)
        ]

    def each_return(self, i, act):
        if i == 0:
            act(self.return_copies(0))
            return

        @pl.when(self.at_end)
        def _():
            act(self.over_copies(i, i - 2, 0) if i > 1 else self.return_copies(i))

        @pl.when(self.between)
        def _():
            act(self.over_copies(i, i - 1, 1) if i < 3 else self.return_copies(i))

    def sum_copy(self, c, h):
        cols = self.halves()[h]
        return rcopy(
            self.sums.at[c, :, cols],
            self.far.at[:, cols],
            self.sum_s.at[c, h],
            self.far_r.at[h],
            {"sp": self.order[c + 1] * self.inner + self.x},
        )

    def add_over(self, c):
        block = self.order[c + 1] * self.inner + self.x
        pair = 2 * self.side
        backs = [self.back_of(block, pair + s) for s in range(2)]
        for h, cols in enumerate(self.halves()):

            def arrived(s, x_from):
                piece = self.over.at[c, s, x_from, :, cols]
                rcopy(
                    piece,
                    piece,
                    self.over_s.at[0, 0, h],
                    self.over_r.at[c, s, x_from, h],
                    {"sp": (self.own + 1) % self.n_sp},
                ).wait_recv()

            total = 0.0
            for s in range(2):
                for d in range(1, self.inner):
                    arrived(s, (self.x + d) % self.inner)

                @pl.when(self.within != s)
                def _():
                    arrived(s, self.x)

                rows = jnp.concatenate(
                    [self.over[c, s, p, :, cols] for p in range(self.inner)], axis=0
                )
                total = total + jnp.dot(backs[s], rows, preferred_element_type=F32)
            self.sums[c, :, cols] = total.astype(BF16)
            self.sum_copy(c, h).start()

    def down_rows(self, i):
        if i == 0:
            self.loads[4].wait()
        hidden = self.all_hidden(i)
        span = self.inner * self.cap
        for e in range(self.el):
            out = jnp.dot(
                hidden[e * span : (e + 1) * span], self.wd[e], preferred_element_type=F32
            ).astype(BF16)
            for p in range(self.inner):
                self.outs[i, p, e * self.cap : (e + 1) * self.cap, :] = out[
                    p * self.cap : (p + 1) * self.cap
                ]

        def start(group):
            for c in group:
                c.start()

        self.each_return(i, start)
        if i == 0:
            self.ret[self.own] = self.outs[0, self.x]
        elif i < 3:

            @pl.when(self.between)
            def _():
                self.over[i - 1, self.within, self.x] = self.outs[i, self.x]

    def shared_down(self):
        self.loads[5].wait()
        shared = jnp.dot(
            self.all_hidden(self.outer), self.wsd[...], preferred_element_type=F32
        )
        self.acc[...] = self.mixed[...].astype(F32) + shared

    def collect(self, n):
        plane = (self.z, self.mate)[n]
        for d in range(1 - n, self.inner):
            block = plane * self.inner + (self.x + d) % self.inner
            rcopy(
                self.ret.at[block],
                self.ret.at[block],
                self.ret_s.at[n, d],
                self.ret_r.at[block],
                {"sp": (self.own + 1) % self.n_sp},
            ).wait_recv()
        rows = jnp.concatenate(
            [self.ret[plane * self.inner + p] for p in range(self.inner)], axis=0
        )
        self.acc[...] += jnp.dot(self.back[n], rows, preferred_element_type=F32)

    def close(self):
        for h, cols in enumerate(self.halves()):
            piece = self.far.at[:, cols]
            rcopy(
                piece, piece, self.sum_s.at[0, h], self.far_r.at[h], {"sp": (self.own + 1) % self.n_sp}
            ).wait_recv()
            self.out[:, cols] = (self.acc[:, cols] + self.far[:, cols].astype(F32)).astype(BF16)

    def finish(self):
        def sent(c):
            c.wait_send()

        self.spread_own(sent)
        for i in range(1, self.outer):
            self.hand_on(self.order[i], sent)
        groups = [self.meta_group, self.inv_group, self.ssq_group]
        groups += list(self.part_groups.values()) + list(self.hid_groups.values())
        groups += [self.cross_copies(i) for i in range(self.outer)]
        for group in groups:
            for c in group:
                c.wait_send()

        def all_sent(group):
            for c in group:
                c.wait_send()

        for i in range(self.outer):
            self.each_return(i, all_sent)

        @pl.when(self.between)
        def _():
            for c in range(2):
                for h in range(2):
                    self.sum_copy(c, h).wait_send()

    def run(self):
        outer = self.outer
        self.part_groups, self.hid_groups = {}, {}
        self.spread_own(lambda c: c.start())
        self.send_squares()
        self.select(0)
        self.send_scales()
        self.shared_gate_up()
        self.gate_up(0)
        for i in range(1, outer + 2):
            if i < outer:
                self.take_dense(i)
                self.select(i)
            if i > 1:
                self.down_rows(i - 2)
            if i == 1:
                self.hidden(outer)
            if i <= outer:
                self.hidden(i - 1)
            if i == 1:
                self.shared_down()
            if i < outer:
                self.gate_up(i)
        self.collect(0)

        @pl.when(self.between)
        def _():
            for c in range(2):
                self.add_over(c)

        self.collect(1)
        self.close()
        self.finish()


def moe_scratch(n_sp, n_tp, inner, el, cap, tok, width, ff):
    outer, rw = n_sp // inner, el * cap
    chunk = inner * rw // n_tp
    chunk_s = tok // n_tp
    assert chunk == chunk_s
    vmem, dma = pltpu.VMEM, pltpu.SemaphoreType.DMA
    return {
        "wgu": vmem((el, width, 2 * ff), BF16),
        "wd": vmem((el, ff, width), BF16),
        "wsgu": vmem((width, 2 * ff), BF16),
        "wsd": vmem((ff, width), BF16),
        "dense": vmem((outer, tok, width), BF16),
        "picked": vmem((outer, inner, rw, width), BF16),
        "rows": vmem((outer, inner, rw, width), BF16),
        "meta": vmem((n_sp, 8, tok), F32),
        "inv": vmem((n_sp, 8, tok), F32),
        "ssq": vmem((n_tp, 8, tok), F32),
        "gu": vmem((outer + 1, n_tp, chunk, 2 * ff), BF16),
        "parts": vmem((outer + 1, n_tp, chunk, 2 * ff), BF16),
        "hid": vmem((outer + 1, n_tp, chunk, ff), BF16),
        "outs": vmem((outer, inner, rw, width), BF16),
        "ret": vmem((n_sp, rw, width), BF16),
        "back": vmem((2, tok, inner * rw), BF16),
        "over": vmem((2, 2, inner, rw, width), BF16),
        "sums": vmem((2, tok, width), BF16),
        "far": vmem((tok, width), BF16),
        "acc": vmem((tok, width), F32),
        "w_sem": dma((6,)),
        "meta_s": dma((n_sp,)),
        "meta_r": dma((n_sp,)),
        "inv_s": dma((n_sp,)),
        "inv_r": dma((n_sp,)),
        "ssq_s": dma((n_tp,)),
        "ssq_r": dma((n_tp,)),
        "dense_s": dma((outer, 2)),
        "dense_r": dma((outer,)),
        "x_s": dma((outer, inner)),
        "x_r": dma((outer, inner)),
        "part_s": dma((outer + 1, n_tp)),
        "part_r": dma((outer + 1, n_tp)),
        "hid_s": dma((outer + 1, n_tp)),
        "hid_r": dma((outer + 1, n_tp)),
        "ret_s": dma((outer, inner)),
        "ret_r": dma((n_sp,)),
        "over_s": dma((outer, inner, 2)),
        "over_r": dma((2, 2, inner, 2)),
        "sum_s": dma((2, 2)),
        "far_r": dma((2,)),
    }


class Attend:
    def __init__(self, n_sp, n_tp, inner, refs):
        self.n_sp, self.n_tp, self.inner = n_sp, n_tp, inner
        self.outer = n_sp // inner
        self.__dict__.update(refs)
        self.own = lax.axis_index("sp")
        self.me = lax.axis_index("tp")
        self.z = self.own // inner
        self.x = self.own % inner
        self.order = plane_order(self.z, self.outer)
        self.heads, self.tok = self.bias.shape
        self.hd = self.queries.shape[1] // self.heads
        self.partner = self.me + 1 - 2 * (self.me % 2)
        self.peers = [(self.me + 2 * d) % n_tp for d in range(1, n_tp // 2)]

    def load(self):
        pairs = (
            (self.keys, self.kv),
            (self.values, self.vv),
            (self.queries, self.qv),
            (self.bias, self.bv),
        )
        self.loads = [
            pltpu.make_async_copy(src, dst, self.a_sem.at[i]) for i, (src, dst) in enumerate(pairs)
        ]
        for c in self.loads:
            c.start()

    def load_late(self):
        pairs = ((self.stream, self.sv), (self.out_proj, self.wo))
        self.late = [
            pltpu.make_async_copy(src, dst, self.a_sem.at[4 + i])
            for i, (src, dst) in enumerate(pairs)
        ]
        for c in self.late:
            c.start()

    def head_of(self, ref, head):
        return ref.at[:, pl.ds(pl.multiple_of(head * self.hd, self.hd), self.hd)]

    def exchange_copies(self, kind, i):
        src, dst = ((self.kv, self.kb), (self.vv, self.vb), (self.qv, self.qb))[kind]
        plane = self.order[i]
        target = dst.at[self.z, self.x] if kind < 2 else dst.at[self.z]
        return [
            rcopy(
                self.head_of(src, plane),
                target,
                self.e_s.at[kind, i],
                self.q_r.at[self.z] if kind == 2 else self.kv_r.at[kind, self.z, self.x],
                {"sp": plane * self.inner + self.x},
            )
        ]

    def side_copies(self, kind, i):
        dst = (self.kb, self.vb)[kind]
        plane = self.order[i]
        src = dst.at[plane, self.x] if i else self.head_of((self.kv, self.vv)[kind], self.z)
        return [
            rcopy(
                src,
                dst.at[plane, self.x],
                self.side_s.at[kind, i, d],
                self.kv_r.at[kind, plane, self.x],
                {"sp": self.z * self.inner + (self.x + d) % self.inner},
            )
            for d in range(1, self.inner)
        ]

    def wait_kv(self, kind, plane, x):
        dst = (self.kb, self.vb)[kind].at[plane, x]
        rcopy(
            dst, dst, self.e_s.at[kind, 0], self.kv_r.at[kind, plane, x], {"sp": (self.own + 1) % self.n_sp}
        ).wait_recv()

    def bias_copies(self):
        return [
            rcopy(
                self.bi.at[self.own],
                self.bi.at[self.own],
                self.bi_s.at[d],
                self.bi_r.at[self.own],
                {"sp": (self.own + d) % self.n_sp},
            )
            for d in range(1, self.n_sp)
        ]

    def exchange(self):
        for kind in range(3):
            self.loads[kind].wait()
            for i in range(self.outer - 1, 0, -1):
                for c in self.exchange_copies(kind, i):
                    c.start()
            if kind < 2:
                for c in self.side_copies(kind, 0):
                    c.start()
        self.loads[3].wait()
        self.bi[self.own, : self.heads, :] = self.bv[...].astype(F32)
        for c in self.bias_copies():
            c.start()
        self.kb[self.z, self.x] = self.head_of(self.kv, self.z)[...]
        self.vb[self.z, self.x] = self.head_of(self.vv, self.z)[...]
        self.qb[self.z] = self.head_of(self.qv, self.z)[...]

    def hand_over(self):
        for i in range(1, self.outer):
            for kind in range(2):
                self.wait_kv(kind, self.order[i], self.x)
                for c in self.side_copies(kind, i):
                    c.start()
        for d in range(1, self.n_sp):
            block = (self.own + d) % self.n_sp
            rcopy(
                self.bi.at[block],
                self.bi.at[block],
                self.bi_s.at[d],
                self.bi_r.at[block],
                {"sp": (self.own + 1) % self.n_sp},
            ).wait_recv()

    def compute(self):
        tok, hd = self.tok, self.hd
        scale = hd ** (-0.5)
        row = lax.broadcasted_iota(jnp.int32, (tok, tok), 0)
        col = lax.broadcasted_iota(jnp.int32, (tok, tok), 1)
        later = (row > col).astype(F32)
        sums = jnp.concatenate([later, jnp.ones((tok, tok), F32)], axis=1).astype(BF16)
        sums = jnp.concatenate([sums, sums], axis=0)
        for j in range(self.outer):
            for d in range(1, self.inner):
                for kind in range(2):
                    self.wait_kv(kind, j, (self.x + d) % self.inner)

            @pl.when(self.z != j)
            def _():
                rcopy(
                    self.qb.at[j], self.qb.at[j], self.e_s.at[2, 0], self.q_r.at[j], {"sp": (self.own + 1) % self.n_sp}
                ).wait_recv()

            q = self.qb[j]
            acc = jnp.zeros((tok, hd), F32)
            carry = jnp.zeros((tok, tok), F32)
            for k in range(j, -1, -1):
                for p in range(self.inner - 1, -1, -1):
                    bias = self.bi[k * self.inner + p, pl.ds(self.z, 1), :]
                    logit = rows_contract(q, self.kb[k, p]) * scale + bias
                    low = jnp.log(1.0 + jnp.exp(-jnp.abs(logit)))
                    fail = -(jnp.maximum(logit, 0.0) + low)
                    hit = jnp.minimum(logit, 0.0) - low
                    if k == j:
                        before = col < row + (self.x - p) * tok
                        fail = jnp.where(before, fail, 0.0)
                    high = fail.astype(BF16)
                    rest = (fail - high.astype(F32)).astype(BF16)
                    both = jnp.dot(
                        jnp.concatenate([high, rest], axis=1), sums, preferred_element_type=F32
                    )
                    w = jnp.exp(hit + both[:, :tok] + carry)
                    if k == j:
                        w = jnp.where(before, w, 0.0)
                    carry = carry + both[:, tok:]
                    acc = acc + jnp.dot(
                        w.astype(BF16), self.vb[k, p], preferred_element_type=F32
                    )
            self.ob[j] = acc.astype(BF16)

            @pl.when(self.z != j)
            def _():
                self.out_copy(j).start()

            @pl.when(self.z == j)
            def _():
                self.att[self.me, self.z] = self.ob[j]

    def out_copy(self, j):
        return rcopy(
            self.ob.at[j],
            self.att.at[self.me, self.z],
            self.o_s.at[j],
            self.att_r.at[self.me, self.z],
            {"sp": j * self.inner + self.x},
        )

    def wait_att(self, source, head):
        piece = self.att.at[source, head]
        rcopy(
            piece, piece, self.o_s.at[0], self.att_r.at[source, head], {"tp": (self.me + 1) % self.n_tp}
        ).wait_recv()

    def piece_copies(self, source, head, slot, targets):
        piece = self.att.at[source, head]
        return [
            rcopy(piece, piece, self.g_s.at[slot + n, head], self.att_r.at[source, head], {"tp": to})
            for n, to in enumerate(targets)
        ]

    def gather(self):
        wide = self.heads * self.hd

        def part(source):
            rows = jnp.concatenate([self.att[source, h] for h in range(self.outer)], axis=1)
            first = pl.multiple_of(source * wide, wide)
            return jnp.dot(rows, self.wo[pl.ds(first, wide), :], preferred_element_type=F32)

        slots = 1 + len(self.peers)
        for i in range(self.outer):
            head = self.order[i]
            if i:
                self.wait_att(self.me, head)
            for c in self.piece_copies(self.me, head, 0, self.peers + [self.partner]):
                c.start()
        for c in self.late:
            c.wait()
        self.acc[...] = self.sv[...].astype(F32) + part(self.me)
        for n, peer in enumerate(self.peers):
            for i in range(self.outer):
                self.wait_att(peer, self.order[i])
                for c in self.piece_copies(peer, self.order[i], slots + n, [self.partner]):
                    c.start()
        for i in range(self.outer):
            self.wait_att(self.partner, self.order[i])
        self.acc[...] += part(self.partner)
        for peer in self.peers:
            self.acc[...] += part(peer)
        others = [(self.partner + 2 * d) % self.n_tp for d in range(1, self.n_tp // 2)]
        for other in others:
            for i in range(self.outer):
                self.wait_att(other, self.order[i])
        total = self.acc[...]
        for other in others:
            total = total + part(other)
        self.mixed[...] = total.astype(BF16)

    def finish(self):
        groups = [self.bias_copies()]
        for i in range(1, self.outer):
            groups += [self.exchange_copies(kind, i) for kind in range(3)]
        for i in range(self.outer):
            groups += [self.side_copies(kind, i) for kind in range(2)]
            groups.append(
                self.piece_copies(self.me, self.order[i], 0, self.peers + [self.partner])
            )
            for n, peer in enumerate(self.peers):
                groups.append(
                    self.piece_copies(
                        peer, self.order[i], 1 + len(self.peers) + n, [self.partner]
                    )
                )
        for group in groups:
            for c in group:
                c.wait_send()
        for j in range(self.outer):

            @pl.when(self.z != j)
            def _():
                self.out_copy(j).wait_send()


LAYER_INPUTS = (
    "queries", "keys", "values", "bias", "stream", "out_proj", "gain_in", "ids_in", "wts_in",
    "gate", "up", "down", "s_gate", "s_up", "s_down",
)


def attend_scratch(n_sp, n_tp, inner, heads, hd, tok, width, top_k):
    outer = n_sp // inner
    vmem, dma = pltpu.VMEM, pltpu.SemaphoreType.DMA
    wide = heads * hd
    return {
        "qv": vmem((tok, wide), BF16),
        "kv": vmem((tok, wide), BF16),
        "vv": vmem((tok, wide), BF16),
        "bv": vmem((heads, tok), BF16),
        "sv": vmem((tok, width), BF16),
        "wo": vmem((n_tp * wide, width), BF16),
        "qb": vmem((outer, tok, hd), BF16),
        "kb": vmem((outer, inner, tok, hd), BF16),
        "vb": vmem((outer, inner, tok, hd), BF16),
        "bi": vmem((n_sp, 8, tok), F32),
        "ob": vmem((outer, tok, hd), BF16),
        "att": vmem((n_tp, outer, tok, hd), BF16),
        "mixed": vmem((tok, width), BF16),
        "gain": vmem((1, width), F32),
        "ids": vmem((top_k, tok), jnp.int32),
        "wts": vmem((top_k, tok), F32),
        "a_sem": dma((6,)),
        "s_sem": dma((3,)),
        "e_s": dma((3, outer)),
        "q_r": dma((outer,)),
        "kv_r": dma((2, outer, inner)),
        "side_s": dma((2, outer, inner)),
        "bi_s": dma((n_sp,)),
        "bi_r": dma((n_sp,)),
        "o_s": dma((outer,)),
        "att_r": dma((n_tp, outer)),
        "g_s": dma((n_tp, outer)),
    }


def layer_kernel(n_sp, n_tp, inner, el, cap, names, *refs):
    named = dict(zip(names, refs))
    first = Attend(n_sp, n_tp, inner, named)
    second = Experts(n_sp, n_tp, inner, el, cap, named)
    first.load()
    small = [
        pltpu.make_async_copy(named[name + "_in"], named[name], named["s_sem"].at[i])
        for i, name in enumerate(("ids", "wts", "gain"))
    ]
    for c in small:
        c.start()
    greet_all(n_sp, n_tp, first.own, first.me)
    first.load_late()
    second.load_weights()
    for c in small:
        c.wait()
    second.route()
    second.build_back()
    await_all(n_sp, n_tp)
    first.exchange()
    second.send_route()
    first.hand_over()
    first.compute()
    first.gather()
    second.run()
    first.finish()


def layer(operands, n_sp, n_tp, inner, cap, heads, hd):
    tok, width = operands[4].shape
    el, ff = operands[11].shape[:2]
    top_k = operands[7].shape[0]
    scratch = attend_scratch(n_sp, n_tp, inner, heads, hd, tok, width, top_k)
    scratch |= moe_scratch(n_sp, n_tp, inner, el, cap, tok, width, ff)
    hbm = pl.BlockSpec(memory_space=pltpu.MemorySpace.HBM)
    names = LAYER_INPUTS + ("out",) + tuple(scratch)
    return pl.pallas_call(
        functools.partial(layer_kernel, n_sp, n_tp, inner, el, cap, names),
        out_shape=jax.ShapeDtypeStruct((tok, width), BF16),
        in_specs=[hbm] * len(operands),
        out_specs=pl.BlockSpec(memory_space=pltpu.VMEM),
        scratch_shapes=list(scratch.values()),
        compiler_params=pltpu.CompilerParams(
            vmem_limit_bytes=56 * 2**20, collective_id=0, has_side_effects=True
        ),
        cost_estimate=pl.CostEstimate(flops=10**10, bytes_accessed=2**24, transcendentals=10**6),
    )(*operands)


def body(
    queries,
    key_rows,
    value_rows,
    break_bias,
    stream,
    out_proj,
    norm_gain,
    expert_ids,
    route_weights,
    gate_proj,
    up_proj,
    down_proj,
    shared_gate,
    shared_up,
    shared_down,
):
    tok = queries.shape[0]
    heads = break_bias.shape[1]
    hd = queries.shape[1] // heads
    n_sp = lax.axis_size("sp")
    n_tp = lax.axis_size("tp")
    width = stream.shape[1] * n_tp

    bias_wide = jnp.pad(break_bias, ((0, 0), (0, hd - heads)))

    experts_local = gate_proj.shape[0]
    experts = experts_local * n_sp
    top_k = expert_ids.shape[1]
    cap = 2 * top_k * tok // experts
    n_inner = max(d for d in range(1, n_sp + 1) if n_sp % d == 0 and d * d <= n_sp)
    plane_rows = n_inner * experts_local * cap
    if heads * n_inner == n_sp and heads == 4 and plane_rows == tok and cap % 16 == 0 and tok % (16 * n_tp) == 0:
        operands = (
            queries, key_rows, value_rows, break_bias.T, stream, out_proj, norm_gain[None, :],
            expert_ids.T, route_weights.T, gate_proj, up_proj, down_proj,
            shared_gate, shared_up, shared_down,
        )
        return layer(operands, n_sp, n_tp, n_inner, cap, heads, hd)
    expert_of = jnp.arange(experts, dtype=jnp.int32)
    named = expert_ids[:, :, None] == expert_of[None, None, :]
    named_any = jnp.any(named, axis=1).astype(BF16)
    token = jnp.arange(tok, dtype=jnp.int32)
    earlier = (token[None, :] < token[:, None]).astype(BF16)
    rank_all = jnp.dot(earlier, named_any, preferred_element_type=F32)
    rank = jnp.sum(jnp.where(named, rank_all[:, None, :], 0.0), axis=2).astype(jnp.int32)
    slot = expert_ids * cap + rank
    slots = experts * cap
    place = jnp.arange(slots, dtype=jnp.int32)
    spot = slot[:, :, None] == place[None, None, :]
    send_pick = jnp.any(spot, axis=1).astype(BF16)
    back_pick = jnp.sum(jnp.where(spot, route_weights[:, :, None], 0.0), axis=1).astype(BF16)

    attended = attention(queries, key_rows, value_rows, bias_wide, heads, hd, n_sp)
    projected = jnp.dot(
        lax.all_gather(attended, "tp", axis=1, tiled=True), out_proj, preferred_element_type=F32
    )
    mixed = (stream.astype(F32) + projected).astype(BF16)
    mixed = lax.optimization_barrier(mixed)
    mixed_f = mixed.astype(F32)
    square_sum = lax.psum(jnp.sum(mixed_f * mixed_f, axis=1), "tp")
    inv_rms = lax.rsqrt(square_sum / width + EPS)
    normed = (mixed_f * inv_rms[:, None] * norm_gain[None, :]).astype(BF16)

    send = lax.dot_general(
        send_pick, normed, (((0,), (0,)), ((), ())), preferred_element_type=F32
    ).astype(BF16)
    send = send.reshape(n_sp, experts_local * cap, normed.shape[1])
    arrived = lax.all_to_all(send, "sp", split_axis=0, concat_axis=0, tiled=True)
    arrived = arrived.reshape(n_sp, experts_local, cap, -1)
    gates, ups = [], []
    for e in range(experts_local):
        rows = arrived[:, e].reshape(n_sp * cap, -1)
        gates.append(jnp.dot(rows, gate_proj[e], preferred_element_type=F32).astype(BF16))
        ups.append(jnp.dot(rows, up_proj[e], preferred_element_type=F32).astype(BF16))
    gates.append(jnp.dot(normed, shared_gate, preferred_element_type=F32).astype(BF16))
    ups.append(jnp.dot(normed, shared_up, preferred_element_type=F32).astype(BF16))
    gate_all = jnp.concatenate(gates, axis=0)
    up_all = jnp.concatenate(ups, axis=0)
    gate_up = jnp.concatenate([gate_all, up_all], axis=1)
    hidden = exchange(gate_up, n_tp)
    outs = []
    for e in range(experts_local):
        rows = hidden[e * n_sp * cap : (e + 1) * n_sp * cap]
        out = jnp.dot(rows, down_proj[e], preferred_element_type=F32).astype(BF16)
        outs.append(out.reshape(n_sp, 1, cap, -1))
    expert_out = jnp.concatenate(outs, axis=1).reshape(n_sp, experts_local * cap, -1)
    returned = lax.all_to_all(expert_out, "sp", split_axis=0, concat_axis=0, tiled=True)
    returned = returned.reshape(slots, -1)
    shared_out = jnp.dot(
        hidden[experts_local * n_sp * cap :], shared_down, preferred_element_type=F32
    )
    routed = jnp.dot(back_pick, returned, preferred_element_type=F32)
    return (mixed_f + shared_out + routed).astype(BF16)


def solution(mesh):
    in_specs = (
        P("sp", "tp"),
        P("sp", "tp"),
        P("sp", "tp"),
        P("sp", "tp"),
        P("sp", "tp"),
        P(None, "tp"),
        P("tp"),
        P("sp", None),
        P("sp", None),
        P("sp", "tp", None),
        P("sp", "tp", None),
        P("sp", None, "tp"),
        P("tp", None),
        P("tp", None),
        P(None, "tp"),
    )
    return jax.shard_map(body, mesh=mesh, in_specs=in_specs, out_specs=P("sp", "tp"), check_vma=False)
```

```python
import functools

import jax
import jax.numpy as jnp
from jax import lax
from jax.experimental import pallas as pl
from jax.experimental.pallas import tpu as pltpu
from jax.sharding import PartitionSpec as P

EPS = 1e-06
F32 = jnp.float32
BF16 = jnp.bfloat16


def attention_kernel(
    heads, hd, n_sp, inner, q_ref, k_ref, v_ref, b_ref, o_ref, kbuf, vbuf, bbuf, acc, carry, send_sem, recv_sem
):
    tok = q_ref.shape[0]
    own = lax.axis_index("sp")
    outer = n_sp // inner
    z_own = own // inner
    x_own = own % inner
    above = z_own < outer - 1
    below = z_own > 0

    barrier = pltpu.get_barrier_semaphore()

    def greet(target):
        pl.semaphore_signal(
            barrier, inc=1, device_id={"sp": target}, device_id_type=pl.DeviceIdType.MESH
        )

    @pl.when(above)
    def _():
        greet(own + inner)

    @pl.when(below)
    def _():
        greet(own - inner)

    for d in range(1, inner):
        greet(z_own * inner + (x_own + d) % inner)
    pl.semaphore_wait(barrier, inner - 1 + above.astype(jnp.int32) + below.astype(jnp.int32))

    def copies(sources, block, z_block, lane, target):
        return [
            pltpu.make_async_remote_copy(
                src_ref=src,
                dst_ref=dst.at[block],
                send_sem=send_sem.at[kind, z_block, lane],
                recv_sem=recv_sem.at[kind, block],
                device_id={"sp": target},
                device_id_type=pl.DeviceIdType.MESH,
            )
            for kind, (src, dst) in enumerate(zip(sources, (kbuf, vbuf, bbuf)))
        ]

    def held(block):
        return (kbuf.at[block], vbuf.at[block], bbuf.at[block])

    def start_all(group):
        for c in group:
            c.start()

    def wait_sent(group):
        for c in group:
            c.wait_send()

    def wait_arrived(block):
        for c in copies(held(block), block, 0, 0, (own + 1) % n_sp):
            c.wait_recv()

    def own_sends(act):
        mine = (k_ref, v_ref, b_ref)

        @pl.when(above)
        def _():
            act(copies(mine, own, z_own, 0, own + inner))

        for d in range(1, inner):
            x_to = (x_own + d) % inner

            @pl.when(x_to > x_own)
            def _():
                act(copies(mine, own, z_own, d, z_own * inner + x_to))

    def relays(z_block, act):
        block = z_block * inner + x_own

        @pl.when(above)
        def _():
            act(copies(held(block), block, z_block, 0, own + inner))

        for d in range(1, inner):
            act(copies(held(block), block, z_block, d, z_own * inner + (x_own + d) % inner))

    own_sends(start_all)

    scale = hd ** (-0.5)
    row = lax.broadcasted_iota(jnp.int32, (tok, tok), 0)
    col = lax.broadcasted_iota(jnp.int32, (tok, tok), 1)
    later = (row > col).astype(F32)
    sums = jnp.concatenate([later, jnp.ones((tok, tok), F32)], axis=1).astype(BF16)
    sums = jnp.concatenate([sums, sums], axis=0)
    pick_rows = max(16, heads)
    pick = (
        lax.broadcasted_iota(jnp.int32, (pick_rows, hd), 0)
        == lax.broadcasted_iota(jnp.int32, (pick_rows, hd), 1)
    ).astype(F32).astype(BF16)
    acc[...] = jnp.zeros_like(acc)
    carry[...] = jnp.zeros_like(carry)

    def compute(keys, values, offsets, diagonal):
        bias = lax.dot_general(
            pick, offsets[...], (((1,), (1,)), ((), ())), preferred_element_type=F32
        )
        for h in range(heads):
            cols = slice(h * hd, (h + 1) * hd)
            z = lax.dot_general(
                q_ref[:, cols], keys[:, cols], (((1,), (1,)), ((), ())), preferred_element_type=F32
            )
            z = z * scale + bias[h : h + 1, :]
            low = jnp.log1p(jnp.exp(-jnp.abs(z)))
            fail = -(jnp.maximum(z, 0.0) + low)
            hit = jnp.minimum(z, 0.0) - low
            if diagonal:
                before = col < row
                fail = jnp.where(before, fail, 0.0)
            high = fail.astype(BF16)
            rest = (fail - high.astype(F32)).astype(BF16)
            both = jnp.dot(
                jnp.concatenate([high, rest], axis=1), sums, preferred_element_type=F32
            )
            before_sum = carry[h]
            w = jnp.exp(hit + both[:, :tok] + before_sum)
            if diagonal:
                w = jnp.where(before, w, 0.0)
            carry[h] = before_sum + both[:, tok:]
            acc[:, cols] += jnp.dot(w.astype(BF16), values[:, cols], preferred_element_type=F32)

    compute(k_ref, v_ref, b_ref, True)

    def group(i, _):
        z_block = z_own - i

        @pl.when(z_block > 0)
        def _():
            wait_arrived((z_block - 1) * inner + x_own)
            relays(z_block - 1, start_all)

        def member(m, _):
            x_block = inner - 1 - m
            block = z_block * inner + x_block

            @pl.when(block < own)
            def _():
                @pl.when(x_block != x_own)
                def _():
                    wait_arrived(block)

                compute(*held(block), False)

            return 0

        lax.fori_loop(0, inner, member, 0)
        return 0

    lax.fori_loop(0, z_own + 1, group, 0)
    o_ref[...] = acc[...].astype(BF16)

    own_sends(wait_sent)

    def drain(z_block, _):
        relays(z_block, wait_sent)
        return 0

    lax.fori_loop(0, z_own, drain, 0)


def attention(queries, keys, values, bias, heads, hd, n_sp):
    tok = queries.shape[0]
    inner = max(d for d in range(1, n_sp + 1) if n_sp % d == 0 and d * d <= n_sp)
    vmem = pl.BlockSpec(memory_space=pltpu.VMEM)
    return pl.pallas_call(
        functools.partial(attention_kernel, heads, hd, n_sp, inner),
        out_shape=jax.ShapeDtypeStruct((tok, heads * hd), BF16),
        in_specs=[vmem] * 4,
        out_specs=vmem,
        scratch_shapes=[
            pltpu.VMEM((n_sp, tok, heads * hd), BF16),
            pltpu.VMEM((n_sp, tok, heads * hd), BF16),
            pltpu.VMEM((n_sp, tok, hd), BF16),
            pltpu.VMEM((tok, heads * hd), F32),
            pltpu.VMEM((heads, tok, tok), F32),
            pltpu.SemaphoreType.DMA((3, n_sp // inner, inner)),
            pltpu.SemaphoreType.DMA((3, n_sp)),
        ],
        compiler_params=pltpu.CompilerParams(
            vmem_limit_bytes=40 * 2**20, collective_id=0, has_side_effects=True
        ),
        cost_estimate=pl.CostEstimate(flops=2 * 10**9, bytes_accessed=2**22, transcendentals=10**6),
    )(queries, keys, values, bias)


def exchange_kernel(n_tp, gu_ref, o_ref, parts, mine, spread, send_parts, recv_parts, send_rows, recv_rows):
    width = gu_ref.shape[2] // 2
    me = lax.axis_index("tp")
    barrier = pltpu.get_barrier_semaphore()
    others = [(me + d) % n_tp for d in range(1, n_tp)]
    for to in others:
        pl.semaphore_signal(
            barrier, inc=1, device_id={"tp": to}, device_id_type=pl.DeviceIdType.MESH
        )
    pl.semaphore_wait(barrier, n_tp - 1)
    first, second = [], []
    for d, to in enumerate(others):
        copy = pltpu.make_async_remote_copy(
            src_ref=gu_ref.at[to],
            dst_ref=parts.at[d],
            send_sem=send_parts.at[d],
            recv_sem=recv_parts.at[d],
            device_id={"tp": to},
            device_id_type=pl.DeviceIdType.MESH,
        )
        copy.start()
        first.append(copy)
    total = gu_ref[me].astype(F32)
    for d, copy in enumerate(first):
        copy.wait_recv()
        total = total + parts[d].astype(F32)
    gate = total[:, :width]
    mine[...] = (jax.nn.silu(gate) * total[:, width:]).astype(BF16)
    for d, to in enumerate(others):
        copy = pltpu.make_async_remote_copy(
            src_ref=mine,
            dst_ref=spread.at[d],
            send_sem=send_rows.at[d],
            recv_sem=recv_rows.at[d],
            device_id={"tp": to},
            device_id_type=pl.DeviceIdType.MESH,
        )
        copy.start()
        second.append(copy)
    o_ref[me] = mine[...]
    for d, copy in enumerate(second):
        copy.wait_recv()
        o_ref[(me + n_tp - 1 - d) % n_tp] = spread[d]
    for copy in first + second:
        copy.wait_send()


def exchange(gate_up, n_tp):
    rows, width = gate_up.shape[0] // n_tp, gate_up.shape[1] // 2
    vmem = pl.BlockSpec(memory_space=pltpu.VMEM)
    dma = pltpu.SemaphoreType.DMA((n_tp - 1,))
    hidden = pl.pallas_call(
        functools.partial(exchange_kernel, n_tp),
        out_shape=jax.ShapeDtypeStruct((n_tp, rows, width), BF16),
        in_specs=[vmem],
        out_specs=vmem,
        scratch_shapes=[
            pltpu.VMEM((n_tp - 1, rows, 2 * width), BF16),
            pltpu.VMEM((rows, width), BF16),
            pltpu.VMEM((n_tp - 1, rows, width), BF16),
            dma,
            dma,
            dma,
            dma,
        ],
        compiler_params=pltpu.CompilerParams(
            vmem_limit_bytes=24 * 2**20, collective_id=1, has_side_effects=True
        ),
        cost_estimate=pl.CostEstimate(flops=10**8, bytes_accessed=2**21, transcendentals=10**5),
    )(gate_up.reshape(n_tp, rows, 2 * width))
    return hidden.reshape(n_tp * rows, width)


MESH = pl.DeviceIdType.MESH
CUTS = 4


def rows_contract(lhs, rhs):
    return lax.dot_general(lhs, rhs, (((1,), (1,)), ((), ())), preferred_element_type=F32)


def rcopy(src, dst, send_sem, recv_sem, where):
    return pltpu.make_async_remote_copy(
        src_ref=src,
        dst_ref=dst,
        send_sem=send_sem,
        recv_sem=recv_sem,
        device_id=where,
        device_id_type=MESH,
    )


def plane_order(z, outer):
    step = 1 - 2 * ((2 * z) // outer)
    return [(z + step * i + outer) % outer for i in range(outer)]


def greet_all(n_sp, n_tp, own, me):
    barrier = pltpu.get_barrier_semaphore()
    for d in range(1, n_sp):
        pl.semaphore_signal(
            barrier, inc=1, device_id={"sp": (own + d) % n_sp}, device_id_type=MESH
        )
    for d in range(1, n_tp):
        pl.semaphore_signal(
            barrier, inc=1, device_id={"tp": (me + d) % n_tp}, device_id_type=MESH
        )


def await_all(n_sp, n_tp):
    pl.semaphore_wait(pltpu.get_barrier_semaphore(), n_sp + n_tp - 2)


class Experts:
    def __init__(self, n_sp, n_tp, inner, experts_local, cap, refs):
        self.n_sp, self.n_tp, self.inner = n_sp, n_tp, inner
        self.outer = n_sp // inner
        self.el, self.cap = experts_local, cap
        self.rw = experts_local * cap
        self.__dict__.update(refs)
        self.own = lax.axis_index("sp")
        self.me = lax.axis_index("tp")
        self.z = self.own // inner
        self.x = self.own % inner
        self.side = self.z // 2
        self.within = self.z % 2
        self.mate = self.z + 1 - 2 * self.within
        self.middle = 1 + self.side
        self.order = [self.z, 2 - self.side, 3 - 3 * self.side, self.mate]
        self.core = self.me % 2
        self.partner = self.me + 1 - 2 * self.core
        self.chip = self.me // 2
        self.between = (self.z > 0) & (self.z < self.outer - 1)
        self.at_end = jnp.logical_not(self.between)
        self.tok, self.width = self.mixed.shape
        self.ff = self.down.shape[1]
        self.total_width = self.width * n_tp

    def load_weights(self):
        ff = self.ff
        self.loads = [
            pltpu.make_async_copy(src, dst, self.w_sem.at[i])
            for i, (src, dst) in enumerate(
                (
                    (self.s_gate, self.wsgu.at[:, pl.ds(0, ff)]),
                    (self.s_up, self.wsgu.at[:, pl.ds(ff, ff)]),
                    (self.gate, self.wgu.at[:, :, pl.ds(0, ff)]),
                    (self.up, self.wgu.at[:, :, pl.ds(ff, ff)]),
                    (self.down, self.wd),
                    (self.s_down, self.wsd),
                )
            )
        ]
        for load in self.loads:
            load.start()

    def meta_copies(self, ref, send, recv):
        return [
            rcopy(
                ref.at[self.own],
                ref.at[self.own],
                send.at[d],
                recv.at[self.own],
                {"sp": (self.own + d) % self.n_sp},
            )
            for d in range(1, self.n_sp)
        ]

    def wait_table(self, ref, send, recv, block):
        rcopy(
            ref.at[block], ref.at[block], send.at[0], recv.at[block], {"sp": (self.own + 1) % self.n_sp}
        ).wait_recv()

    def route(self):
        ids = self.ids[...]
        experts = self.el * self.n_sp
        top_k, tok = ids.shape
        expert_of = lax.broadcasted_iota(jnp.int32, (experts, tok), 0)
        named = [ids[k : k + 1, :] == expert_of for k in range(top_k)]
        named_any = functools.reduce(jnp.logical_or, named).astype(F32).astype(BF16)
        before = (
            lax.broadcasted_iota(jnp.int32, (tok, tok), 0)
            < lax.broadcasted_iota(jnp.int32, (tok, tok), 1)
        ).astype(F32).astype(BF16)
        rank = jnp.dot(named_any, before, preferred_element_type=F32)
        self.meta[self.own] = jnp.zeros((8, tok), F32)
        for k in range(top_k):
            mine = jnp.sum(jnp.where(named[k], rank, 0.0), axis=0, keepdims=True)
            slot = ids[k : k + 1, :].astype(F32) * self.cap + mine
            self.meta[self.own, k : k + 1, :] = slot
            self.meta[self.own, top_k + k : top_k + k + 1, :] = self.wts[k : k + 1, :]
        self.top_k = top_k

    def send_route(self):
        self.meta_group = self.meta_copies(self.meta, self.meta_s, self.meta_r)
        for c in self.meta_group:
            c.start()

    def wait_route(self):
        for d in range(1, self.n_sp):
            self.wait_table(self.meta, self.meta_s, self.meta_r, (self.own + d) % self.n_sp)

    def slot_hits(self, block, first, count):
        spot = (
            lax.broadcasted_iota(jnp.int32, (count, self.tok), 0) + first
        ).astype(F32)
        return [self.meta[block, k : k + 1, :] == spot for k in range(self.top_k)]

    def back_of(self, block, plane):
        rows = self.inner * self.rw
        hits = self.slot_hits(block, plane * rows, rows)
        weight = sum(
            jnp.where(
                hits[k], self.meta[block, self.top_k + k : self.top_k + k + 1, :], 0.0
            )
            for k in range(self.top_k)
        )
        return jnp.transpose(weight).astype(BF16)

    def build_back(self):
        self.back[0] = self.back_of(self.own, self.z)
        self.back[1] = self.back_of(self.own, self.mate)

    def halves(self):
        half = self.width // 2
        return [pl.ds(h * half, half) for h in range(2)]

    def dense_copies(self, src, plane, target, only=None):
        return [
            rcopy(
                src.at[:, cols],
                self.dense.at[plane, :, cols],
                self.dense_s.at[plane, h],
                self.dense_r.at[plane, h],
                {"sp": target * self.inner + self.x},
            )
            for h, cols in enumerate(self.halves())
            if only is None or h == only
        ]

    def own_copies(self):
        at_end = self.at_end.astype(jnp.int32)
        target = at_end * self.mate + (1 - at_end) * (3 - self.z)
        return self.dense_copies(self.mixed, self.z, target)

    def relay_copies(self, only=None):
        return self.dense_copies(self.dense.at[self.mate], self.mate, 3 - self.z, only)

    def receive(self, plane, h):
        piece = self.dense.at[plane, :, self.halves()[h]]
        rcopy(
            piece, piece, self.dense_s.at[plane, h], self.dense_r.at[plane, h], {"sp": (self.own + 1) % self.n_sp}
        ).wait_recv()

    def pick_rows(self, block, plane):
        rows = self.inner * self.rw
        hits = self.slot_hits(block, plane * rows, rows)
        return functools.reduce(jnp.logical_or, hits).astype(F32).astype(BF16)

    def ahead_copies(self, i, h):
        cols = self.halves()[h]
        return [
            rcopy(
                self.ahead.at[i, (self.x + d) % self.inner, :, cols],
                self.rows.at[i or 3, self.x, :, cols],
                self.ahead_s.at[i, d, h],
                self.x_r.at[i or 3, self.x, h],
                {"sp": self.mate * self.inner + (self.x + d) % self.inner},
            )
            for d in range(self.inner)
        ]

    def push(self, i, h):
        cols = self.halves()[h]
        pick = self.pick_rows(self.order[i] * self.inner + self.x, self.mate)
        source = self.dense[self.order[i], :, cols] if i else self.mixed[:, cols]
        got = jnp.dot(pick, source, preferred_element_type=F32).astype(BF16)
        for p in range(self.inner):
            self.ahead[i, p, :, cols] = got[p * self.rw : (p + 1) * self.rw]
        for c in self.ahead_copies(i, h):
            c.start()

    def cross_copies(self, i):
        return [
            rcopy(
                self.picked.at[i, (self.x + d) % self.inner, :, cols],
                self.rows.at[i, self.x, :, cols],
                self.x_s.at[i, d, h],
                self.x_r.at[i, self.x, h],
                {"sp": self.z * self.inner + (self.x + d) % self.inner},
            )
            for h, cols in enumerate(self.halves())
            for d in range(1, self.inner)
        ]

    def select(self, i):
        pick = self.pick_rows(self.order[i] * self.inner + self.x, self.z)
        source = self.dense[self.order[i]] if i else self.mixed[...]
        got = jnp.dot(pick, source, preferred_element_type=F32).astype(BF16)
        for p in range(self.inner):
            self.picked[i, p] = got[p * self.rw : (p + 1) * self.rw]
        for c in self.cross_copies(i):
            c.start()
        self.rows[i, self.x] = self.picked[i, self.x]

    def wait_rows(self, i):
        def arrived(x_from):
            for h, cols in enumerate(self.halves()):
                piece = self.rows.at[i, x_from, :, cols]
                rcopy(
                    piece,
                    piece,
                    self.x_s.at[i, 0, h],
                    self.x_r.at[i, x_from, h],
                    {"sp": (self.own + 1) % self.n_sp},
                ).wait_recv()

        if i:

            @pl.when(self.at_end)
            def _():
                arrived(self.x)

        for d in range(1, self.inner):
            arrived((self.x + d) % self.inner)

    def tp_copies(self, src, dst, send, recv):
        return [
            rcopy(src(to), dst, send.at[d], recv.at[self.me], {"tp": to})
            for d, to in ((d, (self.me + d) % self.n_tp) for d in range(1, self.n_tp))
        ]

    def tp_wait(self, dst, send, recv):
        for d in range(1, self.n_tp):
            other = (self.me + d) % self.n_tp
            rcopy(
                dst(other), dst(other), send.at[0], recv.at[other], {"tp": (self.me + 1) % self.n_tp}
            ).wait_recv()

    def send_squares(self):
        wide = self.mixed[...].astype(F32)
        column = jnp.sum(wide * wide, axis=1, keepdims=True)
        row = jnp.transpose(jnp.broadcast_to(column, (self.tok, self.tok)))
        self.ssq[self.me] = row[:8]
        self.ssq_group = self.tp_copies(
            lambda to: self.ssq.at[self.me], self.ssq.at[self.me], self.ssq_s, self.ssq_r
        )
        for c in self.ssq_group:
            c.start()

    def send_scales(self):
        self.tp_wait(lambda other: self.ssq.at[other], self.ssq_s, self.ssq_r)
        total = self.ssq[0]
        for p in range(1, self.n_tp):
            total = total + self.ssq[p]
        self.inv[self.own] = lax.rsqrt(total / self.total_width + EPS)
        self.inv_group = self.meta_copies(self.inv, self.inv_s, self.inv_r)
        for c in self.inv_group:
            c.start()

    def part_copy(self, s):
        return rcopy(
            self.gu.at[s, 1 - self.core],
            self.parts.at[s],
            self.part_s.at[s],
            self.part_r.at[s],
            {"tp": self.partner},
        )

    def pair_copies(self, s):
        return [
            rcopy(
                self.pairs.at[s],
                self.sides.at[s, self.chip],
                self.pair_s.at[s, d],
                self.pair_r.at[s, self.chip],
                {"tp": (self.me + 2 * d) % self.n_tp},
            )
            for d in range(1, self.n_tp // 2)
        ]

    def hid_copy(self, s):
        mine = self.hid.at[s, self.core]
        return rcopy(
            mine, mine, self.hid_s.at[s], self.hid_r.at[s], {"tp": self.partner}
        )

    def send_parts(self, s, value):
        half = value.shape[0] // 2
        for c in range(2):
            self.gu[s, c] = value[c * half : (c + 1) * half]
        self.part_copy(s).start()

    def pair(self, s):
        self.part_copy(s).wait_recv()
        self.pairs[s] = (
            self.gu[s, self.core].astype(F32) + self.parts[s].astype(F32)
        ).astype(BF16)
        for c in self.pair_copies(s):
            c.start()

    def gate_up(self, i):
        if i == 0:
            self.loads[2].wait()
            self.loads[3].wait()
        self.wait_rows(i)
        normed = []
        for d in range(self.inner):
            block = self.order[i] * self.inner + (self.x + d) % self.inner
            if i or d:
                self.wait_table(self.inv, self.inv_s, self.inv_r, block)
        for p in range(self.inner):
            block = self.order[i] * self.inner + p
            hits = self.slot_hits(block, self.own * self.rw, self.rw)
            pick = functools.reduce(jnp.logical_or, hits)
            scale = jnp.sum(
                jnp.where(pick, self.inv[block, 0:1, :], 0.0), axis=1, keepdims=True
            )
            wide = self.rows[i, p].astype(F32)
            normed.append((wide * scale * self.gain[...]).astype(BF16))
        out = []
        for e in range(self.el):
            rows = jnp.concatenate(
                [n[e * self.cap : (e + 1) * self.cap] for n in normed], axis=0
            )
            out.append(jnp.dot(rows, self.wgu[e], preferred_element_type=F32).astype(BF16))
        self.send_parts(i, jnp.concatenate(out, axis=0))

    def shared_gate_up(self):
        self.loads[0].wait()
        self.loads[1].wait()
        scale = jnp.transpose(jnp.broadcast_to(self.inv[self.own, 0:1, :], (self.tok, self.tok)))
        normed = (
            self.mixed[...].astype(F32) * scale[:, 0:1] * self.gain[...]
        ).astype(BF16)
        value = jnp.dot(normed, self.wsgu[...], preferred_element_type=F32).astype(BF16)
        self.send_parts(self.outer, value)

    def hidden(self, s):
        total = self.pairs[s].astype(F32)
        for d in range(1, self.n_tp // 2):
            other = (self.chip + d) % (self.n_tp // 2)
            rcopy(
                self.sides.at[s, other],
                self.sides.at[s, other],
                self.pair_s.at[s, d],
                self.pair_r.at[s, other],
                {"tp": self.partner},
            ).wait_recv()
            total = total + self.sides[s, other].astype(F32)
        act = jax.nn.silu(total[:, : self.ff]) * total[:, self.ff :]
        self.hid[s, self.core] = act.astype(BF16)
        self.hid_copy(s).start()

    def all_hidden(self, s):
        other = self.hid.at[s, 1 - self.core]
        rcopy(other, other, self.hid_s.at[s], self.hid_r.at[s], {"tp": self.partner}).wait_recv()
        return jnp.concatenate([self.hid[s, c] for c in range(2)], axis=0)

    def cuts(self):
        cut = self.width // CUTS
        return [pl.ds(h * cut, cut) for h in range(CUTS)]

    def return_copies(self, i):
        return [
            rcopy(
                self.outs.at[i, (self.x + d) % self.inner],
                self.ret.at[self.own],
                self.ret_s.at[i, d],
                self.ret_r.at[self.own],
                {"sp": self.order[i] * self.inner + (self.x + d) % self.inner},
            )
            for d in range(0 if i else 1, self.inner)
        ]

    def over_copies(self, i, c, first):
        return [
            rcopy(
                self.outs.at[i, (self.x + d) % self.inner, :, cols],
                self.over.at[c, self.within, self.x, :, cols],
                self.over_s.at[i, d, h],
                self.over_r.at[c, self.within, self.x, h],
                {"sp": self.middle * self.inner + (self.x + d) % self.inner},
            )
            for h, cols in enumerate(self.cuts())
            for d in range(first, self.inner)
        ]

    def side_out_copies(self, i):
        return [
            rcopy(
                self.outs.at[i, (self.x + d) % self.inner, :, cols],
                self.beside.at[i - 1, self.x, :, cols],
                self.beside_s.at[i - 1, d, h],
                self.beside_r.at[i - 1, self.x, h],
                {"sp": self.z * self.inner + (self.x + d) % self.inner},
            )
            for h, cols in enumerate(self.cuts())
            for d in range(1, self.inner)
        ]

    def column_copies(self, i, d, h):
        cols = self.cuts()[h]
        x_of = (self.x + d) % self.inner
        src = self.beside.at[i - 1, x_of, :, cols] if d else self.outs.at[i, self.x, :, cols]
        if i == 3:
            dst = self.ret.at[self.z * self.inner + x_of, :, cols]
            arrived = self.ret_h.at[x_of, h]
        else:
            dst = self.over.at[i - 1, self.within, x_of, :, cols]
            arrived = self.over_r.at[i - 1, self.within, x_of, h]
        return [
            rcopy(src, dst, self.over_s.at[i, d, h], arrived, {"sp": self.mate * self.inner + self.x})
        ]

    def bring_along(self, i):
        for h, cols in enumerate(self.cuts()):
            for d in range(1, self.inner):
                x_of = (self.x + d) % self.inner
                piece = self.beside.at[i - 1, x_of, :, cols]
                rcopy(
                    piece,
                    piece,
                    self.beside_s.at[i - 1, d, h],
                    self.beside_r.at[i - 1, x_of, h],
                    {"sp": (self.own + 1) % self.n_sp},
                ).wait_recv()
                for c in self.column_copies(i, d, h):
                    c.start()

    def each_return(self, i, act, sent=False):
        if i == 0:
            act(self.return_copies(0))
            return

        @pl.when(self.at_end)
        def _():
            act(self.side_out_copies(i))
            for h in range(CUTS):
                for d in range(self.inner if sent else 1):
                    act(self.column_copies(i, d, h))

        @pl.when(self.between)
        def _():
            act(self.over_copies(i, i - 1, 1) if i < 3 else self.return_copies(i))

    def sum_copy(self, c, h):
        cols = self.cuts()[h]
        return rcopy(
            self.sums.at[c, :, cols],
            self.far.at[:, cols],
            self.sum_s.at[c, h],
            self.far_r.at[h],
            {"sp": self.order[c + 1] * self.inner + self.x},
        )

    def add_over(self, c):
        block = self.order[c + 1] * self.inner + self.x
        pair = 2 * self.side
        backs = [self.back_of(block, pair + s) for s in range(2)]
        for h, cols in enumerate(self.cuts()):

            def arrived(s, x_from):
                piece = self.over.at[c, s, x_from, :, cols]
                rcopy(
                    piece,
                    piece,
                    self.over_s.at[0, 0, h],
                    self.over_r.at[c, s, x_from, h],
                    {"sp": (self.own + 1) % self.n_sp},
                ).wait_recv()

            total = 0.0
            for s in range(2):
                for d in range(1, self.inner):
                    arrived(s, (self.x + d) % self.inner)

                @pl.when(self.within != s)
                def _():
                    arrived(s, self.x)

                rows = jnp.concatenate(
                    [self.over[c, s, p, :, cols] for p in range(self.inner)], axis=0
                )
                total = total + jnp.dot(backs[s], rows, preferred_element_type=F32)
            self.sums[c, :, cols] = total.astype(BF16)
            self.sum_copy(c, h).start()

    def down_rows(self, i):
        if i == 0:
            self.loads[4].wait()
        hidden = self.all_hidden(i)
        span = self.inner * self.cap
        for e in range(self.el):
            out = jnp.dot(
                hidden[e * span : (e + 1) * span], self.wd[e], preferred_element_type=F32
            ).astype(BF16)
            for p in range(self.inner):
                self.outs[i, p, e * self.cap : (e + 1) * self.cap, :] = out[
                    p * self.cap : (p + 1) * self.cap
                ]

        def start(group):
            for c in group:
                c.start()

        self.each_return(i, start)
        if i == 0:
            self.ret[self.own] = self.outs[0, self.x]
        elif i < 3:

            @pl.when(self.between)
            def _():
                self.over[i - 1, self.within, self.x] = self.outs[i, self.x]

    def shared_down(self):
        self.loads[5].wait()
        shared = jnp.dot(
            self.all_hidden(self.outer), self.wsd[...], preferred_element_type=F32
        )
        self.acc[...] = self.mixed[...].astype(F32) + shared

    def collect(self, n):
        plane = (self.z, self.mate)[n]

        def whole(d):
            block = plane * self.inner + (self.x + d) % self.inner
            rcopy(
                self.ret.at[block],
                self.ret.at[block],
                self.ret_s.at[n, d],
                self.ret_r.at[block],
                {"sp": (self.own + 1) % self.n_sp},
            ).wait_recv()

        def in_halves(d):
            x_of = (self.x + d) % self.inner
            for h, cols in enumerate(self.cuts()):
                piece = self.ret.at[plane * self.inner + x_of, :, cols]
                rcopy(
                    piece, piece, self.ret_s.at[n, d], self.ret_h.at[x_of, h], {"sp": (self.own + 1) % self.n_sp}
                ).wait_recv()

        if n == 0:
            for d in range(1, self.inner):
                whole(d)
        else:

            @pl.when(self.at_end)
            def _():
                for d in range(self.inner):
                    whole(d)

            @pl.when(self.between)
            def _():
                for d in range(self.inner):
                    in_halves(d)

        rows = jnp.concatenate(
            [self.ret[plane * self.inner + p] for p in range(self.inner)], axis=0
        )
        self.acc[...] += jnp.dot(self.back[n], rows, preferred_element_type=F32)

    def close(self):
        for h, cols in enumerate(self.cuts()):
            piece = self.far.at[:, cols]
            rcopy(
                piece, piece, self.sum_s.at[0, h], self.far_r.at[h], {"sp": (self.own + 1) % self.n_sp}
            ).wait_recv()
            self.out[:, cols] = (self.acc[:, cols] + self.far[:, cols].astype(F32)).astype(BF16)

    def finish(self):
        groups = [self.meta_group, self.inv_group, self.ssq_group]
        for n in range(self.outer + 1):
            groups += [[self.part_copy(n)], self.pair_copies(n), [self.hid_copy(n)]]
        groups += [self.cross_copies(0), self.own_copies()]
        for group in groups:
            for c in group:
                c.wait_send()

        def all_sent(group):
            for c in group:
                c.wait_send()

        for i in range(self.outer):
            self.each_return(i, all_sent, True)

        @pl.when(self.between)
        def _():
            all_sent(self.relay_copies())
            for i in range(1, self.outer):
                all_sent(self.cross_copies(i))
            for h in range(2):
                for i in range(self.outer - 1):
                    all_sent(self.ahead_copies(i, h))
            for c in range(2):
                for h in range(CUTS):
                    self.sum_copy(c, h).wait_send()

    def middle_only(self, *steps):
        @pl.when(self.between)
        def _():
            for step in steps:
                step()

    def end_only(self, step):
        @pl.when(self.at_end)
        def _():
            step()

    def relay(self, h):
        self.receive(self.mate, h)
        for c in self.relay_copies(h):
            c.start()

    def pass_on(self, i, h):
        self.receive(self.order[i], h)
        self.push(i, h)

    def run(self):
        for c in self.own_copies():
            c.start()
        self.wait_route()
        self.middle_only(lambda: self.push(0, 0))
        self.send_squares()
        self.select(0)
        self.middle_only(lambda: self.relay(0), lambda: self.pass_on(1, 0))
        self.send_scales()
        self.middle_only(
            lambda: self.relay(1), lambda: self.pass_on(1, 1), lambda: self.select(1)
        )
        shared = self.outer
        self.shared_gate_up()
        self.gate_up(0)
        self.pair(shared)
        self.pair(0)
        self.middle_only(
            lambda: self.pass_on(2, 0),
            lambda: self.pass_on(2, 1),
            lambda: self.push(0, 1),
            lambda: self.select(2),
            lambda: self.select(3),
        )
        self.gate_up(1)
        self.hidden(shared)
        self.hidden(0)
        self.pair(1)
        self.shared_down()
        self.down_rows(0)
        self.gate_up(2)
        self.hidden(1)
        self.pair(2)
        self.gate_up(3)
        self.down_rows(1)
        self.pair(3)
        self.hidden(2)
        self.end_only(lambda: self.bring_along(1))
        self.down_rows(2)
        self.hidden(3)
        self.end_only(lambda: self.bring_along(2))
        self.down_rows(3)
        self.collect(0)
        self.end_only(lambda: self.bring_along(3))
        self.middle_only(lambda: self.add_over(0), lambda: self.add_over(1))
        self.collect(1)
        self.close()
        self.finish()


def moe_scratch(n_sp, n_tp, inner, el, cap, tok, width, ff):
    outer, rw = n_sp // inner, el * cap
    assert inner * rw == tok
    vmem, dma = pltpu.VMEM, pltpu.SemaphoreType.DMA
    return {
        "wgu": vmem((el, width, 2 * ff), BF16),
        "wd": vmem((el, ff, width), BF16),
        "wsgu": vmem((width, 2 * ff), BF16),
        "wsd": vmem((ff, width), BF16),
        "dense": vmem((outer, tok, width), BF16),
        "ahead": vmem((outer - 1, inner, rw, width), BF16),
        "picked": vmem((outer, inner, rw, width), BF16),
        "rows": vmem((outer, inner, rw, width), BF16),
        "meta": vmem((n_sp, 8, tok), F32),
        "inv": vmem((n_sp, 8, tok), F32),
        "ssq": vmem((n_tp, 8, tok), F32),
        "gu": vmem((outer + 1, 2, tok // 2, 2 * ff), BF16),
        "parts": vmem((outer + 1, tok // 2, 2 * ff), BF16),
        "pairs": vmem((outer + 1, tok // 2, 2 * ff), BF16),
        "sides": vmem((outer + 1, n_tp // 2, tok // 2, 2 * ff), BF16),
        "hid": vmem((outer + 1, 2, tok // 2, ff), BF16),
        "outs": vmem((outer, inner, rw, width), BF16),
        "ret": vmem((n_sp, rw, width), BF16),
        "back": vmem((2, tok, inner * rw), BF16),
        "over": vmem((2, 2, inner, rw, width), BF16),
        "sums": vmem((2, tok, width), BF16),
        "far": vmem((tok, width), BF16),
        "acc": vmem((tok, width), F32),
        "w_sem": dma((6,)),
        "meta_s": dma((n_sp,)),
        "meta_r": dma((n_sp,)),
        "inv_s": dma((n_sp,)),
        "inv_r": dma((n_sp,)),
        "ssq_s": dma((n_tp,)),
        "ssq_r": dma((n_tp,)),
        "dense_s": dma((outer, 2)),
        "dense_r": dma((outer, 2)),
        "x_s": dma((outer, inner, 2)),
        "x_r": dma((outer, inner, 2)),
        "ahead_s": dma((outer - 1, inner, 2)),
        "part_s": dma((outer + 1,)),
        "part_r": dma((outer + 1,)),
        "pair_s": dma((outer + 1, n_tp // 2)),
        "pair_r": dma((outer + 1, n_tp // 2)),
        "hid_s": dma((outer + 1,)),
        "hid_r": dma((outer + 1,)),
        "ret_s": dma((outer, inner)),
        "ret_r": dma((n_sp,)),
        "beside": vmem((outer - 1, inner, rw, width), BF16),
        "beside_s": dma((outer - 1, inner, CUTS)),
        "beside_r": dma((outer - 1, inner, CUTS)),
        "ret_h": dma((inner, CUTS)),
        "over_s": dma((outer, inner, CUTS)),
        "over_r": dma((2, 2, inner, CUTS)),
        "sum_s": dma((2, CUTS)),
        "far_r": dma((CUTS,)),
    }


class Attend:
    def __init__(self, n_sp, n_tp, inner, refs):
        self.n_sp, self.n_tp, self.inner = n_sp, n_tp, inner
        self.outer = n_sp // inner
        self.__dict__.update(refs)
        self.own = lax.axis_index("sp")
        self.me = lax.axis_index("tp")
        self.z = self.own // inner
        self.x = self.own % inner
        self.order = plane_order(self.z, self.outer)
        self.heads, self.tok = self.bias.shape
        self.hd = self.queries.shape[1] // self.heads
        self.partner = self.me + 1 - 2 * (self.me % 2)
        self.peers = [(self.me + 2 * d) % n_tp for d in range(1, n_tp // 2)]

    def load(self):
        pairs = (
            (self.keys, self.kv),
            (self.values, self.vv),
            (self.queries, self.qv),
            (self.bias, self.bv),
        )
        self.loads = [
            pltpu.make_async_copy(src, dst, self.a_sem.at[i]) for i, (src, dst) in enumerate(pairs)
        ]
        for c in self.loads:
            c.start()

    def load_late(self):
        pairs = ((self.stream, self.sv), (self.out_proj, self.wo))
        self.late = [
            pltpu.make_async_copy(src, dst, self.a_sem.at[4 + i])
            for i, (src, dst) in enumerate(pairs)
        ]
        for c in self.late:
            c.start()

    def head_of(self, ref, head):
        return ref.at[:, pl.ds(pl.multiple_of(head * self.hd, self.hd), self.hd)]

    def exchange_copies(self, kind, i):
        src, dst = ((self.kv, self.kb), (self.vv, self.vb), (self.qv, self.qb))[kind]
        plane = self.order[i]
        target = dst.at[self.z, self.x] if kind < 2 else dst.at[self.z]
        return [
            rcopy(
                self.head_of(src, plane),
                target,
                self.e_s.at[kind, i],
                self.q_r.at[self.z] if kind == 2 else self.kv_r.at[kind, self.z, self.x],
                {"sp": plane * self.inner + self.x},
            )
        ]

    def side_copies(self, kind, i):
        dst = (self.kb, self.vb)[kind]
        plane = self.order[i]
        src = dst.at[plane, self.x] if i else self.head_of((self.kv, self.vv)[kind], self.z)
        return [
            rcopy(
                src,
                dst.at[plane, self.x],
                self.side_s.at[kind, i, d],
                self.kv_r.at[kind, plane, self.x],
                {"sp": self.z * self.inner + (self.x + d) % self.inner},
            )
            for d in range(1, self.inner)
        ]

    def wait_kv(self, kind, plane, x):
        dst = (self.kb, self.vb)[kind].at[plane, x]
        rcopy(
            dst, dst, self.e_s.at[kind, 0], self.kv_r.at[kind, plane, x], {"sp": (self.own + 1) % self.n_sp}
        ).wait_recv()

    def bias_copies(self):
        return [
            rcopy(
                self.bi.at[self.own],
                self.bi.at[self.own],
                self.bi_s.at[d],
                self.bi_r.at[self.own],
                {"sp": (self.own + d) % self.n_sp},
            )
            for d in range(1, self.n_sp)
        ]

    def exchange(self):
        for kind in range(3):
            self.loads[kind].wait()
            for i in range(self.outer - 1, 0, -1):
                for c in self.exchange_copies(kind, i):
                    c.start()
            if kind < 2:
                for c in self.side_copies(kind, 0):
                    c.start()
        self.loads[3].wait()
        self.bi[self.own, : self.heads, :] = self.bv[...].astype(F32)
        for c in self.bias_copies():
            c.start()
        self.kb[self.z, self.x] = self.head_of(self.kv, self.z)[...]
        self.vb[self.z, self.x] = self.head_of(self.vv, self.z)[...]
        self.qb[self.z] = self.head_of(self.qv, self.z)[...]

    def hand_over(self):
        for i in range(1, self.outer):
            for kind in range(2):
                self.wait_kv(kind, self.order[i], self.x)
                for c in self.side_copies(kind, i):
                    c.start()
        for d in range(1, self.n_sp):
            block = (self.own + d) % self.n_sp
            rcopy(
                self.bi.at[block],
                self.bi.at[block],
                self.bi_s.at[d],
                self.bi_r.at[block],
                {"sp": (self.own + 1) % self.n_sp},
            ).wait_recv()

    def compute(self):
        tok, hd = self.tok, self.hd
        scale = hd ** (-0.5)
        row = lax.broadcasted_iota(jnp.int32, (tok, tok), 0)
        col = lax.broadcasted_iota(jnp.int32, (tok, tok), 1)
        later = (row > col).astype(F32)
        sums = jnp.concatenate([later, jnp.ones((tok, tok), F32)], axis=1).astype(BF16)
        sums = jnp.concatenate([sums, sums], axis=0)
        for j in range(self.outer):
            for d in range(1, self.inner):
                for kind in range(2):
                    self.wait_kv(kind, j, (self.x + d) % self.inner)

            @pl.when(self.z != j)
            def _():
                rcopy(
                    self.qb.at[j], self.qb.at[j], self.e_s.at[2, 0], self.q_r.at[j], {"sp": (self.own + 1) % self.n_sp}
                ).wait_recv()

            q = self.qb[j]
            acc = jnp.zeros((tok, hd), F32)
            carry = jnp.zeros((tok, tok), F32)
            for k in range(j, -1, -1):
                for p in range(self.inner - 1, -1, -1):
                    bias = self.bi[k * self.inner + p, pl.ds(self.z, 1), :]
                    logit = rows_contract(q, self.kb[k, p]) * scale + bias
                    low = jnp.log(1.0 + jnp.exp(-jnp.abs(logit)))
                    fail = -(jnp.maximum(logit, 0.0) + low)
                    hit = jnp.minimum(logit, 0.0) - low
                    if k == j:
                        before = col < row + (self.x - p) * tok
                        fail = jnp.where(before, fail, 0.0)
                    high = fail.astype(BF16)
                    rest = (fail - high.astype(F32)).astype(BF16)
                    both = jnp.dot(
                        jnp.concatenate([high, rest], axis=1), sums, preferred_element_type=F32
                    )
                    w = jnp.exp(hit + both[:, :tok] + carry)
                    if k == j:
                        w = jnp.where(before, w, 0.0)
                    carry = carry + both[:, tok:]
                    acc = acc + jnp.dot(
                        w.astype(BF16), self.vb[k, p], preferred_element_type=F32
                    )
            self.ob[j] = acc.astype(BF16)

            @pl.when(self.z != j)
            def _():
                self.out_copy(j).start()

            @pl.when(self.z == j)
            def _():
                self.att[self.me, self.z] = self.ob[j]

    def out_copy(self, j):
        return rcopy(
            self.ob.at[j],
            self.att.at[self.me, self.z],
            self.o_s.at[j],
            self.att_r.at[self.me, self.z],
            {"sp": j * self.inner + self.x},
        )

    def wait_att(self, source, head):
        piece = self.att.at[source, head]
        rcopy(
            piece, piece, self.o_s.at[0], self.att_r.at[source, head], {"tp": (self.me + 1) % self.n_tp}
        ).wait_recv()

    def piece_copies(self, source, head, slot, targets):
        piece = self.att.at[source, head]
        return [
            rcopy(piece, piece, self.g_s.at[slot + n, head], self.att_r.at[source, head], {"tp": to})
            for n, to in enumerate(targets)
        ]

    def gather(self):
        wide = self.heads * self.hd

        def part(source):
            rows = jnp.concatenate([self.att[source, h] for h in range(self.outer)], axis=1)
            first = pl.multiple_of(source * wide, wide)
            return jnp.dot(rows, self.wo[pl.ds(first, wide), :], preferred_element_type=F32)

        slots = 1 + len(self.peers)
        for i in range(self.outer):
            head = self.order[i]
            if i:
                self.wait_att(self.me, head)
            for c in self.piece_copies(self.me, head, 0, self.peers + [self.partner]):
                c.start()
        for c in self.late:
            c.wait()
        self.acc[...] = self.sv[...].astype(F32) + part(self.me)
        for n, peer in enumerate(self.peers):
            for i in range(self.outer):
                self.wait_att(peer, self.order[i])
                for c in self.piece_copies(peer, self.order[i], slots + n, [self.partner]):
                    c.start()
        for i in range(self.outer):
            self.wait_att(self.partner, self.order[i])
        self.acc[...] += part(self.partner)
        for peer in self.peers:
            self.acc[...] += part(peer)
        others = [(self.partner + 2 * d) % self.n_tp for d in range(1, self.n_tp // 2)]
        for other in others:
            for i in range(self.outer):
                self.wait_att(other, self.order[i])
        total = self.acc[...]
        for other in others:
            total = total + part(other)
        self.mixed[...] = total.astype(BF16)

    def finish(self):
        groups = [self.bias_copies()]
        for i in range(1, self.outer):
            groups += [self.exchange_copies(kind, i) for kind in range(3)]
        for i in range(self.outer):
            groups += [self.side_copies(kind, i) for kind in range(2)]
            groups.append(
                self.piece_copies(self.me, self.order[i], 0, self.peers + [self.partner])
            )
            for n, peer in enumerate(self.peers):
                groups.append(
                    self.piece_copies(
                        peer, self.order[i], 1 + len(self.peers) + n, [self.partner]
                    )
                )
        for group in groups:
            for c in group:
                c.wait_send()
        for j in range(self.outer):

            @pl.when(self.z != j)
            def _():
                self.out_copy(j).wait_send()


LAYER_INPUTS = (
    "queries", "keys", "values", "bias", "stream", "out_proj", "gain_in", "ids_in", "wts_in",
    "gate", "up", "down", "s_gate", "s_up", "s_down",
)


def attend_scratch(n_sp, n_tp, inner, heads, hd, tok, width, top_k):
    outer = n_sp // inner
    vmem, dma = pltpu.VMEM, pltpu.SemaphoreType.DMA
    wide = heads * hd
    return {
        "qv": vmem((tok, wide), BF16),
        "kv": vmem((tok, wide), BF16),
        "vv": vmem((tok, wide), BF16),
        "bv": vmem((heads, tok), BF16),
        "sv": vmem((tok, width), BF16),
        "wo": vmem((n_tp * wide, width), BF16),
        "qb": vmem((outer, tok, hd), BF16),
        "kb": vmem((outer, inner, tok, hd), BF16),
        "vb": vmem((outer, inner, tok, hd), BF16),
        "bi": vmem((n_sp, 8, tok), F32),
        "ob": vmem((outer, tok, hd), BF16),
        "att": vmem((n_tp, outer, tok, hd), BF16),
        "mixed": vmem((tok, width), BF16),
        "gain": vmem((1, width), F32),
        "ids": vmem((top_k, tok), jnp.int32),
        "wts": vmem((top_k, tok), F32),
        "a_sem": dma((6,)),
        "s_sem": dma((3,)),
        "e_s": dma((3, outer)),
        "q_r": dma((outer,)),
        "kv_r": dma((2, outer, inner)),
        "side_s": dma((2, outer, inner)),
        "bi_s": dma((n_sp,)),
        "bi_r": dma((n_sp,)),
        "o_s": dma((outer,)),
        "att_r": dma((n_tp, outer)),
        "g_s": dma((n_tp, outer)),
    }


def layer_kernel(n_sp, n_tp, inner, el, cap, names, *refs):
    named = dict(zip(names, refs))
    first = Attend(n_sp, n_tp, inner, named)
    second = Experts(n_sp, n_tp, inner, el, cap, named)
    first.load()
    small = [
        pltpu.make_async_copy(named[name + "_in"], named[name], named["s_sem"].at[i])
        for i, name in enumerate(("ids", "wts", "gain"))
    ]
    for c in small:
        c.start()
    greet_all(n_sp, n_tp, first.own, first.me)
    first.load_late()
    second.load_weights()
    for c in small:
        c.wait()
    second.route()
    second.build_back()
    await_all(n_sp, n_tp)
    first.exchange()
    second.send_route()
    first.hand_over()
    first.compute()
    first.gather()
    second.run()
    first.finish()


def layer(operands, n_sp, n_tp, inner, cap, heads, hd):
    tok, width = operands[4].shape
    el, ff = operands[11].shape[:2]
    top_k = operands[7].shape[0]
    scratch = attend_scratch(n_sp, n_tp, inner, heads, hd, tok, width, top_k)
    scratch |= moe_scratch(n_sp, n_tp, inner, el, cap, tok, width, ff)
    hbm = pl.BlockSpec(memory_space=pltpu.MemorySpace.HBM)
    names = LAYER_INPUTS + ("out",) + tuple(scratch)
    return pl.pallas_call(
        functools.partial(layer_kernel, n_sp, n_tp, inner, el, cap, names),
        out_shape=jax.ShapeDtypeStruct((tok, width), BF16),
        in_specs=[hbm] * len(operands),
        out_specs=pl.BlockSpec(memory_space=pltpu.VMEM),
        scratch_shapes=list(scratch.values()),
        compiler_params=pltpu.CompilerParams(
            vmem_limit_bytes=56 * 2**20, collective_id=0, has_side_effects=True
        ),
        cost_estimate=pl.CostEstimate(flops=10**10, bytes_accessed=2**24, transcendentals=10**6),
    )(*operands)


def body(
    queries,
    key_rows,
    value_rows,
    break_bias,
    stream,
    out_proj,
    norm_gain,
    expert_ids,
    route_weights,
    gate_proj,
    up_proj,
    down_proj,
    shared_gate,
    shared_up,
    shared_down,
):
    tok = queries.shape[0]
    heads = break_bias.shape[1]
    hd = queries.shape[1] // heads
    n_sp = lax.axis_size("sp")
    n_tp = lax.axis_size("tp")
    width = stream.shape[1] * n_tp

    bias_wide = jnp.pad(break_bias, ((0, 0), (0, hd - heads)))

    experts_local = gate_proj.shape[0]
    experts = experts_local * n_sp
    top_k = expert_ids.shape[1]
    cap = 2 * top_k * tok // experts
    n_inner = max(d for d in range(1, n_sp + 1) if n_sp % d == 0 and d * d <= n_sp)
    plane_rows = n_inner * experts_local * cap
    if heads * n_inner == n_sp and heads == 4 and plane_rows == tok and cap % 16 == 0 and tok % (16 * n_tp) == 0:
        operands = (
            queries, key_rows, value_rows, break_bias.T, stream, out_proj, norm_gain[None, :],
            expert_ids.T, route_weights.T, gate_proj, up_proj, down_proj,
            shared_gate, shared_up, shared_down,
        )
        return layer(operands, n_sp, n_tp, n_inner, cap, heads, hd)
    expert_of = jnp.arange(experts, dtype=jnp.int32)
    named = expert_ids[:, :, None] == expert_of[None, None, :]
    named_any = jnp.any(named, axis=1).astype(BF16)
    token = jnp.arange(tok, dtype=jnp.int32)
    earlier = (token[None, :] < token[:, None]).astype(BF16)
    rank_all = jnp.dot(earlier, named_any, preferred_element_type=F32)
    rank = jnp.sum(jnp.where(named, rank_all[:, None, :], 0.0), axis=2).astype(jnp.int32)
    slot = expert_ids * cap + rank
    slots = experts * cap
    place = jnp.arange(slots, dtype=jnp.int32)
    spot = slot[:, :, None] == place[None, None, :]
    send_pick = jnp.any(spot, axis=1).astype(BF16)
    back_pick = jnp.sum(jnp.where(spot, route_weights[:, :, None], 0.0), axis=1).astype(BF16)

    attended = attention(queries, key_rows, value_rows, bias_wide, heads, hd, n_sp)
    projected = jnp.dot(
        lax.all_gather(attended, "tp", axis=1, tiled=True), out_proj, preferred_element_type=F32
    )
    mixed = (stream.astype(F32) + projected).astype(BF16)
    mixed = lax.optimization_barrier(mixed)
    mixed_f = mixed.astype(F32)
    square_sum = lax.psum(jnp.sum(mixed_f * mixed_f, axis=1), "tp")
    inv_rms = lax.rsqrt(square_sum / width + EPS)
    normed = (mixed_f * inv_rms[:, None] * norm_gain[None, :]).astype(BF16)

    send = lax.dot_general(
        send_pick, normed, (((0,), (0,)), ((), ())), preferred_element_type=F32
    ).astype(BF16)
    send = send.reshape(n_sp, experts_local * cap, normed.shape[1])
    arrived = lax.all_to_all(send, "sp", split_axis=0, concat_axis=0, tiled=True)
    arrived = arrived.reshape(n_sp, experts_local, cap, -1)
    gates, ups = [], []
    for e in range(experts_local):
        rows = arrived[:, e].reshape(n_sp * cap, -1)
        gates.append(jnp.dot(rows, gate_proj[e], preferred_element_type=F32).astype(BF16))
        ups.append(jnp.dot(rows, up_proj[e], preferred_element_type=F32).astype(BF16))
    gates.append(jnp.dot(normed, shared_gate, preferred_element_type=F32).astype(BF16))
    ups.append(jnp.dot(normed, shared_up, preferred_element_type=F32).astype(BF16))
    gate_all = jnp.concatenate(gates, axis=0)
    up_all = jnp.concatenate(ups, axis=0)
    gate_up = jnp.concatenate([gate_all, up_all], axis=1)
    hidden = exchange(gate_up, n_tp)
    outs = []
    for e in range(experts_local):
        rows = hidden[e * n_sp * cap : (e + 1) * n_sp * cap]
        out = jnp.dot(rows, down_proj[e], preferred_element_type=F32).astype(BF16)
        outs.append(out.reshape(n_sp, 1, cap, -1))
    expert_out = jnp.concatenate(outs, axis=1).reshape(n_sp, experts_local * cap, -1)
    returned = lax.all_to_all(expert_out, "sp", split_axis=0, concat_axis=0, tiled=True)
    returned = returned.reshape(slots, -1)
    shared_out = jnp.dot(
        hidden[experts_local * n_sp * cap :], shared_down, preferred_element_type=F32
    )
    routed = jnp.dot(back_pick, returned, preferred_element_type=F32)
    return (mixed_f + shared_out + routed).astype(BF16)


def solution(mesh):
    in_specs = (
        P("sp", "tp"),
        P("sp", "tp"),
        P("sp", "tp"),
        P("sp", "tp"),
        P("sp", "tp"),
        P(None, "tp"),
        P("tp"),
        P("sp", None),
        P("sp", None),
        P("sp", "tp", None),
        P("sp", "tp", None),
        P("sp", None, "tp"),
        P("tp", None),
        P("tp", None),
        P(None, "tp"),
    )
    return jax.shard_map(body, mesh=mesh, in_specs=in_specs, out_specs=P("sp", "tp"), check_vma=False)
```

```python
import functools

import jax
import jax.numpy as jnp
from jax import lax
from jax.experimental import pallas as pl
from jax.experimental.pallas import tpu as pltpu
from jax.sharding import PartitionSpec as P

EPS = 1e-06
F32 = jnp.float32
BF16 = jnp.bfloat16


def attention_kernel(
    heads, hd, n_sp, inner, q_ref, k_ref, v_ref, b_ref, o_ref, kbuf, vbuf, bbuf, acc, carry, send_sem, recv_sem
):
    tok = q_ref.shape[0]
    own = lax.axis_index("sp")
    outer = n_sp // inner
    z_own = own // inner
    x_own = own % inner
    above = z_own < outer - 1
    below = z_own > 0

    barrier = pltpu.get_barrier_semaphore()

    def greet(target):
        pl.semaphore_signal(
            barrier, inc=1, device_id={"sp": target}, device_id_type=pl.DeviceIdType.MESH
        )

    @pl.when(above)
    def _():
        greet(own + inner)

    @pl.when(below)
    def _():
        greet(own - inner)

    for d in range(1, inner):
        greet(z_own * inner + (x_own + d) % inner)
    pl.semaphore_wait(barrier, inner - 1 + above.astype(jnp.int32) + below.astype(jnp.int32))

    def copies(sources, block, z_block, lane, target):
        return [
            pltpu.make_async_remote_copy(
                src_ref=src,
                dst_ref=dst.at[block],
                send_sem=send_sem.at[kind, z_block, lane],
                recv_sem=recv_sem.at[kind, block],
                device_id={"sp": target},
                device_id_type=pl.DeviceIdType.MESH,
            )
            for kind, (src, dst) in enumerate(zip(sources, (kbuf, vbuf, bbuf)))
        ]

    def held(block):
        return (kbuf.at[block], vbuf.at[block], bbuf.at[block])

    def start_all(group):
        for c in group:
            c.start()

    def wait_sent(group):
        for c in group:
            c.wait_send()

    def wait_arrived(block):
        for c in copies(held(block), block, 0, 0, (own + 1) % n_sp):
            c.wait_recv()

    def own_sends(act):
        mine = (k_ref, v_ref, b_ref)

        @pl.when(above)
        def _():
            act(copies(mine, own, z_own, 0, own + inner))

        for d in range(1, inner):
            x_to = (x_own + d) % inner

            @pl.when(x_to > x_own)
            def _():
                act(copies(mine, own, z_own, d, z_own * inner + x_to))

    def relays(z_block, act):
        block = z_block * inner + x_own

        @pl.when(above)
        def _():
            act(copies(held(block), block, z_block, 0, own + inner))

        for d in range(1, inner):
            act(copies(held(block), block, z_block, d, z_own * inner + (x_own + d) % inner))

    own_sends(start_all)

    scale = hd ** (-0.5)
    row = lax.broadcasted_iota(jnp.int32, (tok, tok), 0)
    col = lax.broadcasted_iota(jnp.int32, (tok, tok), 1)
    later = (row > col).astype(F32)
    sums = jnp.concatenate([later, jnp.ones((tok, tok), F32)], axis=1).astype(BF16)
    sums = jnp.concatenate([sums, sums], axis=0)
    pick_rows = max(16, heads)
    pick = (
        lax.broadcasted_iota(jnp.int32, (pick_rows, hd), 0)
        == lax.broadcasted_iota(jnp.int32, (pick_rows, hd), 1)
    ).astype(F32).astype(BF16)
    acc[...] = jnp.zeros_like(acc)
    carry[...] = jnp.zeros_like(carry)

    def compute(keys, values, offsets, diagonal):
        bias = lax.dot_general(
            pick, offsets[...], (((1,), (1,)), ((), ())), preferred_element_type=F32
        )
        for h in range(heads):
            cols = slice(h * hd, (h + 1) * hd)
            z = lax.dot_general(
                q_ref[:, cols], keys[:, cols], (((1,), (1,)), ((), ())), preferred_element_type=F32
            )
            z = z * scale + bias[h : h + 1, :]
            low = jnp.log1p(jnp.exp(-jnp.abs(z)))
            fail = -(jnp.maximum(z, 0.0) + low)
            hit = jnp.minimum(z, 0.0) - low
            if diagonal:
                before = col < row
                fail = jnp.where(before, fail, 0.0)
            high = fail.astype(BF16)
            rest = (fail - high.astype(F32)).astype(BF16)
            both = jnp.dot(
                jnp.concatenate([high, rest], axis=1), sums, preferred_element_type=F32
            )
            before_sum = carry[h]
            w = jnp.exp(hit + both[:, :tok] + before_sum)
            if diagonal:
                w = jnp.where(before, w, 0.0)
            carry[h] = before_sum + both[:, tok:]
            acc[:, cols] += jnp.dot(w.astype(BF16), values[:, cols], preferred_element_type=F32)

    compute(k_ref, v_ref, b_ref, True)

    def group(i, _):
        z_block = z_own - i

        @pl.when(z_block > 0)
        def _():
            wait_arrived((z_block - 1) * inner + x_own)
            relays(z_block - 1, start_all)

        def member(m, _):
            x_block = inner - 1 - m
            block = z_block * inner + x_block

            @pl.when(block < own)
            def _():
                @pl.when(x_block != x_own)
                def _():
                    wait_arrived(block)

                compute(*held(block), False)

            return 0

        lax.fori_loop(0, inner, member, 0)
        return 0

    lax.fori_loop(0, z_own + 1, group, 0)
    o_ref[...] = acc[...].astype(BF16)

    own_sends(wait_sent)

    def drain(z_block, _):
        relays(z_block, wait_sent)
        return 0

    lax.fori_loop(0, z_own, drain, 0)


def attention(queries, keys, values, bias, heads, hd, n_sp):
    tok = queries.shape[0]
    inner = max(d for d in range(1, n_sp + 1) if n_sp % d == 0 and d * d <= n_sp)
    vmem = pl.BlockSpec(memory_space=pltpu.VMEM)
    return pl.pallas_call(
        functools.partial(attention_kernel, heads, hd, n_sp, inner),
        out_shape=jax.ShapeDtypeStruct((tok, heads * hd), BF16),
        in_specs=[vmem] * 4,
        out_specs=vmem,
        scratch_shapes=[
            pltpu.VMEM((n_sp, tok, heads * hd), BF16),
            pltpu.VMEM((n_sp, tok, heads * hd), BF16),
            pltpu.VMEM((n_sp, tok, hd), BF16),
            pltpu.VMEM((tok, heads * hd), F32),
            pltpu.VMEM((heads, tok, tok), F32),
            pltpu.SemaphoreType.DMA((3, n_sp // inner, inner)),
            pltpu.SemaphoreType.DMA((3, n_sp)),
        ],
        compiler_params=pltpu.CompilerParams(
            vmem_limit_bytes=40 * 2**20, collective_id=0, has_side_effects=True
        ),
        cost_estimate=pl.CostEstimate(flops=2 * 10**9, bytes_accessed=2**22, transcendentals=10**6),
    )(queries, keys, values, bias)


def exchange_kernel(n_tp, gu_ref, o_ref, parts, mine, spread, send_parts, recv_parts, send_rows, recv_rows):
    width = gu_ref.shape[2] // 2
    me = lax.axis_index("tp")
    barrier = pltpu.get_barrier_semaphore()
    others = [(me + d) % n_tp for d in range(1, n_tp)]
    for to in others:
        pl.semaphore_signal(
            barrier, inc=1, device_id={"tp": to}, device_id_type=pl.DeviceIdType.MESH
        )
    pl.semaphore_wait(barrier, n_tp - 1)
    first, second = [], []
    for d, to in enumerate(others):
        copy = pltpu.make_async_remote_copy(
            src_ref=gu_ref.at[to],
            dst_ref=parts.at[d],
            send_sem=send_parts.at[d],
            recv_sem=recv_parts.at[d],
            device_id={"tp": to},
            device_id_type=pl.DeviceIdType.MESH,
        )
        copy.start()
        first.append(copy)
    total = gu_ref[me].astype(F32)
    for d, copy in enumerate(first):
        copy.wait_recv()
        total = total + parts[d].astype(F32)
    gate = total[:, :width]
    mine[...] = (jax.nn.silu(gate) * total[:, width:]).astype(BF16)
    for d, to in enumerate(others):
        copy = pltpu.make_async_remote_copy(
            src_ref=mine,
            dst_ref=spread.at[d],
            send_sem=send_rows.at[d],
            recv_sem=recv_rows.at[d],
            device_id={"tp": to},
            device_id_type=pl.DeviceIdType.MESH,
        )
        copy.start()
        second.append(copy)
    o_ref[me] = mine[...]
    for d, copy in enumerate(second):
        copy.wait_recv()
        o_ref[(me + n_tp - 1 - d) % n_tp] = spread[d]
    for copy in first + second:
        copy.wait_send()


def exchange(gate_up, n_tp):
    rows, width = gate_up.shape[0] // n_tp, gate_up.shape[1] // 2
    vmem = pl.BlockSpec(memory_space=pltpu.VMEM)
    dma = pltpu.SemaphoreType.DMA((n_tp - 1,))
    hidden = pl.pallas_call(
        functools.partial(exchange_kernel, n_tp),
        out_shape=jax.ShapeDtypeStruct((n_tp, rows, width), BF16),
        in_specs=[vmem],
        out_specs=vmem,
        scratch_shapes=[
            pltpu.VMEM((n_tp - 1, rows, 2 * width), BF16),
            pltpu.VMEM((rows, width), BF16),
            pltpu.VMEM((n_tp - 1, rows, width), BF16),
            dma,
            dma,
            dma,
            dma,
        ],
        compiler_params=pltpu.CompilerParams(
            vmem_limit_bytes=24 * 2**20, collective_id=1, has_side_effects=True
        ),
        cost_estimate=pl.CostEstimate(flops=10**8, bytes_accessed=2**21, transcendentals=10**5),
    )(gate_up.reshape(n_tp, rows, 2 * width))
    return hidden.reshape(n_tp * rows, width)


MESH = pl.DeviceIdType.MESH
CUTS = 4


def rows_contract(lhs, rhs):
    return lax.dot_general(lhs, rhs, (((1,), (1,)), ((), ())), preferred_element_type=F32)


def rcopy(src, dst, send_sem, recv_sem, where):
    return pltpu.make_async_remote_copy(
        src_ref=src,
        dst_ref=dst,
        send_sem=send_sem,
        recv_sem=recv_sem,
        device_id=where,
        device_id_type=MESH,
    )


def plane_order(z, outer):
    step = 1 - 2 * ((2 * z) // outer)
    return [(z + step * i + outer) % outer for i in range(outer)]


def greet_all(n_sp, n_tp, own, me):
    barrier = pltpu.get_barrier_semaphore()
    for d in range(1, n_sp):
        pl.semaphore_signal(
            barrier, inc=1, device_id={"sp": (own + d) % n_sp}, device_id_type=MESH
        )
    for d in range(1, n_tp):
        pl.semaphore_signal(
            barrier, inc=1, device_id={"tp": (me + d) % n_tp}, device_id_type=MESH
        )


def await_all(n_sp, n_tp):
    pl.semaphore_wait(pltpu.get_barrier_semaphore(), n_sp + n_tp - 2)


class Experts:
    def __init__(self, n_sp, n_tp, inner, experts_local, cap, refs):
        self.n_sp, self.n_tp, self.inner = n_sp, n_tp, inner
        self.outer = n_sp // inner
        self.el, self.cap = experts_local, cap
        self.rw = experts_local * cap
        self.__dict__.update(refs)
        self.own = lax.axis_index("sp")
        self.me = lax.axis_index("tp")
        self.z = self.own // inner
        self.x = self.own % inner
        self.side = self.z // 2
        self.within = self.z % 2
        self.mate = self.z + 1 - 2 * self.within
        self.middle = 1 + self.side
        self.order = [self.z, 2 - self.side, 3 - 3 * self.side, self.mate]
        self.core = self.me % 2
        self.partner = self.me + 1 - 2 * self.core
        self.chip = self.me // 2
        self.between = (self.z > 0) & (self.z < self.outer - 1)
        self.at_end = jnp.logical_not(self.between)
        self.tok, self.width = self.mixed.shape
        self.ff = self.down.shape[1]
        self.total_width = self.width * n_tp

    def load_weights(self):
        ff = self.ff
        self.loads = [
            pltpu.make_async_copy(src, dst, self.w_sem.at[i])
            for i, (src, dst) in enumerate(
                (
                    (self.s_gate, self.wsgu.at[:, pl.ds(0, ff)]),
                    (self.s_up, self.wsgu.at[:, pl.ds(ff, ff)]),
                    (self.gate, self.wgu.at[:, :, pl.ds(0, ff)]),
                    (self.up, self.wgu.at[:, :, pl.ds(ff, ff)]),
                    (self.down, self.wd),
                    (self.s_down, self.wsd),
                )
            )
        ]
        for load in self.loads:
            load.start()

    def meta_copies(self, ref, send, recv):
        return [
            rcopy(
                ref.at[self.own],
                ref.at[self.own],
                send.at[d],
                recv.at[self.own],
                {"sp": (self.own + d) % self.n_sp},
            )
            for d in range(1, self.n_sp)
        ]

    def wait_table(self, ref, send, recv, block):
        rcopy(
            ref.at[block], ref.at[block], send.at[0], recv.at[block], {"sp": (self.own + 1) % self.n_sp}
        ).wait_recv()

    def route(self):
        ids = self.ids[...]
        experts = self.el * self.n_sp
        top_k, tok = ids.shape
        expert_of = lax.broadcasted_iota(jnp.int32, (experts, tok), 0)
        named = [ids[k : k + 1, :] == expert_of for k in range(top_k)]
        named_any = functools.reduce(jnp.logical_or, named).astype(F32).astype(BF16)
        before = (
            lax.broadcasted_iota(jnp.int32, (tok, tok), 0)
            < lax.broadcasted_iota(jnp.int32, (tok, tok), 1)
        ).astype(F32).astype(BF16)
        rank = jnp.dot(named_any, before, preferred_element_type=F32)
        self.meta[self.own] = jnp.zeros((8, tok), F32)
        for k in range(top_k):
            mine = jnp.sum(jnp.where(named[k], rank, 0.0), axis=0, keepdims=True)
            slot = ids[k : k + 1, :].astype(F32) * self.cap + mine
            self.meta[self.own, k : k + 1, :] = slot
            self.meta[self.own, top_k + k : top_k + k + 1, :] = self.wts[k : k + 1, :]
        self.top_k = top_k

    def send_route(self):
        self.meta_group = self.meta_copies(self.meta, self.meta_s, self.meta_r)
        for c in self.meta_group:
            c.start()

    def wait_route(self):
        for d in range(1, self.n_sp):
            self.wait_table(self.meta, self.meta_s, self.meta_r, (self.own + d) % self.n_sp)

    def slot_hits(self, block, first, count):
        spot = (
            lax.broadcasted_iota(jnp.int32, (count, self.tok), 0) + first
        ).astype(F32)
        return [self.meta[block, k : k + 1, :] == spot for k in range(self.top_k)]

    def back_of(self, block, plane):
        rows = self.inner * self.rw
        hits = self.slot_hits(block, plane * rows, rows)
        weight = sum(
            jnp.where(
                hits[k], self.meta[block, self.top_k + k : self.top_k + k + 1, :], 0.0
            )
            for k in range(self.top_k)
        )
        return jnp.transpose(weight).astype(BF16)

    def build_back(self):
        self.back[0] = self.back_of(self.own, self.z)
        self.back[1] = self.back_of(self.own, self.mate)

    def halves(self):
        half = self.width // 2
        return [pl.ds(h * half, half) for h in range(2)]

    def dense_copies(self, src, plane, target, only=None):
        return [
            rcopy(
                src.at[:, cols],
                self.dense.at[plane, :, cols],
                self.dense_s.at[plane, h],
                self.dense_r.at[plane, h],
                {"sp": target * self.inner + self.x},
            )
            for h, cols in enumerate(self.halves())
            if only is None or h == only
        ]

    def own_copies(self):
        at_end = self.at_end.astype(jnp.int32)
        target = at_end * self.mate + (1 - at_end) * (3 - self.z)
        return self.dense_copies(self.mixed, self.z, target)

    def relay_copies(self, only=None):
        return self.dense_copies(self.dense.at[self.mate], self.mate, 3 - self.z, only)

    def receive(self, plane, h):
        piece = self.dense.at[plane, :, self.halves()[h]]
        rcopy(
            piece, piece, self.dense_s.at[plane, h], self.dense_r.at[plane, h], {"sp": (self.own + 1) % self.n_sp}
        ).wait_recv()

    def pick_rows(self, block, plane):
        rows = self.inner * self.rw
        hits = self.slot_hits(block, plane * rows, rows)
        return functools.reduce(jnp.logical_or, hits).astype(F32).astype(BF16)

    def ahead_copies(self, i, h):
        cols = self.halves()[h]
        return [
            rcopy(
                self.ahead.at[i, (self.x + d) % self.inner, :, cols],
                self.rows.at[i or 3, self.x, :, cols],
                self.ahead_s.at[i, d, h],
                self.x_r.at[i or 3, self.x, h],
                {"sp": self.mate * self.inner + (self.x + d) % self.inner},
            )
            for d in range(self.inner)
        ]

    def push(self, i, h):
        cols = self.halves()[h]
        pick = self.pick_rows(self.order[i] * self.inner + self.x, self.mate)
        source = self.dense[self.order[i], :, cols] if i else self.mixed[:, cols]
        got = jnp.dot(pick, source, preferred_element_type=F32).astype(BF16)
        for p in range(self.inner):
            self.ahead[i, p, :, cols] = got[p * self.rw : (p + 1) * self.rw]
        for c in self.ahead_copies(i, h):
            c.start()

    def cross_copies(self, i):
        return [
            rcopy(
                self.picked.at[i, (self.x + d) % self.inner, :, cols],
                self.rows.at[i, self.x, :, cols],
                self.x_s.at[i, d, h],
                self.x_r.at[i, self.x, h],
                {"sp": self.z * self.inner + (self.x + d) % self.inner},
            )
            for h, cols in enumerate(self.halves())
            for d in range(1, self.inner)
        ]

    def select(self, i):
        pick = self.pick_rows(self.order[i] * self.inner + self.x, self.z)
        source = self.dense[self.order[i]] if i else self.mixed[...]
        got = jnp.dot(pick, source, preferred_element_type=F32).astype(BF16)
        for p in range(self.inner):
            self.picked[i, p] = got[p * self.rw : (p + 1) * self.rw]
        for c in self.cross_copies(i):
            c.start()
        self.rows[i, self.x] = self.picked[i, self.x]

    def wait_rows(self, i):
        def arrived(x_from):
            for h, cols in enumerate(self.halves()):
                piece = self.rows.at[i, x_from, :, cols]
                rcopy(
                    piece,
                    piece,
                    self.x_s.at[i, 0, h],
                    self.x_r.at[i, x_from, h],
                    {"sp": (self.own + 1) % self.n_sp},
                ).wait_recv()

        if i:

            @pl.when(self.at_end)
            def _():
                arrived(self.x)

        for d in range(1, self.inner):
            arrived((self.x + d) % self.inner)

    def tp_copies(self, src, dst, send, recv):
        return [
            rcopy(src(to), dst, send.at[d], recv.at[self.me], {"tp": to})
            for d, to in ((d, (self.me + d) % self.n_tp) for d in range(1, self.n_tp))
        ]

    def tp_wait(self, dst, send, recv):
        for d in range(1, self.n_tp):
            other = (self.me + d) % self.n_tp
            rcopy(
                dst(other), dst(other), send.at[0], recv.at[other], {"tp": (self.me + 1) % self.n_tp}
            ).wait_recv()

    def send_squares(self):
        wide = self.mixed[...].astype(F32)
        column = jnp.sum(wide * wide, axis=1, keepdims=True)
        row = jnp.transpose(jnp.broadcast_to(column, (self.tok, self.tok)))
        self.ssq[self.me] = row[:8]
        self.ssq_group = self.tp_copies(
            lambda to: self.ssq.at[self.me], self.ssq.at[self.me], self.ssq_s, self.ssq_r
        )
        for c in self.ssq_group:
            c.start()

    def send_scales(self):
        self.tp_wait(lambda other: self.ssq.at[other], self.ssq_s, self.ssq_r)
        total = self.ssq[0]
        for p in range(1, self.n_tp):
            total = total + self.ssq[p]
        self.inv[self.own] = lax.rsqrt(total / self.total_width + EPS)
        self.inv_group = self.meta_copies(self.inv, self.inv_s, self.inv_r)
        for c in self.inv_group:
            c.start()

    def part_copy(self, s):
        return rcopy(
            self.gu.at[s, 1 - self.core],
            self.parts.at[s],
            self.part_s.at[s],
            self.part_r.at[s],
            {"tp": self.partner},
        )

    def pair_copies(self, s):
        return [
            rcopy(
                self.pairs.at[s],
                self.sides.at[s, self.chip],
                self.pair_s.at[s, d],
                self.pair_r.at[s, self.chip],
                {"tp": (self.me + 2 * d) % self.n_tp},
            )
            for d in range(1, self.n_tp // 2)
        ]

    def hid_copy(self, s):
        mine = self.hid.at[s, self.core]
        return rcopy(
            mine, mine, self.hid_s.at[s], self.hid_r.at[s], {"tp": self.partner}
        )

    def send_parts(self, s, value):
        half = value.shape[0] // 2
        for c in range(2):
            self.gu[s, c] = value[c * half : (c + 1) * half]
        self.part_copy(s).start()

    def pair(self, s):
        self.part_copy(s).wait_recv()
        self.pairs[s] = (
            self.gu[s, self.core].astype(F32) + self.parts[s].astype(F32)
        ).astype(BF16)
        for c in self.pair_copies(s):
            c.start()

    def gate_up(self, i):
        if i == 0:
            self.loads[2].wait()
            self.loads[3].wait()
        self.wait_rows(i)
        normed = []
        for d in range(self.inner):
            block = self.order[i] * self.inner + (self.x + d) % self.inner
            if i or d:
                self.wait_table(self.inv, self.inv_s, self.inv_r, block)
        for p in range(self.inner):
            block = self.order[i] * self.inner + p
            hits = self.slot_hits(block, self.own * self.rw, self.rw)
            pick = functools.reduce(jnp.logical_or, hits)
            scale = jnp.sum(
                jnp.where(pick, self.inv[block, 0:1, :], 0.0), axis=1, keepdims=True
            )
            wide = self.rows[i, p].astype(F32)
            normed.append((wide * scale * self.gain[...]).astype(BF16))
        out = []
        for e in range(self.el):
            rows = jnp.concatenate(
                [n[e * self.cap : (e + 1) * self.cap] for n in normed], axis=0
            )
            out.append(jnp.dot(rows, self.wgu[e], preferred_element_type=F32).astype(BF16))
        self.send_parts(i, jnp.concatenate(out, axis=0))

    def shared_gate_up(self):
        self.loads[0].wait()
        self.loads[1].wait()
        scale = jnp.transpose(jnp.broadcast_to(self.inv[self.own, 0:1, :], (self.tok, self.tok)))
        normed = (
            self.mixed[...].astype(F32) * scale[:, 0:1] * self.gain[...]
        ).astype(BF16)
        value = jnp.dot(normed, self.wsgu[...], preferred_element_type=F32).astype(BF16)
        self.send_parts(self.outer, value)

    def hidden(self, s):
        total = self.pairs[s].astype(F32)
        for d in range(1, self.n_tp // 2):
            other = (self.chip + d) % (self.n_tp // 2)
            rcopy(
                self.sides.at[s, other],
                self.sides.at[s, other],
                self.pair_s.at[s, d],
                self.pair_r.at[s, other],
                {"tp": self.partner},
            ).wait_recv()
            total = total + self.sides[s, other].astype(F32)
        act = jax.nn.silu(total[:, : self.ff]) * total[:, self.ff :]
        self.hid[s, self.core] = act.astype(BF16)
        self.hid_copy(s).start()

    def all_hidden(self, s):
        other = self.hid.at[s, 1 - self.core]
        rcopy(other, other, self.hid_s.at[s], self.hid_r.at[s], {"tp": self.partner}).wait_recv()
        return jnp.concatenate([self.hid[s, c] for c in range(2)], axis=0)

    def cuts(self):
        cut = self.width // CUTS
        return [pl.ds(h * cut, cut) for h in range(CUTS)]

    def return_copies(self, i):
        return [
            rcopy(
                self.outs.at[i, (self.x + d) % self.inner],
                self.ret.at[self.own],
                self.ret_s.at[i, d],
                self.ret_r.at[self.own],
                {"sp": self.order[i] * self.inner + (self.x + d) % self.inner},
            )
            for d in range(0 if i else 1, self.inner)
        ]

    def over_copies(self, i, c, first):
        return [
            rcopy(
                self.outs.at[i, (self.x + d) % self.inner, :, cols],
                self.over.at[c, self.within, self.x, :, cols],
                self.over_s.at[i, d, h],
                self.over_r.at[c, self.within, self.x, h],
                {"sp": self.middle * self.inner + (self.x + d) % self.inner},
            )
            for h, cols in enumerate(self.cuts())
            for d in range(first, self.inner)
        ]

    def side_out_copies(self, i):
        return [
            rcopy(
                self.outs.at[i, (self.x + d) % self.inner, :, cols],
                self.beside.at[i - 1, self.x, :, cols],
                self.beside_s.at[i - 1, d, h],
                self.beside_r.at[i - 1, self.x, h],
                {"sp": self.z * self.inner + (self.x + d) % self.inner},
            )
            for h, cols in enumerate(self.cuts())
            for d in range(1, self.inner)
        ]

    def column_copies(self, i, d, h):
        cols = self.cuts()[h]
        x_of = (self.x + d) % self.inner
        src = self.beside.at[i - 1, x_of, :, cols] if d else self.outs.at[i, self.x, :, cols]
        if i == 3:
            dst = self.ret.at[self.z * self.inner + x_of, :, cols]
            arrived = self.ret_h.at[x_of, h]
        else:
            dst = self.over.at[i - 1, self.within, x_of, :, cols]
            arrived = self.over_r.at[i - 1, self.within, x_of, h]
        return [
            rcopy(src, dst, self.over_s.at[i, d, h], arrived, {"sp": self.mate * self.inner + self.x})
        ]

    def bring_along(self, i):
        for h, cols in enumerate(self.cuts()):
            for d in range(1, self.inner):
                x_of = (self.x + d) % self.inner
                piece = self.beside.at[i - 1, x_of, :, cols]
                rcopy(
                    piece,
                    piece,
                    self.beside_s.at[i - 1, d, h],
                    self.beside_r.at[i - 1, x_of, h],
                    {"sp": (self.own + 1) % self.n_sp},
                ).wait_recv()
                for c in self.column_copies(i, d, h):
                    c.start()

    def each_return(self, i, act, sent=False):
        if i == 0:
            act(self.return_copies(0))
            return

        @pl.when(self.at_end)
        def _():
            act(self.side_out_copies(i))
            for h in range(CUTS):
                for d in range(self.inner if sent else 1):
                    act(self.column_copies(i, d, h))

        @pl.when(self.between)
        def _():
            act(self.over_copies(i, i - 1, 1) if i < 3 else self.return_copies(i))

    def sum_copy(self, c, h):
        cols = self.cuts()[h]
        return rcopy(
            self.sums.at[c, :, cols],
            self.far.at[:, cols],
            self.sum_s.at[c, h],
            self.far_r.at[h],
            {"sp": self.order[c + 1] * self.inner + self.x},
        )

    def add_over(self, c):
        block = self.order[c + 1] * self.inner + self.x
        pair = 2 * self.side
        backs = [self.back_of(block, pair + s) for s in range(2)]
        for h, cols in enumerate(self.cuts()):

            def arrived(s, x_from):
                piece = self.over.at[c, s, x_from, :, cols]
                rcopy(
                    piece,
                    piece,
                    self.over_s.at[0, 0, h],
                    self.over_r.at[c, s, x_from, h],
                    {"sp": (self.own + 1) % self.n_sp},
                ).wait_recv()

            total = 0.0
            for s in range(2):
                for d in range(1, self.inner):
                    arrived(s, (self.x + d) % self.inner)

                @pl.when(self.within != s)
                def _():
                    arrived(s, self.x)

                rows = jnp.concatenate(
                    [self.over[c, s, p, :, cols] for p in range(self.inner)], axis=0
                )
                total = total + jnp.dot(backs[s], rows, preferred_element_type=F32)
            self.sums[c, :, cols] = total.astype(BF16)
            self.sum_copy(c, h).start()

    def down_rows(self, i):
        if i == 0:
            self.loads[4].wait()
        hidden = self.all_hidden(i)
        span = self.inner * self.cap
        for e in range(self.el):
            out = jnp.dot(
                hidden[e * span : (e + 1) * span], self.wd[e], preferred_element_type=F32
            ).astype(BF16)
            for p in range(self.inner):
                self.outs[i, p, e * self.cap : (e + 1) * self.cap, :] = out[
                    p * self.cap : (p + 1) * self.cap
                ]

        def start(group):
            for c in group:
                c.start()

        self.each_return(i, start)
        if i == 0:
            self.ret[self.own] = self.outs[0, self.x]
        elif i < 3:

            @pl.when(self.between)
            def _():
                self.over[i - 1, self.within, self.x] = self.outs[i, self.x]

    def shared_down(self):
        self.loads[5].wait()
        shared = jnp.dot(
            self.all_hidden(self.outer), self.wsd[...], preferred_element_type=F32
        )
        self.acc[...] = self.mixed[...].astype(F32) + shared

    def collect(self, n):
        plane = (self.z, self.mate)[n]

        def whole(d):
            block = plane * self.inner + (self.x + d) % self.inner
            rcopy(
                self.ret.at[block],
                self.ret.at[block],
                self.ret_s.at[n, d],
                self.ret_r.at[block],
                {"sp": (self.own + 1) % self.n_sp},
            ).wait_recv()

        def in_halves(d):
            x_of = (self.x + d) % self.inner
            for h, cols in enumerate(self.cuts()):
                piece = self.ret.at[plane * self.inner + x_of, :, cols]
                rcopy(
                    piece, piece, self.ret_s.at[n, d], self.ret_h.at[x_of, h], {"sp": (self.own + 1) % self.n_sp}
                ).wait_recv()

        if n == 0:
            for d in range(1, self.inner):
                whole(d)
        else:

            @pl.when(self.at_end)
            def _():
                for d in range(self.inner):
                    whole(d)

            @pl.when(self.between)
            def _():
                for d in range(self.inner):
                    in_halves(d)

        rows = jnp.concatenate(
            [self.ret[plane * self.inner + p] for p in range(self.inner)], axis=0
        )
        self.acc[...] += jnp.dot(self.back[n], rows, preferred_element_type=F32)

    def close(self):
        for h, cols in enumerate(self.cuts()):
            piece = self.far.at[:, cols]
            rcopy(
                piece, piece, self.sum_s.at[0, h], self.far_r.at[h], {"sp": (self.own + 1) % self.n_sp}
            ).wait_recv()
            self.out[:, cols] = (self.acc[:, cols] + self.far[:, cols].astype(F32)).astype(BF16)

    def finish(self):
        groups = [self.meta_group, self.inv_group, self.ssq_group]
        for n in range(self.outer + 1):
            groups += [[self.part_copy(n)], self.pair_copies(n), [self.hid_copy(n)]]
        groups += [self.cross_copies(0), self.own_copies()]
        for group in groups:
            for c in group:
                c.wait_send()

        def all_sent(group):
            for c in group:
                c.wait_send()

        for i in range(self.outer):
            self.each_return(i, all_sent, True)

        @pl.when(self.between)
        def _():
            all_sent(self.relay_copies())
            for i in range(1, self.outer):
                all_sent(self.cross_copies(i))
            for h in range(2):
                for i in range(self.outer - 1):
                    all_sent(self.ahead_copies(i, h))
            for c in range(2):
                for h in range(CUTS):
                    self.sum_copy(c, h).wait_send()

    def middle_only(self, *steps):
        @pl.when(self.between)
        def _():
            for step in steps:
                step()

    def end_only(self, step):
        @pl.when(self.at_end)
        def _():
            step()

    def relay(self, h):
        self.receive(self.mate, h)
        for c in self.relay_copies(h):
            c.start()

    def pass_on(self, i, h):
        self.receive(self.order[i], h)
        self.push(i, h)

    def run(self):
        for c in self.own_copies():
            c.start()
        self.wait_route()
        self.middle_only(lambda: self.push(0, 0), lambda: self.push(0, 1))
        self.send_squares()
        self.select(0)
        self.middle_only(lambda: self.relay(0), lambda: self.pass_on(1, 0))
        self.send_scales()
        self.middle_only(
            lambda: self.relay(1), lambda: self.pass_on(1, 1), lambda: self.select(1)
        )
        shared = self.outer
        self.shared_gate_up()
        self.gate_up(0)
        self.pair(shared)
        self.pair(0)
        self.middle_only(
            lambda: self.pass_on(2, 0),
            lambda: self.pass_on(2, 1),
            lambda: self.select(2),
            lambda: self.select(3),
        )
        self.gate_up(1)
        self.hidden(shared)
        self.hidden(0)
        self.pair(1)
        self.shared_down()
        self.down_rows(0)
        self.gate_up(2)
        self.hidden(1)
        self.pair(2)
        self.gate_up(3)
        self.pair(3)
        self.down_rows(1)
        self.hidden(2)
        self.end_only(lambda: self.bring_along(1))
        self.down_rows(2)
        self.hidden(3)
        self.end_only(lambda: self.bring_along(2))
        self.down_rows(3)
        self.collect(0)
        self.end_only(lambda: self.bring_along(3))
        self.middle_only(lambda: self.add_over(0), lambda: self.add_over(1))
        self.collect(1)
        self.close()
        self.finish()


def moe_scratch(n_sp, n_tp, inner, el, cap, tok, width, ff):
    outer, rw = n_sp // inner, el * cap
    assert inner * rw == tok
    vmem, dma = pltpu.VMEM, pltpu.SemaphoreType.DMA
    return {
        "wgu": vmem((el, width, 2 * ff), BF16),
        "wd": vmem((el, ff, width), BF16),
        "wsgu": vmem((width, 2 * ff), BF16),
        "wsd": vmem((ff, width), BF16),
        "dense": vmem((outer, tok, width), BF16),
        "ahead": vmem((outer - 1, inner, rw, width), BF16),
        "picked": vmem((outer, inner, rw, width), BF16),
        "rows": vmem((outer, inner, rw, width), BF16),
        "meta": vmem((n_sp, 8, tok), F32),
        "inv": vmem((n_sp, 8, tok), F32),
        "ssq": vmem((n_tp, 8, tok), F32),
        "gu": vmem((outer + 1, 2, tok // 2, 2 * ff), BF16),
        "parts": vmem((outer + 1, tok // 2, 2 * ff), BF16),
        "pairs": vmem((outer + 1, tok // 2, 2 * ff), BF16),
        "sides": vmem((outer + 1, n_tp // 2, tok // 2, 2 * ff), BF16),
        "hid": vmem((outer + 1, 2, tok // 2, ff), BF16),
        "outs": vmem((outer, inner, rw, width), BF16),
        "ret": vmem((n_sp, rw, width), BF16),
        "back": vmem((2, tok, inner * rw), BF16),
        "over": vmem((2, 2, inner, rw, width), BF16),
        "sums": vmem((2, tok, width), BF16),
        "far": vmem((tok, width), BF16),
        "acc": vmem((tok, width), F32),
        "w_sem": dma((6,)),
        "meta_s": dma((n_sp,)),
        "meta_r": dma((n_sp,)),
        "inv_s": dma((n_sp,)),
        "inv_r": dma((n_sp,)),
        "ssq_s": dma((n_tp,)),
        "ssq_r": dma((n_tp,)),
        "dense_s": dma((outer, 2)),
        "dense_r": dma((outer, 2)),
        "x_s": dma((outer, inner, 2)),
        "x_r": dma((outer, inner, 2)),
        "ahead_s": dma((outer - 1, inner, 2)),
        "part_s": dma((outer + 1,)),
        "part_r": dma((outer + 1,)),
        "pair_s": dma((outer + 1, n_tp // 2)),
        "pair_r": dma((outer + 1, n_tp // 2)),
        "hid_s": dma((outer + 1,)),
        "hid_r": dma((outer + 1,)),
        "ret_s": dma((outer, inner)),
        "ret_r": dma((n_sp,)),
        "beside": vmem((outer - 1, inner, rw, width), BF16),
        "beside_s": dma((outer - 1, inner, CUTS)),
        "beside_r": dma((outer - 1, inner, CUTS)),
        "ret_h": dma((inner, CUTS)),
        "over_s": dma((outer, inner, CUTS)),
        "over_r": dma((2, 2, inner, CUTS)),
        "sum_s": dma((2, CUTS)),
        "far_r": dma((CUTS,)),
    }


class Attend:
    def __init__(self, n_sp, n_tp, inner, refs):
        self.n_sp, self.n_tp, self.inner = n_sp, n_tp, inner
        self.outer = n_sp // inner
        self.__dict__.update(refs)
        self.own = lax.axis_index("sp")
        self.me = lax.axis_index("tp")
        self.z = self.own // inner
        self.x = self.own % inner
        self.order = plane_order(self.z, self.outer)
        self.heads, self.tok = self.bias.shape
        self.hd = self.queries.shape[1] // self.heads
        self.partner = self.me + 1 - 2 * (self.me % 2)
        self.peers = [(self.me + 2 * d) % n_tp for d in range(1, n_tp // 2)]

    def load(self):
        pairs = (
            (self.keys, self.kv),
            (self.values, self.vv),
            (self.queries, self.qv),
            (self.bias, self.bv),
        )
        self.loads = [
            pltpu.make_async_copy(src, dst, self.a_sem.at[i]) for i, (src, dst) in enumerate(pairs)
        ]
        for c in self.loads:
            c.start()

    def load_late(self):
        pairs = ((self.stream, self.sv), (self.out_proj, self.wo))
        self.late = [
            pltpu.make_async_copy(src, dst, self.a_sem.at[4 + i])
            for i, (src, dst) in enumerate(pairs)
        ]
        for c in self.late:
            c.start()

    def head_of(self, ref, head):
        return ref.at[:, pl.ds(pl.multiple_of(head * self.hd, self.hd), self.hd)]

    def exchange_copies(self, kind, i):
        src, dst = ((self.kv, self.kb), (self.vv, self.vb), (self.qv, self.qb))[kind]
        plane = self.order[i]
        target = dst.at[self.z, self.x] if kind < 2 else dst.at[self.z]
        return [
            rcopy(
                self.head_of(src, plane),
                target,
                self.e_s.at[kind, i],
                self.q_r.at[self.z] if kind == 2 else self.kv_r.at[kind, self.z, self.x],
                {"sp": plane * self.inner + self.x},
            )
        ]

    def side_copies(self, kind, i):
        dst = (self.kb, self.vb)[kind]
        plane = self.order[i]
        src = dst.at[plane, self.x] if i else self.head_of((self.kv, self.vv)[kind], self.z)
        return [
            rcopy(
                src,
                dst.at[plane, self.x],
                self.side_s.at[kind, i, d],
                self.kv_r.at[kind, plane, self.x],
                {"sp": self.z * self.inner + (self.x + d) % self.inner},
            )
            for d in range(1, self.inner)
        ]

    def wait_kv(self, kind, plane, x):
        dst = (self.kb, self.vb)[kind].at[plane, x]
        rcopy(
            dst, dst, self.e_s.at[kind, 0], self.kv_r.at[kind, plane, x], {"sp": (self.own + 1) % self.n_sp}
        ).wait_recv()

    def bias_copies(self):
        return [
            rcopy(
                self.bi.at[self.own],
                self.bi.at[self.own],
                self.bi_s.at[d],
                self.bi_r.at[self.own],
                {"sp": (self.own + d) % self.n_sp},
            )
            for d in range(1, self.n_sp)
        ]

    def exchange(self):
        for kind in range(3):
            self.loads[kind].wait()
            for i in range(self.outer - 1, 0, -1):
                for c in self.exchange_copies(kind, i):
                    c.start()
            if kind < 2:
                for c in self.side_copies(kind, 0):
                    c.start()
        self.loads[3].wait()
        self.bi[self.own, : self.heads, :] = self.bv[...].astype(F32)
        for c in self.bias_copies():
            c.start()
        self.kb[self.z, self.x] = self.head_of(self.kv, self.z)[...]
        self.vb[self.z, self.x] = self.head_of(self.vv, self.z)[...]
        self.qb[self.z] = self.head_of(self.qv, self.z)[...]

    def hand_over(self):
        for i in range(1, self.outer):
            for kind in range(2):
                self.wait_kv(kind, self.order[i], self.x)
                for c in self.side_copies(kind, i):
                    c.start()
        for d in range(1, self.n_sp):
            block = (self.own + d) % self.n_sp
            rcopy(
                self.bi.at[block],
                self.bi.at[block],
                self.bi_s.at[d],
                self.bi_r.at[block],
                {"sp": (self.own + 1) % self.n_sp},
            ).wait_recv()

    def compute(self):
        tok, hd = self.tok, self.hd
        scale = hd ** (-0.5)
        row = lax.broadcasted_iota(jnp.int32, (tok, tok), 0)
        col = lax.broadcasted_iota(jnp.int32, (tok, tok), 1)
        later = (row > col).astype(F32)
        sums = jnp.concatenate([later, jnp.ones((tok, tok), F32)], axis=1).astype(BF16)
        sums = jnp.concatenate([sums, sums], axis=0)
        for j in range(self.outer):
            for d in range(1, self.inner):
                for kind in range(2):
                    self.wait_kv(kind, j, (self.x + d) % self.inner)

            @pl.when(self.z != j)
            def _():
                rcopy(
                    self.qb.at[j], self.qb.at[j], self.e_s.at[2, 0], self.q_r.at[j], {"sp": (self.own + 1) % self.n_sp}
                ).wait_recv()

            q = self.qb[j]
            acc = jnp.zeros((tok, hd), F32)
            carry = jnp.zeros((tok, tok), F32)
            for k in range(j, -1, -1):
                for p in range(self.inner - 1, -1, -1):
                    bias = self.bi[k * self.inner + p, pl.ds(self.z, 1), :]
                    logit = rows_contract(q, self.kb[k, p]) * scale + bias
                    low = jnp.log(1.0 + jnp.exp(-jnp.abs(logit)))
                    fail = -(jnp.maximum(logit, 0.0) + low)
                    hit = jnp.minimum(logit, 0.0) - low
                    if k == j:
                        before = col < row + (self.x - p) * tok
                        fail = jnp.where(before, fail, 0.0)
                    high = fail.astype(BF16)
                    rest = (fail - high.astype(F32)).astype(BF16)
                    both = jnp.dot(
                        jnp.concatenate([high, rest], axis=1), sums, preferred_element_type=F32
                    )
                    w = jnp.exp(hit + both[:, :tok] + carry)
                    if k == j:
                        w = jnp.where(before, w, 0.0)
                    carry = carry + both[:, tok:]
                    acc = acc + jnp.dot(
                        w.astype(BF16), self.vb[k, p], preferred_element_type=F32
                    )
            self.ob[j] = acc.astype(BF16)

            @pl.when(self.z != j)
            def _():
                self.out_copy(j).start()

            @pl.when(self.z == j)
            def _():
                self.att[self.me, self.z] = self.ob[j]

    def out_copy(self, j):
        return rcopy(
            self.ob.at[j],
            self.att.at[self.me, self.z],
            self.o_s.at[j],
            self.att_r.at[self.me, self.z],
            {"sp": j * self.inner + self.x},
        )

    def wait_att(self, source, head):
        piece = self.att.at[source, head]
        rcopy(
            piece, piece, self.o_s.at[0], self.att_r.at[source, head], {"tp": (self.me + 1) % self.n_tp}
        ).wait_recv()

    def piece_copies(self, source, head, slot, targets):
        piece = self.att.at[source, head]
        return [
            rcopy(piece, piece, self.g_s.at[slot + n, head], self.att_r.at[source, head], {"tp": to})
            for n, to in enumerate(targets)
        ]

    def gather(self):
        wide = self.heads * self.hd

        def part(source):
            rows = jnp.concatenate([self.att[source, h] for h in range(self.outer)], axis=1)
            first = pl.multiple_of(source * wide, wide)
            return jnp.dot(rows, self.wo[pl.ds(first, wide), :], preferred_element_type=F32)

        slots = 1 + len(self.peers)
        for i in range(self.outer):
            head = self.order[i]
            if i:
                self.wait_att(self.me, head)
            for c in self.piece_copies(self.me, head, 0, self.peers + [self.partner]):
                c.start()
        for c in self.late:
            c.wait()
        self.acc[...] = self.sv[...].astype(F32) + part(self.me)
        for n, peer in enumerate(self.peers):
            for i in range(self.outer):
                self.wait_att(peer, self.order[i])
                for c in self.piece_copies(peer, self.order[i], slots + n, [self.partner]):
                    c.start()
        for i in range(self.outer):
            self.wait_att(self.partner, self.order[i])
        self.acc[...] += part(self.partner)
        for peer in self.peers:
            self.acc[...] += part(peer)
        others = [(self.partner + 2 * d) % self.n_tp for d in range(1, self.n_tp // 2)]
        for other in others:
            for i in range(self.outer):
                self.wait_att(other, self.order[i])
        total = self.acc[...]
        for other in others:
            total = total + part(other)
        self.mixed[...] = total.astype(BF16)

    def finish(self):
        groups = [self.bias_copies()]
        for i in range(1, self.outer):
            groups += [self.exchange_copies(kind, i) for kind in range(3)]
        for i in range(self.outer):
            groups += [self.side_copies(kind, i) for kind in range(2)]
            groups.append(
                self.piece_copies(self.me, self.order[i], 0, self.peers + [self.partner])
            )
            for n, peer in enumerate(self.peers):
                groups.append(
                    self.piece_copies(
                        peer, self.order[i], 1 + len(self.peers) + n, [self.partner]
                    )
                )
        for group in groups:
            for c in group:
                c.wait_send()
        for j in range(self.outer):

            @pl.when(self.z != j)
            def _():
                self.out_copy(j).wait_send()


LAYER_INPUTS = (
    "queries", "keys", "values", "bias", "stream", "out_proj", "gain_in", "ids_in", "wts_in",
    "gate", "up", "down", "s_gate", "s_up", "s_down",
)


def attend_scratch(n_sp, n_tp, inner, heads, hd, tok, width, top_k):
    outer = n_sp // inner
    vmem, dma = pltpu.VMEM, pltpu.SemaphoreType.DMA
    wide = heads * hd
    return {
        "qv": vmem((tok, wide), BF16),
        "kv": vmem((tok, wide), BF16),
        "vv": vmem((tok, wide), BF16),
        "bv": vmem((heads, tok), BF16),
        "sv": vmem((tok, width), BF16),
        "wo": vmem((n_tp * wide, width), BF16),
        "qb": vmem((outer, tok, hd), BF16),
        "kb": vmem((outer, inner, tok, hd), BF16),
        "vb": vmem((outer, inner, tok, hd), BF16),
        "bi": vmem((n_sp, 8, tok), F32),
        "ob": vmem((outer, tok, hd), BF16),
        "att": vmem((n_tp, outer, tok, hd), BF16),
        "mixed": vmem((tok, width), BF16),
        "gain": vmem((1, width), F32),
        "ids": vmem((top_k, tok), jnp.int32),
        "wts": vmem((top_k, tok), F32),
        "a_sem": dma((6,)),
        "s_sem": dma((3,)),
        "e_s": dma((3, outer)),
        "q_r": dma((outer,)),
        "kv_r": dma((2, outer, inner)),
        "side_s": dma((2, outer, inner)),
        "bi_s": dma((n_sp,)),
        "bi_r": dma((n_sp,)),
        "o_s": dma((outer,)),
        "att_r": dma((n_tp, outer)),
        "g_s": dma((n_tp, outer)),
    }


def layer_kernel(n_sp, n_tp, inner, el, cap, names, *refs):
    named = dict(zip(names, refs))
    first = Attend(n_sp, n_tp, inner, named)
    second = Experts(n_sp, n_tp, inner, el, cap, named)
    first.load()
    small = [
        pltpu.make_async_copy(named[name + "_in"], named[name], named["s_sem"].at[i])
        for i, name in enumerate(("ids", "wts", "gain"))
    ]
    for c in small:
        c.start()
    greet_all(n_sp, n_tp, first.own, first.me)
    first.load_late()
    second.load_weights()
    for c in small:
        c.wait()
    second.route()
    second.build_back()
    await_all(n_sp, n_tp)
    first.exchange()
    second.send_route()
    first.hand_over()
    first.compute()
    first.gather()
    second.run()
    first.finish()


def layer(operands, n_sp, n_tp, inner, cap, heads, hd):
    tok, width = operands[4].shape
    el, ff = operands[11].shape[:2]
    top_k = operands[7].shape[0]
    scratch = attend_scratch(n_sp, n_tp, inner, heads, hd, tok, width, top_k)
    scratch |= moe_scratch(n_sp, n_tp, inner, el, cap, tok, width, ff)
    hbm = pl.BlockSpec(memory_space=pltpu.MemorySpace.HBM)
    names = LAYER_INPUTS + ("out",) + tuple(scratch)
    return pl.pallas_call(
        functools.partial(layer_kernel, n_sp, n_tp, inner, el, cap, names),
        out_shape=jax.ShapeDtypeStruct((tok, width), BF16),
        in_specs=[hbm] * len(operands),
        out_specs=pl.BlockSpec(memory_space=pltpu.VMEM),
        scratch_shapes=list(scratch.values()),
        compiler_params=pltpu.CompilerParams(
            vmem_limit_bytes=56 * 2**20, collective_id=0, has_side_effects=True
        ),
        cost_estimate=pl.CostEstimate(flops=10**10, bytes_accessed=2**24, transcendentals=10**6),
    )(*operands)


def body(
    queries,
    key_rows,
    value_rows,
    break_bias,
    stream,
    out_proj,
    norm_gain,
    expert_ids,
    route_weights,
    gate_proj,
    up_proj,
    down_proj,
    shared_gate,
    shared_up,
    shared_down,
):
    tok = queries.shape[0]
    heads = break_bias.shape[1]
    hd = queries.shape[1] // heads
    n_sp = lax.axis_size("sp")
    n_tp = lax.axis_size("tp")
    width = stream.shape[1] * n_tp

    bias_wide = jnp.pad(break_bias, ((0, 0), (0, hd - heads)))

    experts_local = gate_proj.shape[0]
    experts = experts_local * n_sp
    top_k = expert_ids.shape[1]
    cap = 2 * top_k * tok // experts
    n_inner = max(d for d in range(1, n_sp + 1) if n_sp % d == 0 and d * d <= n_sp)
    plane_rows = n_inner * experts_local * cap
    if heads * n_inner == n_sp and heads == 4 and plane_rows == tok and cap % 16 == 0 and tok % (16 * n_tp) == 0:
        operands = (
            queries, key_rows, value_rows, break_bias.T, stream, out_proj, norm_gain[None, :],
            expert_ids.T, route_weights.T, gate_proj, up_proj, down_proj,
            shared_gate, shared_up, shared_down,
        )
        return layer(operands, n_sp, n_tp, n_inner, cap, heads, hd)
    expert_of = jnp.arange(experts, dtype=jnp.int32)
    named = expert_ids[:, :, None] == expert_of[None, None, :]
    named_any = jnp.any(named, axis=1).astype(BF16)
    token = jnp.arange(tok, dtype=jnp.int32)
    earlier = (token[None, :] < token[:, None]).astype(BF16)
    rank_all = jnp.dot(earlier, named_any, preferred_element_type=F32)
    rank = jnp.sum(jnp.where(named, rank_all[:, None, :], 0.0), axis=2).astype(jnp.int32)
    slot = expert_ids * cap + rank
    slots = experts * cap
    place = jnp.arange(slots, dtype=jnp.int32)
    spot = slot[:, :, None] == place[None, None, :]
    send_pick = jnp.any(spot, axis=1).astype(BF16)
    back_pick = jnp.sum(jnp.where(spot, route_weights[:, :, None], 0.0), axis=1).astype(BF16)

    attended = attention(queries, key_rows, value_rows, bias_wide, heads, hd, n_sp)
    projected = jnp.dot(
        lax.all_gather(attended, "tp", axis=1, tiled=True), out_proj, preferred_element_type=F32
    )
    mixed = (stream.astype(F32) + projected).astype(BF16)
    mixed = lax.optimization_barrier(mixed)
    mixed_f = mixed.astype(F32)
    square_sum = lax.psum(jnp.sum(mixed_f * mixed_f, axis=1), "tp")
    inv_rms = lax.rsqrt(square_sum / width + EPS)
    normed = (mixed_f * inv_rms[:, None] * norm_gain[None, :]).astype(BF16)

    send = lax.dot_general(
        send_pick, normed, (((0,), (0,)), ((), ())), preferred_element_type=F32
    ).astype(BF16)
    send = send.reshape(n_sp, experts_local * cap, normed.shape[1])
    arrived = lax.all_to_all(send, "sp", split_axis=0, concat_axis=0, tiled=True)
    arrived = arrived.reshape(n_sp, experts_local, cap, -1)
    gates, ups = [], []
    for e in range(experts_local):
        rows = arrived[:, e].reshape(n_sp * cap, -1)
        gates.append(jnp.dot(rows, gate_proj[e], preferred_element_type=F32).astype(BF16))
        ups.append(jnp.dot(rows, up_proj[e], preferred_element_type=F32).astype(BF16))
    gates.append(jnp.dot(normed, shared_gate, preferred_element_type=F32).astype(BF16))
    ups.append(jnp.dot(normed, shared_up, preferred_element_type=F32).astype(BF16))
    gate_all = jnp.concatenate(gates, axis=0)
    up_all = jnp.concatenate(ups, axis=0)
    gate_up = jnp.concatenate([gate_all, up_all], axis=1)
    hidden = exchange(gate_up, n_tp)
    outs = []
    for e in range(experts_local):
        rows = hidden[e * n_sp * cap : (e + 1) * n_sp * cap]
        out = jnp.dot(rows, down_proj[e], preferred_element_type=F32).astype(BF16)
        outs.append(out.reshape(n_sp, 1, cap, -1))
    expert_out = jnp.concatenate(outs, axis=1).reshape(n_sp, experts_local * cap, -1)
    returned = lax.all_to_all(expert_out, "sp", split_axis=0, concat_axis=0, tiled=True)
    returned = returned.reshape(slots, -1)
    shared_out = jnp.dot(
        hidden[experts_local * n_sp * cap :], shared_down, preferred_element_type=F32
    )
    routed = jnp.dot(back_pick, returned, preferred_element_type=F32)
    return (mixed_f + shared_out + routed).astype(BF16)


def solution(mesh):
    in_specs = (
        P("sp", "tp"),
        P("sp", "tp"),
        P("sp", "tp"),
        P("sp", "tp"),
        P("sp", "tp"),
        P(None, "tp"),
        P("tp"),
        P("sp", None),
        P("sp", None),
        P("sp", "tp", None),
        P("sp", "tp", None),
        P("sp", None, "tp"),
        P("tp", None),
        P("tp", None),
        P(None, "tp"),
    )
    return jax.shard_map(body, mesh=mesh, in_specs=in_specs, out_specs=P("sp", "tp"), check_vma=False)
```
